32 devices in a mesh: sp: 8 (over z, x), dp: 4 (over y, core).
Axes of the slice: x: 2, y: 2, z: 4, core: 2. Of those that a mesh axis runs over, the one named last changes fastest.
Arguments:
- residual_in: bfloat16 [4, 1024, 2048], P('dp', 'sp'), may hold values from -6 to 6
- query_proj: bfloat16 [4, 1024, 2048], P('dp', 'sp'), may hold values from -8 to 8
- key_proj: bfloat16 [4, 1024, 512], P('dp', 'sp'), may hold values from -8 to 8
- value_proj: bfloat16 [4, 1024, 512], P('dp', 'sp'), may hold values from -6 to 6
- query_gain: float32 [128], replicated, may hold values from 0.1 to 7
- key_gain: float32 [128], replicated, may hold values from 0.1 to 7
- out_weight: bfloat16 [2048, 2048], replicated, may hold values from -0.125 to 0.125
- post_gain: float32 [2048], replicated, may hold values from 0.1 to 1.9
- pre_gain: float32 [2048], replicated, may hold values from 0.1 to 1.9
- route_ids: int32 [4, 1024, 2], P('dp', 'sp'), may hold values from 0 to 31, as said below
- group_weight: float32 [4, 1024], P('dp', 'sp'), may hold values from 0.25 to 1
- first_share: float32 [4, 1024], P('dp', 'sp'), may hold values from 0.5 to 1
- gate_weight: bfloat16 [32, 2048, 512], P(('sp', 'dp')), may hold values from -0.125 to 0.125
- up_weight: bfloat16 [32, 2048, 512], P(('sp', 'dp')), may hold values from -0.125 to 0.125
- down_weight: bfloat16 [32, 512, 2048], P(('sp', 'dp')), may hold values from -0.25 to 0.25
Outputs:
- layer_out: bfloat16 [4, 1024, 2048], P('dp', 'sp')
The draws below stay inside these ranges and needn't reach their ends.
Inputs may be any that keep to these rules, and one draw needn't show every extreme that they name: `route_ids`: each token names two different experts of one group of 8 consecutive experts. Among the 128 tokens of one device each group is chosen by exactly 32 tokens, no expert is named by more than 16 of them, and in every draw one expert of each group is named by exactly 16 tokens of every device.
All inputs are finite; a program needn't handle non-finite values.
Results may differ from the reference program's by a relative error of at most 0.009.
The reference program's roundings to bfloat16 on the way count: a program that leaves them out, or rounds other values in their place, can miss the bound.
Values may be sent and summed in bfloat16 or wider, within the bound.
A program may use at most 128 MiB of HBM per device.

```python
import jax
import jax.numpy as jnp
from jax import lax

D = 2048
HEADS = 16
KV_HEADS = 4
HEAD_DIM = 128
FF = 512
GROUPS = 4
GRID_W = 64
TOK_DEV = 128
SEQS = 4
SEQ = 1024
EXPERTS = 32
CAP = 16
N_SP = 8
N_DP = 4


def draw_query_proj(key, part):
    own = jax.random.fold_in(key, 11)
    base = jax.random.truncated_normal(own, -6.0, 6.0, (SEQS, SEQ, HEADS * HEAD_DIM), jnp.float32)
    return base.astype(jnp.bfloat16)


def draw_key_proj(key, part):
    own = jax.random.fold_in(key, 12)
    base = jax.random.truncated_normal(own, -6.0, 6.0, (SEQS, SEQ, KV_HEADS * HEAD_DIM), jnp.float32)
    return base.astype(jnp.bfloat16)


def gain_table(own):
    return 1.0 + 0.18 * jax.random.truncated_normal(own, -5.0, 5.0, (HEAD_DIM,), jnp.float32)


def draw_query_gain(key, part):
    return gain_table(jax.random.fold_in(key, 21))


def draw_key_gain(key, part):
    return gain_table(jax.random.fold_in(key, 22))


def draw_route_ids(key, part):
    per_group = TOK_DEV // GROUPS
    group_width = EXPERTS // GROUPS
    middle = CAP // 2
    hot = jax.random.randint(jax.random.fold_in(key, 31), (GROUPS,), 0, group_width)
    block_count = SEQS * (SEQ // TOK_DEV)

    def one_block(block_key):
        key_tok, key_rest = jax.random.split(block_key)
        order = jax.random.permutation(key_tok, TOK_DEV)
        firsts = []
        seconds = []
        for group_id in range(GROUPS):
            group_key = jax.random.fold_in(key_rest, group_id)
            key_perm, key_shift, key_swap = jax.random.split(group_key, 3)
            shuffled = jax.random.permutation(key_perm, group_width).astype(jnp.int32)
            shifts = jax.random.randint(key_shift, (group_width // 2,), -middle, middle + 1)
            hot_place = jnp.sum(jnp.where(shuffled == hot[group_id], jnp.arange(group_width, dtype=jnp.int32), 0))
            sign_value = 1 - 2 * (hot_place % 2)
            shifts = shifts.at[hot_place // 2].set(middle * sign_value)
            counts = jnp.zeros((group_width,), jnp.int32).at[shuffled[0::2]].set(middle + shifts).at[shuffled[1::2]].set(middle - shifts)
            listed = jnp.repeat(jnp.arange(group_width, dtype=jnp.int32), counts, total_repeat_length=2 * per_group)
            first_pick = listed[:per_group]
            second_pick = listed[per_group:]
            swap_bits = jax.random.randint(key_swap, (per_group,), 0, 2)
            leading = jnp.where(swap_bits == 1, second_pick, first_pick)
            trailing = jnp.where(swap_bits == 1, first_pick, second_pick)
            firsts.append(leading + group_id * group_width)
            seconds.append(trailing + group_id * group_width)
        pairs = jnp.stack([jnp.concatenate(firsts), jnp.concatenate(seconds)], axis=1).astype(jnp.int32)
        return jnp.zeros((TOK_DEV, 2), jnp.int32).at[order].set(pairs)
    blocks_all = jax.vmap(one_block)(jax.random.split(jax.random.fold_in(key, 32), block_count))
    return blocks_all.reshape(SEQS, SEQ, 2)


def level_of(rng, shape, cuts, least, top_value):
    level, own = 1.0, jax.random.fold_in(rng, 6)
    for axis_at, shards_of in cuts:
        steps = jnp.exp(jax.random.uniform(jax.random.fold_in(own, axis_at), (shards_of,), jnp.float32, least / len(cuts), top_value / len(cuts)))
        level = level * jnp.repeat(steps, shape[axis_at] // shards_of).reshape([-1 if axis == axis_at else 1 for axis in range(len(shape))])
    return level


def bell_draw(key, shape, deviation, bound, cuts=(), kind=jnp.bfloat16):
    entries = jax.random.normal(key, shape, jnp.float32) * deviation
    if len(cuts) > 0:
        entries = level_of(key, shape, cuts, -0.22, 0.18) * entries
    return jnp.clip(entries, min=-bound, max=bound).astype(kind)


def setup_inputs(seed: int = 0) -> dict:
    keys = jax.random.split(jax.random.key(seed), 16)
    residual_in = bell_draw(keys[0], (SEQS, SEQ, D), 1.0, 6.0, ((0, 4), (1, 8)))
    query_proj = draw_query_proj(jax.random.fold_in(keys[15], 71), 0)
    key_proj = draw_key_proj(jax.random.fold_in(keys[15], 71), 0)
    value_proj = bell_draw(keys[3], (SEQS, SEQ, KV_HEADS * HEAD_DIM), 1.0, 6.0, ((0, 4), (1, 8)))
    query_gain = draw_query_gain(jax.random.fold_in(keys[15], 71), 0)
    key_gain = draw_key_gain(jax.random.fold_in(keys[15], 71), 0)
    out_weight = bell_draw(keys[6], (D, D), D ** -0.5, 0.125)
    post_gain = jnp.clip(1.0 + 0.18 * jax.random.normal(keys[7], (D,), jnp.float32), 0.1, 1.9)
    pre_gain = jnp.clip(1.0 + 0.18 * jax.random.normal(keys[8], (D,), jnp.float32), 0.1, 1.9)
    route_ids = draw_route_ids(jax.random.fold_in(keys[15], 71), 0)
    group_weight = jnp.clip(0.25 + 0.75 * jax.random.uniform(keys[10], (SEQS, SEQ), jnp.float32) ** level_of(keys[10], (SEQS, SEQ), ((0, 4), (1, 8)), -0.2, 0.2), 0.25, 1.0)
    first_share = jnp.clip(0.5 + 0.5 * jax.random.uniform(keys[11], (SEQS, SEQ), jnp.float32) ** level_of(keys[11], (SEQS, SEQ), ((0, 4), (1, 8)), -0.2, 0.2), 0.5, 1.0)
    gate_weight = bell_draw(keys[12], (EXPERTS, D, FF), D ** -0.5, 0.125, ((0, 32),))
    up_weight = bell_draw(keys[13], (EXPERTS, D, FF), D ** -0.5, 0.125, ((0, 32),))
    down_weight = bell_draw(keys[14], (EXPERTS, FF, D), FF ** -0.5, 0.25, ((0, 32),))
    return {"residual_in": residual_in, "query_proj": query_proj, "key_proj": key_proj, "value_proj": value_proj, "query_gain": query_gain, "key_gain": key_gain, "out_weight": out_weight, "post_gain": post_gain, "pre_gain": pre_gain, "route_ids": route_ids, "group_weight": group_weight, "first_share": first_share, "gate_weight": gate_weight, "up_weight": up_weight, "down_weight": down_weight}


EPSILON = 1e-06

def rotate_heads(raw_heads, gain_vec, positions):
    floats = raw_heads.astype(jnp.float32)
    normed = floats * lax.rsqrt(lax.optimization_barrier(jnp.mean(floats * floats, axis=-1, keepdims=True)) + EPSILON) * gain_vec
    quarter = raw_heads.shape[-1] // 4
    inverse = 10000.0 ** (-jnp.arange(quarter, dtype=jnp.float32) / quarter)
    grid_rows = (positions // GRID_W).astype(jnp.float32)[:, None] * inverse
    grid_cols = (positions % GRID_W).astype(jnp.float32)[:, None] * inverse
    angles = jnp.concatenate([grid_rows, grid_rows, grid_cols, grid_cols], axis=-1)[:, None, :]
    pieces = normed.reshape(normed.shape[:-1] + (2, 2, quarter))
    turned = jnp.stack([-pieces[..., 1, :], pieces[..., 0, :]], axis=-2).reshape(normed.shape)
    return (normed * jnp.cos(angles) + turned * jnp.sin(angles)).astype(jnp.bfloat16)

def attend_blocks(queries, keys_all, values_all):
    count_q, kv_count, group_size, head_width = queries.shape
    block = min(512, count_q)
    blocks = count_q // block
    scale = head_width ** (-0.5)
    zero_index = jnp.zeros((), jnp.int32)

    def one_item(item):
        which = (item // kv_count).astype(jnp.int32)
        head_index = (item % kv_count).astype(jnp.int32)
        start_row = (which * block).astype(jnp.int32)
        q_block = lax.dynamic_slice(queries, (start_row, head_index, zero_index, zero_index), (block, 1, group_size, head_width))[:, 0]
        key_block = lax.dynamic_slice(keys_all, (zero_index, head_index, zero_index), (keys_all.shape[0], 1, head_width))[:, 0]
        value_block = lax.dynamic_slice(values_all, (zero_index, head_index, zero_index), (values_all.shape[0], 1, head_width))[:, 0]
        scores = jnp.einsum('qgd,sd->gqs', q_block.astype(jnp.float32), key_block.astype(jnp.float32)) * scale
        shifted = jnp.exp(scores - lax.optimization_barrier(jnp.max(scores, axis=-1, keepdims=True)))
        weights = (shifted / lax.optimization_barrier(jnp.sum(shifted, axis=-1, keepdims=True))).astype(jnp.bfloat16)
        return jnp.einsum('gqs,sd->qgd', weights.astype(jnp.float32), value_block.astype(jnp.float32)).astype(jnp.bfloat16)
    results = lax.map(one_item, jnp.arange(blocks * kv_count, dtype=jnp.int32))
    results = results.reshape(blocks, kv_count, block, group_size, head_width).transpose(0, 2, 1, 3, 4)
    return results.reshape(count_q, kv_count * group_size * head_width)

def rms_scale(values, gain_vec):
    floats = values.astype(jnp.float32)
    return floats * lax.rsqrt(lax.optimization_barrier(jnp.mean(floats * floats, axis=-1, keepdims=True)) + EPSILON) * gain_vec

def reference(residual_in, query_proj, key_proj, value_proj, query_gain, key_gain, out_weight, post_gain, pre_gain, route_ids, group_weight, first_share, gate_weight, up_weight, down_weight):
    group_size = HEADS // KV_HEADS

    def one_sequence(inputs):
        query_seq, key_seq, value_seq = inputs
        positions = jnp.arange(SEQ, dtype=jnp.int32)
        query_turned = rotate_heads(query_seq.reshape(SEQ, HEADS, HEAD_DIM), query_gain, positions)
        key_turned = rotate_heads(key_seq.reshape(SEQ, KV_HEADS, HEAD_DIM), key_gain, positions)
        return attend_blocks(query_turned.reshape(SEQ, KV_HEADS, group_size, HEAD_DIM), key_turned, value_seq.reshape(SEQ, KV_HEADS, HEAD_DIM))
    attended = lax.map(one_sequence, (query_proj, key_proj, value_proj)).reshape(SEQS * SEQ, D)
    mixed = jnp.dot(attended, out_weight, preferred_element_type=jnp.float32).astype(jnp.bfloat16)
    stream = (residual_in.reshape(SEQS * SEQ, D).astype(jnp.float32) + rms_scale(mixed, post_gain)).astype(jnp.bfloat16)
    normed = rms_scale(stream, pre_gain).astype(jnp.bfloat16)
    chosen = route_ids.reshape(-1).astype(jnp.int32)
    assigns = chosen.shape[0]
    order = jnp.argsort(chosen, stable=True).astype(jnp.int32)
    counts = jax.ops.segment_sum(jnp.ones((assigns,), jnp.int32), chosen, num_segments=EXPERTS).astype(jnp.int32)
    starts = (jnp.cumsum(counts) - counts).astype(jnp.int32)
    most = CAP * N_SP * N_DP
    order_pad = jnp.concatenate([order, jnp.full((most,), assigns, jnp.int32)])
    normed_pad = jnp.concatenate([normed, jnp.zeros((1, D), jnp.bfloat16)], axis=0)

    def per_expert(carry, inputs):
        index, gate_one, up_one, down_one = inputs
        picked = lax.dynamic_slice(order_pad, (starts[index].astype(jnp.int32),), (most,))
        valid = jnp.arange(most, dtype=jnp.int32) < counts[index]
        picked = jnp.where(valid, picked, assigns).astype(jnp.int32)
        rows_in = normed_pad[picked // 2]
        gated = jnp.dot(rows_in, gate_one, preferred_element_type=jnp.float32)
        lifted = jnp.dot(rows_in, up_one, preferred_element_type=jnp.float32)
        hidden = (jax.nn.silu(gated) * lifted).astype(jnp.bfloat16)
        produced = jnp.dot(hidden, down_one, preferred_element_type=jnp.float32).astype(jnp.bfloat16)
        return (carry.at[picked].set(produced), None)
    outputs, _ = lax.scan(per_expert, jnp.zeros((assigns + 1, D), jnp.bfloat16), (jnp.arange(EXPERTS, dtype=jnp.int32), gate_weight, up_weight, down_weight))
    results = outputs[:assigns].astype(jnp.float32).reshape(SEQS * SEQ, 2, D)
    share = first_share.reshape(-1)
    weight_pair = group_weight.reshape(-1)[:, None] * jnp.stack([share, 1.0 - share], axis=1)
    combined = lax.optimization_barrier(jnp.sum(weight_pair[:, :, None] * results, axis=1))
    return (stream.astype(jnp.float32) + combined).astype(jnp.bfloat16).reshape(SEQS, SEQ, D)
```

```python
import functools

import jax
import jax.numpy as jnp
import numpy as np
from jax import lax
from jax.experimental import pallas as pl
from jax.experimental.pallas import tpu as pltpu
from jax.sharding import PartitionSpec as P

HEAD_DIM = 128
GRID_W = 64
GROUPS = 4
EPSILON = 1e-06
MESH = pl.DeviceIdType.MESH
VMEM_LIMIT = 60 * 1024 * 1024
F32 = jnp.float32
BF16 = jnp.bfloat16


def angle_tables(length):
    quarter = HEAD_DIM // 4
    inverse = 10000.0 ** (-np.arange(quarter, dtype=np.float64) / quarter)
    positions = np.arange(length)
    rows = (positions // GRID_W)[:, None] * inverse
    cols = (positions % GRID_W)[:, None] * inverse
    angles = np.concatenate([rows, rows, cols, cols], axis=-1)
    sign = np.where(np.arange(HEAD_DIM) % (2 * quarter) < quarter, -1.0, 1.0)
    return np.cos(angles).astype(np.float32), (np.sin(angles) * sign).astype(np.float32)


def rotate(raw, gain, cos, sin):
    floats = raw.astype(F32)
    normed = floats * lax.rsqrt(jnp.mean(floats * floats, axis=-1, keepdims=True) + EPSILON) * gain
    quarter = HEAD_DIM // 4
    lane = lax.broadcasted_iota(jnp.int32, normed.shape, 1)
    turned = jnp.where(
        (lane & (2 * quarter - 1)) < quarter,
        pltpu.roll(normed, HEAD_DIM - quarter, 1),
        pltpu.roll(normed, quarter, 1),
    )
    return (normed * cos + turned * sin).astype(BF16)


def remote(src, dst, send_sem, recv_sem, device):
    return pltpu.make_async_remote_copy(
        src_ref=src,
        dst_ref=dst,
        send_sem=send_sem,
        recv_sem=recv_sem,
        device_id=device,
        device_id_type=MESH,
    )


def attention_kernel(
    nz, nx,
    q_ref, k_ref, v_ref, qg_ref, kg_ref, cos_ref, sin_ref, res_ref, post_ref, pre_ref, ow_hbm,
    stream_ref, normed_ref,
    k_all, v_all, q_rot, k_rot, att, acc, ow, ow_sem,
    rk, rv, skx, sku, skd, svx, svu, svd,
):
    tokens, width = q_ref.shape
    heads = width // HEAD_DIM
    kv_heads = k_ref.shape[1] // HEAD_DIM
    group = heads // kv_heads
    me = lax.axis_index("sp")
    dp = lax.axis_index("dp")
    z, x = me // nx, me % nx
    up, down = (me + nx, dp), (me - nx, dp)
    has_up, has_down = z < nz - 1, z > 0
    both = ((k_ref, k_all, rk, skx, sku, skd), (v_ref, v_all, rv, svx, svu, svd))

    load_ow = pltpu.make_async_copy(ow_hbm, ow, ow_sem)
    load_ow.start()

    barrier = pltpu.get_barrier_semaphore()
    around = [(lax.rem(z + 1, nz) * nx + x, dp), (lax.rem(z + nz - 1, nz) * nx + x, dp)]
    beside = [(z * nx + lax.rem(x + off, nx), dp) for off in range(1, nx)]
    for device in around + beside:
        pl.semaphore_signal(barrier, inc=1, device_id=device, device_id_type=MESH)
    pl.semaphore_wait(barrier, len(around) + len(beside))

    def lanes_of(head):
        return pl.ds(pl.multiple_of(head * HEAD_DIM, HEAD_DIM), HEAD_DIM)

    def hop(src, buf, recv, send, slot, head, device):
        return remote(src, buf.at[slot, head], send, recv.at[slot, head], device)

    def send_own(head):
        for raw, buf, recv, sx, su, sd in both:
            src = raw.at[:, lanes_of(head)]

            @pl.when(has_up)
            def _():
                hop(src, buf, recv, su.at[me, head], me, head, up).start()

            @pl.when(has_down)
            def _():
                hop(src, buf, recv, sd.at[me, head], me, head, down).start()

        for raw, buf, recv, sx, su, sd in both:
            src = raw.at[:, lanes_of(head)]
            for off in range(1, nx):
                hop(src, buf, recv, sx.at[me, head, off], me, head, beside[off - 1]).start()

    def arrived(buf, recv, slot, head):
        block = buf.at[slot, head]
        remote(block, block, recv.at[slot, head], recv.at[slot, head], up).wait_recv()

    def relay(head):
        for dist in range(1, nz):
            for below in (True, False):
                source = z - dist if below else z + dist
                present = source >= 0 if below else source < nz
                further = has_up if below else has_down
                onward = up if below else down

                @pl.when(present)
                def _(source=source, below=below, further=further, onward=onward):
                    slot = source * nx + x
                    for _raw, buf, recv, sx, su, sd in both:
                        arrived(buf, recv, slot, head)
                        src = buf.at[slot, head]
                        send = su if below else sd

                        @pl.when(further)
                        def _(src=src, buf=buf, recv=recv, send=send):
                            hop(src, buf, recv, send.at[slot, head], slot, head, onward).start()

                        for off in range(1, nx):
                            hop(
                                src, buf, recv, sx.at[slot, head, off], slot, head,
                                beside[off - 1],
                            ).start()

    length = nz * nx * tokens
    factor = float(HEAD_DIM**-0.5 * np.log2(np.e))
    span = group * HEAD_DIM

    def attend(kv):
        for plane in range(nz):
            for off in range(1, nx):
                slot = plane * nx + lax.rem(x + off, nx)
                arrived(k_all, rk, slot, kv)
                arrived(v_all, rv, slot, kv)
        k_all[me, kv] = k_ref[:, lanes_of(kv)]
        v_all[me, kv] = v_ref[:, lanes_of(kv)]

        def place(slot, carry):
            rows = pl.ds(pl.multiple_of(slot * tokens, tokens), tokens)
            k_rot[rows, :] = rotate(k_all[slot, kv], kg_ref[...], cos_ref[rows, :], sin_ref[rows, :])
            return carry

        lax.fori_loop(0, nz * nx, place, 0)
        keys = k_rot[...]
        values = v_all[:, kv].reshape(length, HEAD_DIM)
        for member in range(group):
            scores = lax.dot_general(
                q_rot[kv * group + member], keys, (((1,), (1,)), ((), ())),
                preferred_element_type=F32,
            )
            top = jnp.max(scores, axis=-1, keepdims=True)
            raised = jnp.exp2((scores - top) * factor)
            probs = (raised * (1.0 / jnp.sum(raised, axis=-1, keepdims=True))).astype(BF16)
            att[:, member * HEAD_DIM : (member + 1) * HEAD_DIM] = jnp.dot(
                probs, values, preferred_element_type=F32
            ).astype(BF16)
        part = ow.at[pl.ds(pl.multiple_of(kv * span, span), span), :]
        tile = 1024
        for start in range(0, width, tile):
            columns = slice(start, start + tile)
            acc[:, columns] += jnp.dot(att[...], part[:, columns], preferred_element_type=F32)

    send_own(0)
    for head in range(1, min(3, kv_heads)):
        send_own(head)
    own = pl.multiple_of(me * tokens, tokens)
    q_cos = cos_ref[pl.ds(own, tokens), :]
    q_sin = sin_ref[pl.ds(own, tokens), :]
    for head in range(heads):
        q_rot[head] = rotate(
            q_ref[:, head * HEAD_DIM : (head + 1) * HEAD_DIM], qg_ref[...], q_cos, q_sin
        )
    acc[...] = jnp.zeros_like(acc)
    relay(0)
    load_ow.wait()

    def one_head(kv, carry):
        @pl.when(kv + 3 < kv_heads)
        def _():
            send_own(kv + 3)

        @pl.when(kv + 1 < kv_heads)
        def _():
            relay(kv + 1)

        attend(kv)
        return carry

    lax.fori_loop(0, kv_heads, one_head, 0)

    blend = acc[...].astype(BF16).astype(F32)
    blend = blend * lax.rsqrt(jnp.mean(blend * blend, axis=-1, keepdims=True) + EPSILON)
    stream = (res_ref[...].astype(F32) + blend * post_ref[...]).astype(BF16)
    stream_ref[...] = stream
    wide = stream.astype(F32)
    wide = wide * lax.rsqrt(jnp.mean(wide * wide, axis=-1, keepdims=True) + EPSILON)
    normed_ref[...] = (wide * pre_ref[...]).astype(BF16)

    def sent(buf, sem, device):
        block = buf.at[0, 0]
        remote(block, block, sem, sem, device).wait_send()

    def drain(head, carry):
        for _raw, buf, recv, sx, su, sd in both:
            for plane in range(nz):
                slot = plane * nx + x

                @pl.when(jnp.logical_and(has_up, z >= plane))
                def _(slot=slot):
                    sent(buf, su.at[slot, head], up)

                @pl.when(jnp.logical_and(has_down, z <= plane))
                def _(slot=slot):
                    sent(buf, sd.at[slot, head], down)

                for off in range(1, nx):
                    sent(buf, sx.at[slot, head, off], beside[off - 1])
        return carry

    lax.fori_loop(0, kv_heads, drain, 0)


def before(tokens):
    row = lax.broadcasted_iota(jnp.int32, (tokens, tokens), 0)
    col = lax.broadcasted_iota(jnp.int32, (tokens, tokens), 1)
    return (row < col).astype(F32).astype(BF16)


def group_choice(meta, first_expert, count, rows):
    tokens = meta.shape[1]
    low = first_expert.astype(F32)
    member = jnp.where((meta[0:1] >= low) & (meta[0:1] < low + float(count)), 1.0, 0.0)
    rank = jnp.dot(
        jnp.broadcast_to(member, (8, tokens)).astype(BF16),
        before(tokens),
        preferred_element_type=F32,
    )[0:1]
    place = lax.broadcasted_iota(jnp.int32, (rows, tokens), 0).astype(F32)
    return jnp.where(rank == place, 1.0, 0.0) * member


def slot_choice(meta, first_expert, count, cap):
    tokens = meta.shape[1]
    names = lax.broadcasted_iota(jnp.int32, (count, tokens), 0).astype(F32)
    names = names + first_expert.astype(F32)
    first = jnp.where(meta[0:1] == names, 1.0, 0.0)
    second = jnp.where(meta[1:2] == names, 1.0, 0.0)
    rank = jnp.dot((first + second).astype(BF16), before(tokens), preferred_element_type=F32)
    row = lax.broadcasted_iota(jnp.int32, (count * cap, count), 0)
    start = lax.broadcasted_iota(jnp.int32, (count * cap, count), 1) * cap
    widen = jnp.where((row >= start) & (row < start + cap), 1.0, 0.0).astype(BF16)

    def widened(values):
        return jnp.dot(widen, values.astype(BF16), preferred_element_type=F32)

    place = lax.broadcasted_iota(jnp.int32, (count * cap, tokens), 0) & (cap - 1)
    hit = jnp.where(widened(rank) == place.astype(F32), 1.0, 0.0)
    return widened(first) * hit, widened(second) * hit


def contract(left, right, dims):
    return lax.dot_general(
        left.astype(BF16), right.astype(BF16), ((dims[:1], dims[1:]), ((), ())),
        preferred_element_type=F32,
    )


def expert_kernel(
    nz, nx, n_dp,
    normed_ref, stream_ref, meta_ref, wg_hbm, wu_hbm, wd_hbm,
    out_ref,
    wg, wu, wd, w_sem, p1, r1, metas, p2, r2, o2, back, mix, fin,
    s1, t1, sm, tm, s2, t2, s3, t3, s4, t4,
):
    tokens, width = normed_ref.shape
    count, cap = p2.shape[1], p2.shape[2]
    rows = p1.shape[1]
    sp = lax.axis_index("sp")
    dp = lax.axis_index("dp")
    z, x = sp // nx, sp % nx
    me = x * n_dp + dp

    loads = [
        pltpu.make_async_copy(src, dst, w_sem.at[i])
        for i, (src, dst) in enumerate(((wg_hbm, wg), (wu_hbm, wu), (wd_hbm, wd)))
    ]
    for load in loads:
        load.start()

    def plane_peer(off):
        j = lax.rem(me + off, count)
        return j, (z * nx + j // n_dp, j % n_dp)

    def column_peer(dist):
        plane = lax.rem(z + dist, nz)
        return plane, (plane * nx + x, dp)

    barrier = pltpu.get_barrier_semaphore()
    for off in range(1, count):
        pl.semaphore_signal(barrier, inc=1, device_id=plane_peer(off)[1], device_id_type=MESH)
    for dist in range(1, nz):
        pl.semaphore_signal(barrier, inc=1, device_id=column_peer(dist)[1], device_id_type=MESH)

    meta = meta_ref[...]
    for g in range(nz):
        pick = group_choice(meta, jnp.int32(g * count), count, rows)
        p1[g] = contract(pick, normed_ref[...], (1, 0)).astype(BF16)
    metas[z] = meta
    r1[z] = p1[z]

    pl.semaphore_wait(barrier, count - 1 + nz - 1)
    for dist in range(1, nz):
        plane, device = column_peer(dist)
        remote(meta_ref, metas.at[z], sm.at[plane], tm.at[z], device).start()
        remote(p1.at[plane], r1.at[z], s1.at[plane], t1.at[z], device).start()

    first_expert = z * count

    def dispatch(dist, carry):
        source, device = column_peer(dist)

        @pl.when(dist > 0)
        def _():
            remote(meta_ref, metas.at[source], sm.at[source], tm.at[source], device).wait_recv()
            remote(p1.at[source], r1.at[source], s1.at[source], t1.at[source], device).wait_recv()

        got = metas[source]
        group = group_choice(got, first_expert, count, rows)
        first, second = slot_choice(got, first_expert, count, cap)
        pick = contract(first + second, group, (1, 1))
        packed = contract(pick, r1[source], (1, 0)).astype(BF16)
        p2[source] = packed.reshape(count, cap, width)
        r2[source, me] = p2[source, me]
        for off in range(1, count):
            j, device = plane_peer(off)
            remote(
                p2.at[source, j], r2.at[source, me], s2.at[source, j], t2.at[source, me], device
            ).start()
        return carry

    lax.fori_loop(0, nz, dispatch, 0)
    for load in loads:
        load.wait()

    def transform(dist, carry):
        source = lax.rem(z + dist + 1, nz)
        for off in range(1, count):
            j, device = plane_peer(off)
            remote(
                p2.at[source, j], r2.at[source, j], s2.at[source, j], t2.at[source, j], device
            ).wait_recv()
        arrived = r2[source].reshape(count * cap, width)
        gated = jnp.dot(arrived, wg[...], preferred_element_type=F32)
        lifted = jnp.dot(arrived, wu[...], preferred_element_type=F32)
        hidden = (gated / (1.0 + jnp.exp(-gated)) * lifted).astype(BF16)
        result = jnp.dot(hidden, wd[...], preferred_element_type=F32).astype(BF16)
        o2[source] = result.reshape(count, cap, width)
        back[source, me] = o2[source, me]
        for off in range(1, count):
            j, device = plane_peer(off)
            remote(
                o2.at[source, j], back.at[source, me], s3.at[source, j], t3.at[source, me], device
            ).start()
        return carry

    lax.fori_loop(0, nz, transform, 0)

    def combine(dist, carry):
        source, column = column_peer(dist + 1)
        for off in range(1, count):
            j, device = plane_peer(off)
            remote(
                o2.at[source, j], back.at[source, j], s3.at[source, j], t3.at[source, j], device
            ).wait_recv()
        got = metas[source]
        group = group_choice(got, first_expert, count, rows)
        first, second = slot_choice(got, first_expert, count, cap)
        outs = back[source].reshape(count * cap, width)
        one = contract(contract(group, first, (1, 1)), outs, (1, 0))
        two = contract(contract(group, second, (1, 1)), outs, (1, 0))
        weight = jnp.sum(group * got[2:3], axis=1, keepdims=True)
        share = jnp.sum(group * got[3:4], axis=1, keepdims=True)
        total = (weight * (share * one + (1.0 - share) * two)).astype(BF16)
        mix[source] = total

        @pl.when(dist == nz - 1)
        def _():
            fin[source] = total

        @pl.when(dist < nz - 1)
        def _():
            remote(mix.at[source], fin.at[z], s4.at[source], t4.at[z], column).start()

        return carry

    lax.fori_loop(0, nz, combine, 0)

    picks = [
        group_choice(meta, jnp.int32(g * count), count, rows) for g in range(nz)
    ]
    for dist in range(1, nz):
        plane, device = column_peer(dist)
        remote(mix.at[plane], fin.at[plane], s4.at[plane], t4.at[plane], device).wait_recv()
    every = jnp.concatenate(picks, axis=0)
    added = contract(every, fin[...].reshape(tokens, width), (0, 0))
    out_ref[...] = (stream_ref[...].astype(F32) + added).astype(BF16)

    for dist in range(1, nz):
        plane, device = column_peer(dist)
        remote(meta_ref, metas.at[z], sm.at[plane], tm.at[z], device).wait_send()
        remote(p1.at[plane], r1.at[z], s1.at[plane], t1.at[z], device).wait_send()
        remote(mix.at[plane], fin.at[z], s4.at[plane], t4.at[z], device).wait_send()

    def drain(source, carry):
        for off in range(1, count):
            j, device = plane_peer(off)
            remote(
                p2.at[source, j], r2.at[source, me], s2.at[source, j], t2.at[source, me], device
            ).wait_send()
            remote(
                o2.at[source, j], back.at[source, me], s3.at[source, j], t3.at[source, me], device
            ).wait_send()
        return carry

    lax.fori_loop(0, nz, drain, 0)


def local(
    residual_in, query_proj, key_proj, value_proj, query_gain, key_gain, out_weight, post_gain,
    pre_gain, route_ids, group_weight, first_share, gate_weight, up_weight, down_weight,
):
    n_sp = lax.axis_size("sp")
    n_dp = lax.axis_size("dp")
    tokens, width = query_proj.shape[1:]
    kv_width = key_proj.shape[2]
    heads, kv_heads = width // HEAD_DIM, kv_width // HEAD_DIM
    nz = GROUPS
    nx = n_sp // nz
    length = n_sp * tokens
    cos, sin = angle_tables(length)
    vmem = pl.BlockSpec(memory_space=pltpu.VMEM)
    hbm = pl.BlockSpec(memory_space=pl.ANY)
    dma = pltpu.SemaphoreType.DMA
    row = jax.ShapeDtypeStruct((tokens, width), BF16)
    stream, normed = pl.pallas_call(
        functools.partial(attention_kernel, nz, nx),
        out_shape=(row, row),
        in_specs=[vmem] * 10 + [hbm],
        out_specs=(vmem, vmem),
        scratch_shapes=[
            pltpu.VMEM((n_sp, kv_heads, tokens, HEAD_DIM), BF16),
            pltpu.VMEM((n_sp, kv_heads, tokens, HEAD_DIM), BF16),
            pltpu.VMEM((heads, tokens, HEAD_DIM), BF16),
            pltpu.VMEM((length, HEAD_DIM), BF16),
            pltpu.VMEM((tokens, width // kv_heads), BF16),
            pltpu.VMEM((tokens, width), F32),
            pltpu.VMEM((width, width), BF16),
            dma,
            dma((n_sp, kv_heads)), dma((n_sp, kv_heads)),
            dma((n_sp, kv_heads, nx)), dma((n_sp, kv_heads)), dma((n_sp, kv_heads)),
            dma((n_sp, kv_heads, nx)), dma((n_sp, kv_heads)), dma((n_sp, kv_heads)),
        ],
        compiler_params=pltpu.CompilerParams(
            collective_id=0, has_side_effects=True, vmem_limit_bytes=VMEM_LIMIT
        ),
        name="attention",
    )(
        query_proj[0], key_proj[0], value_proj[0],
        query_gain.reshape(1, -1), key_gain.reshape(1, -1),
        jnp.asarray(cos), jnp.asarray(sin),
        residual_in[0], post_gain.reshape(1, -1), pre_gain.reshape(1, -1), out_weight,
    )

    experts = gate_weight.shape[0] * n_sp * n_dp
    count = experts // nz
    cap = max(16, 4 * tokens // experts)
    rows = tokens // nz
    ff = gate_weight.shape[2]
    meta = jnp.concatenate(
        [route_ids[0].T.astype(F32), group_weight, first_share, jnp.zeros((4, tokens), F32)], axis=0
    )
    blocks = pltpu.VMEM((nz, count, cap, width), BF16)
    lines = pltpu.VMEM((nz, rows, width), BF16)
    out = pl.pallas_call(
        functools.partial(expert_kernel, nz, nx, n_dp),
        out_shape=row,
        in_specs=[vmem] * 3 + [hbm] * 3,
        out_specs=vmem,
        scratch_shapes=[
            pltpu.VMEM((width, ff), BF16),
            pltpu.VMEM((width, ff), BF16),
            pltpu.VMEM((ff, width), BF16),
            dma((3,)),
            lines, lines,
            pltpu.VMEM((nz, 8, tokens), F32),
            blocks, blocks, blocks, blocks,
            lines, lines,
            dma((nz,)), dma((nz,)), dma((nz,)), dma((nz,)),
            dma((nz, count)), dma((nz, count)), dma((nz, count)), dma((nz, count)),
            dma((nz,)), dma((nz,)),
        ],
        compiler_params=pltpu.CompilerParams(
            collective_id=1, has_side_effects=True, vmem_limit_bytes=VMEM_LIMIT
        ),
        name="experts",
    )(normed, stream, meta, gate_weight[0], up_weight[0], down_weight[0])
    return out.reshape(1, tokens, width)


def layer_kernel(
    nz, nx, cores,
    q_ref, k_ref, v_ref, qg_ref, kg_ref, res_ref, post_ref, pre_ref, route_ref, gw_ref, fs_ref,
    cos_hbm, sin_hbm, ow_hbm, wg_hbm, wu_hbm, wd_hbm,
    out_ref,
    kv, q_rot, att, acc, cos, sin, ow, wg, wu, wd, load_sem,
    rk, sx, su, sd,
    perm, perm_back, mrow, metas, picks, weights, backs,
    zs_sem, zr_sem, ms_sem, mr_sem,
    stream, srt, rows, y, other, part, relay, direct, summed, fin,
    s1, t1, sxd, tx, syd, ty, sc, tc, so, to, sr, tr, sf, tf, s4, t4,
):
    tokens, width = q_ref.shape
    heads = width // HEAD_DIM
    kv_heads = k_ref.shape[1] // HEAD_DIM
    group = heads // kv_heads
    length = nz * nx * tokens
    chips = metas.shape[2]
    count = chips * cores
    block = tokens // nz
    cap = y.shape[2] // chips
    half = block // 2
    me = lax.axis_index("sp")
    dp = lax.axis_index("dp")
    z, x = me // nx, me % nx
    side, core = dp // cores, dp % cores
    up, down = (me + nx, dp), (me - nx, dp)
    beside = (z * nx + 1 - x, dp)
    across = (me, (1 - side) * cores + core)
    partner = (me, side * cores + 1 - core)
    has_up, has_down = z < nz - 1, z > 0
    mine = side * nx + x
    chip_x, chip_y = side * nx + 1 - x, (1 - side) * nx + x
    chip_d = (1 - side) * nx + 1 - x

    def column(plane):
        return (plane * nx + x, dp)

    flip = z >= nz // 2
    low = jnp.where(flip, nz - 1 - z, z)

    def source_of(i):
        if i == 0:
            return z
        near = (i - 1) + jnp.where(low <= i - 1, 1, 0)
        return jnp.where(flip, nz - 1 - near, near)

    sources = [source_of(i) for i in range(nz)]

    own = pl.multiple_of(me * tokens, tokens)
    loads = [
        pltpu.make_async_copy(src, dst, load_sem.at[i])
        for i, (src, dst) in enumerate((
            (cos_hbm.at[pl.ds(own, tokens)], cos), (sin_hbm.at[pl.ds(own, tokens)], sin),
            (ow_hbm, ow), (wg_hbm, wg), (wu_hbm, wu), (wd_hbm, wd),
        ))
    ]
    for load in loads:
        load.start()

    barrier = pltpu.get_barrier_semaphore()
    greeted = [column(lax.rem(z + dist, nz)) for dist in range(1, nz)] + [beside, across, partner]
    for device in greeted:
        pl.semaphore_signal(barrier, inc=1, device_id=device, device_id_type=MESH)

    loads[0].wait()
    loads[1].wait()
    for head in range(kv_heads):
        columns = slice(head * HEAD_DIM, (head + 1) * HEAD_DIM)
        kv[me, head, 1] = v_ref[:, columns]
        kv[me, head, 0] = rotate(k_ref[:, columns], kg_ref[...], cos[...], sin[...])

    pl.semaphore_wait(barrier, len(greeted))

    def hop(slot, head, send, device):
        buf = kv.at[slot, head]
        return remote(buf, buf, send.at[slot, head], rk.at[slot, head], device)

    def arrived(slot, head):
        hop(slot, head, sx, up).wait_recv()

    def crossing(head):
        return lax.rem(head, 2) == 1

    for head in range(kv_heads):
        hop(me, head, sx, beside).start()

        @pl.when(has_up)
        def _(head=head):
            hop(me, head, su, up).start()

        @pl.when(has_down)
        def _(head=head):
            hop(me, head, sd, down).start()

    def relay_kv(head):
        slot_x = z * nx + 1 - x
        arrived(slot_x, head)

        @pl.when(jnp.logical_and(crossing(head), has_up))
        def _():
            hop(slot_x, head, su, up).start()

        @pl.when(jnp.logical_and(crossing(head), has_down))
        def _():
            hop(slot_x, head, sd, down).start()

        for dist in range(1, nz):
            for below in (True, False):
                source = z - dist if below else z + dist
                present = source >= 0 if below else source < nz
                further = has_up if below else has_down
                onward, send = (up, su) if below else (down, sd)

                @pl.when(present)
                def _(source=source, further=further, onward=onward, send=send, dist=dist):
                    slot = source * nx + x
                    arrived(slot, head)

                    @pl.when(further)
                    def _():
                        hop(slot, head, send, onward).start()

                    if dist == 1:
                        @pl.when(jnp.logical_not(crossing(head)))
                        def _():
                            hop(slot, head, sx, beside).start()
                    else:
                        hop(slot, head, sx, beside).start()

    for head in range(heads):
        q_rot[head] = rotate(
            q_ref[:, head * HEAD_DIM : (head + 1) * HEAD_DIM], qg_ref[...], cos[...], sin[...]
        )
    acc[...] = jnp.zeros_like(acc)

    row = lax.broadcasted_iota(jnp.int32, (tokens, tokens), 0)
    lane = lax.broadcasted_iota(jnp.int32, (tokens, tokens), 1)

    def to_lanes(column_of):
        return jnp.sum(jnp.where(row == lane, column_of, 0.0), axis=0, keepdims=True)

    def routing():
        first = route_ref[:, 0:1].astype(F32)
        second = route_ref[:, 1:2].astype(F32)
        of = jnp.zeros_like(first)
        for g in range(1, nz):
            of = of + jnp.where(first >= float(g * count), 1.0, 0.0)
        of_lane = to_lanes(of)
        same = of == of_lane
        rank = jnp.sum(jnp.where(same & (lane < row), 1.0, 0.0), axis=1, keepdims=True)
        rank_lane = jnp.sum(jnp.where(same & (row < lane), 1.0, 0.0), axis=0, keepdims=True)
        place = (of * float(block) + rank).astype(jnp.int32)
        place_lane = (of_lane * float(block) + rank_lane).astype(jnp.int32)
        perm[...] = jnp.where(row == place_lane, 1.0, 0.0).astype(BF16)
        perm_back[...] = jnp.where(place == lane, 1.0, 0.0).astype(BF16)
        fields = (
            to_lanes(first), to_lanes(second),
            gw_ref[...] * fs_ref[...], gw_ref[...] * (1.0 - fs_ref[...]),
        )
        chosen = lax.broadcasted_iota(jnp.int32, (8, tokens), 0).astype(F32) == of_lane
        at = rank.astype(jnp.int32)
        table = jnp.zeros((8, tokens), F32)
        for f, field in enumerate(fields):
            spread = jnp.where(lane == at + f * block, 1.0, 0.0)
            table += lax.dot_general(
                jnp.where(chosen, field, 0.0), spread, (((1,), (0,)), ((), ())),
                precision=lax.Precision.HIGHEST, preferred_element_type=F32,
            )
        for g in range(nz):
            mrow[g] = table[g : g + 1]

    routing()
    metas[z, core, mine] = mrow[z]

    def meta_column(dist):
        plane = lax.rem(z + dist, nz)
        return plane, remote(
            mrow.at[plane], metas.at[z, core, mine], zs_sem.at[plane], zr_sem.at[z], column(plane)
        )

    def meta_arrival(dist):
        plane = lax.rem(z + dist, nz)
        return remote(
            mrow.at[plane], metas.at[plane, core, mine], zs_sem.at[plane], zr_sem.at[plane],
            column(plane),
        )

    for dist in range(1, nz):
        meta_column(dist)[1].start()

    def meta_copy(view, step, device):
        return remote(view, view, ms_sem.at[step], mr_sem.at[step], device)

    pair = pl.ds(side * nx, nx)
    other_pair = pl.ds((1 - side) * nx, nx)
    meta_sends = (
        meta_copy(metas.at[:, core, mine], 0, beside),
        meta_copy(metas.at[:, core, pair], 1, across),
        meta_copy(metas.at[:, core], 2, partner),
    )
    meta_recvs = (
        meta_copy(metas.at[:, core, chip_x], 0, beside),
        meta_copy(metas.at[:, core, other_pair], 1, across),
        meta_copy(metas.at[:, 1 - core], 2, partner),
    )

    def choice(plane, of_core, expert):
        table = metas[plane, of_core].reshape(chips, tokens)
        first = table[:, 0:block] == expert
        second = table[:, block : 2 * block] == expert
        member = jnp.where(first | second, 1.0, 0.0)
        weight = jnp.where(first, table[:, 2 * block : 3 * block], 0.0)
        weight = weight + jnp.where(second, table[:, 3 * block : 4 * block], 0.0)
        r = lax.broadcasted_iota(jnp.int32, (block, block), 0)
        c = lax.broadcasted_iota(jnp.int32, (block, block), 1)
        earlier = jnp.where(r < c, 1.0, 0.0).astype(BF16)
        rank = jnp.dot(
            jnp.concatenate([member] * (8 // chips), axis=0).astype(BF16), earlier,
            preferred_element_type=F32,
        )[:chips]
        place = lax.broadcasted_iota(jnp.int32, (chips, cap, block), 1).astype(F32)
        hit = jnp.where(rank[:, None, :] == place, 1.0, 0.0) * member[:, None, :]
        of_slot = jnp.sum(hit * weight[:, None, :], axis=2, keepdims=True).reshape(chips * cap, 1)
        flat = hit.reshape(chips * cap, block).astype(BF16)
        wide_row = lax.broadcasted_iota(jnp.int32, (block, tokens), 0)
        wide_lane = lax.broadcasted_iota(jnp.int32, (block, tokens), 1)
        widen = jnp.where(lax.rem(wide_lane, block) == wide_row, 1.0, 0.0).astype(BF16)
        spread = jnp.dot(flat, widen, preferred_element_type=F32)
        slot = lax.broadcasted_iota(jnp.int32, (chips * cap, tokens), 0) // cap
        chip = lax.broadcasted_iota(jnp.int32, (chips * cap, tokens), 1) // block
        return jnp.where(slot == chip, spread, 0.0), of_slot

    def tables():
        expert = (z * count + x * (count // nx) + dp).astype(F32)
        twin = (z * count + x * (count // nx) + side * cores + 1 - core).astype(F32)

        def one_plane(plane, carry):
            for of_core in range(cores):
                pick, of_slot = choice(plane, of_core, expert)
                picks[plane, of_core] = pick.astype(BF16)
                weights[plane, of_core] = of_slot
            back, _ = choice(plane, core, expert)
            theirs, _ = choice(plane, core, twin)
            backs[plane] = jnp.concatenate([back, theirs], axis=0).T.astype(BF16)
            return carry

        lax.fori_loop(0, nz, one_plane, 0)

    factor = float(HEAD_DIM**-0.5 * np.log2(np.e))
    span = group * HEAD_DIM

    def attend(head):
        keys = kv[:, head, 0].reshape(length, HEAD_DIM)
        values = kv[:, head, 1].reshape(length, HEAD_DIM)
        for member in range(group):
            scores = lax.dot_general(
                q_rot[head * group + member], keys, (((1,), (1,)), ((), ())),
                preferred_element_type=F32,
            )
            top = jnp.max(scores, axis=-1, keepdims=True)
            raised = jnp.exp2((scores - top) * factor)
            total = jnp.sum(raised, axis=-1, keepdims=True)
            mixed = jnp.dot(raised.astype(BF16), values, preferred_element_type=F32)
            att[:, member * HEAD_DIM : (member + 1) * HEAD_DIM] = (mixed / total).astype(BF16)
        above = ow.at[pl.ds(pl.multiple_of(head * span, span), span), :]
        tile = 1024
        for start in range(0, width, tile):
            columns = slice(start, start + tile)
            acc[:, columns] += jnp.dot(att[...], above[:, columns], preferred_element_type=F32)

    relay_kv(0)
    loads[2].wait()

    def one_head(head, carry):
        @pl.when(head + 1 < kv_heads)
        def _():
            relay_kv(head + 1)

        @pl.when(head == 0)
        def _():
            for dist in range(1, nz):
                meta_arrival(dist).wait_recv()
            meta_sends[0].start()

        @pl.when(head == 1)
        def _():
            meta_recvs[0].wait_recv()
            meta_sends[1].start()

        @pl.when(head == 2)
        def _():
            meta_recvs[1].wait_recv()
            meta_sends[2].start()

        @pl.when(head == kv_heads - 1)
        def _():
            meta_recvs[2].wait_recv()
            tables()

        slot_x = 1 - x
        for dist in range(1, nz):
            arrived(lax.rem(z + dist, nz) * nx + slot_x, head)
        attend(head)
        return carry

    lax.fori_loop(0, kv_heads, one_head, 0)

    blend = acc[...].astype(BF16).astype(F32)
    blend = blend * lax.rsqrt(jnp.mean(blend * blend, axis=-1, keepdims=True) + EPSILON)
    flow = (res_ref[...].astype(F32) + blend * post_ref[...]).astype(BF16)
    stream[...] = flow
    wide = flow.astype(F32)
    wide = wide * lax.rsqrt(jnp.mean(wide * wide, axis=-1, keepdims=True) + EPSILON)
    normed = (wide * pre_ref[...]).astype(BF16)
    srt[...] = jnp.dot(perm[...], normed, preferred_element_type=F32).astype(BF16).reshape(srt.shape)

    def z_send(plane):
        return remote(
            srt.at[plane], rows.at[z, core, mine], s1.at[plane], t1.at[z], column(plane)
        )

    def z_recv(plane):
        return remote(
            srt.at[plane], rows.at[plane, core, mine], s1.at[plane], t1.at[plane], column(plane)
        )

    for i in range(1, nz):
        z_send(sources[i]).start()
    rows[z, core, mine] = srt[z]

    halves = (pl.ds(0, half), pl.ds(half, half))

    def over_x(s, chip, h):
        view = rows.at[s, core, chip, halves[h]]
        return remote(view, view, sxd.at[s, chip, h], tx.at[s, chip, h], beside)

    def over_y(s, chip, h):
        view = rows.at[s, core, chip, halves[h]]
        return remote(view, view, syd.at[s, chip, h], ty.at[s, chip, h], across)

    def over_core(s, of_core, chip):
        view = rows.at[s, of_core, chip]
        return remote(view, view, sc.at[s, chip], tc.at[s, chip], partner)

    def spread_own(i):
        s = sources[i]
        if i > 0:
            z_recv(s).wait_recv()
        over_x(s, mine, 0).start()
        over_y(s, mine, 1).start()
        over_x(s, mine, 1).start()
        over_y(s, mine, 0).start()
        over_core(s, core, mine).start()

    def spread_on(i):
        s = sources[i]
        over_x(s, chip_x, 0).wait_recv()
        over_y(s, chip_x, 0).start()
        over_y(s, chip_y, 1).wait_recv()
        over_x(s, chip_y, 1).start()
        over_x(s, chip_x, 1).wait_recv()
        over_core(s, core, chip_x).start()
        over_y(s, chip_y, 0).wait_recv()
        over_core(s, core, chip_y).start()

    def spread_last(i):
        s = sources[i]
        over_y(s, chip_d, 0).wait_recv()
        over_x(s, chip_d, 1).wait_recv()
        over_core(s, core, chip_d).start()

    def to_partner(s):
        return remote(y.at[s, 1 - core], other.at[s], so.at[s], to.at[s], partner)

    def transform(i):
        s = sources[i]
        for k in range(chips):
            over_core(s, 1 - core, k).wait_recv()
        packed = [
            jnp.dot(
                picks[s, q], rows[s, q].reshape(tokens, width), preferred_element_type=F32
            ).astype(BF16)
            for q in range(cores)
        ]
        packed = jnp.concatenate(packed, axis=0)
        gated = jnp.dot(packed, wg[...], preferred_element_type=F32)
        lifted = jnp.dot(packed, wu[...], preferred_element_type=F32)
        hidden = (gated / (1.0 + jnp.exp(-gated)) * lifted).astype(BF16)
        result = jnp.dot(hidden, wd[...], preferred_element_type=F32)
        slots = chips * cap
        for q in range(cores):
            y[s, q] = (result[q * slots : (q + 1) * slots] * weights[s, q]).astype(BF16)
        to_partner(s).start()

    def to_relay_y(s):
        return remote(part.at[s, chip_d, halves[0]], relay.at[s, 0], sr.at[s, 0], tr.at[s, 0], across)

    def to_relay_x(s):
        return remote(part.at[s, chip_d, halves[1]], relay.at[s, 1], sr.at[s, 1], tr.at[s, 1], beside)

    def direct_x(s):
        return remote(part.at[s, chip_x, halves[1]], direct.at[s, 1], sr.at[s, 2], tr.at[s, 2], beside)

    def direct_y(s):
        return remote(part.at[s, chip_y, halves[0]], direct.at[s, 0], sr.at[s, 3], tr.at[s, 3], across)

    def summed_x(s):
        return remote(part.at[s, chip_x, halves[0]], summed.at[s, 0], sf.at[s, 0], tf.at[s, 0], beside)

    def summed_y(s):
        return remote(part.at[s, chip_y, halves[1]], summed.at[s, 1], sf.at[s, 1], tf.at[s, 1], across)

    def gather_back(i):
        s = sources[i]
        to_partner(s).wait_recv()
        outs = jnp.concatenate([y[s, core], other[s]], axis=0)
        part[s] = jnp.dot(backs[s], outs, preferred_element_type=F32).astype(BF16).reshape(
            chips, block, width
        )
        to_relay_y(s).start()
        to_relay_x(s).start()
        direct_x(s).start()
        direct_y(s).start()

    def add(left, right):
        return (left.astype(F32) + right.astype(F32)).astype(BF16)

    def pass_back(i):
        s = sources[i]
        to_relay_y(s).wait_recv()
        part[s, chip_x, halves[0]] = add(part[s, chip_x, halves[0]], relay[s, 0])
        summed_x(s).start()
        to_relay_x(s).wait_recv()
        part[s, chip_y, halves[1]] = add(part[s, chip_y, halves[1]], relay[s, 1])
        summed_y(s).start()

    def home(s):
        return remote(part.at[s, mine], fin.at[z], s4.at[s], t4.at[z], column(s))

    def finish(i):
        s = sources[i]
        direct_y(s).wait_recv()
        summed_x(s).wait_recv()
        direct_x(s).wait_recv()
        summed_y(s).wait_recv()
        for h in range(2):
            total = part[s, mine, halves[h]].astype(F32) + direct[s, h].astype(F32)
            total = (total + summed[s, h].astype(F32)).astype(BF16)
            if i > 0:
                part[s, mine, halves[h]] = total
            else:
                fin[s, halves[h]] = total
        if i > 0:
            home(s).start()

    def weights_ready(i):
        for load in loads[3:]:
            load.wait()

    for stage, i in plan(
        spread_own, spread_on, spread_last, weights_ready, transform, gather_back, pass_back, finish
    ):
        stage(i)

    for i in range(1, nz):
        s = sources[i]
        remote(part.at[s, mine], fin.at[s], s4.at[s], t4.at[s], column(s)).wait_recv()
    added = jnp.dot(
        perm_back[...], fin[...].reshape(tokens, width), preferred_element_type=F32
    )
    out_ref[...] = (stream[...].astype(F32) + added).astype(BF16)

    def drain_kv(head, carry):
        for plane in range(nz):
            slot = plane * nx + x

            @pl.when(jnp.logical_and(has_up, z >= plane))
            def _(slot=slot):
                hop(slot, head, su, up).wait_send()

            @pl.when(jnp.logical_and(has_down, z <= plane))
            def _(slot=slot):
                hop(slot, head, sd, down).wait_send()

            adjacent = jnp.logical_or(z == plane + 1, z == plane - 1)

            @pl.when(jnp.logical_not(jnp.logical_and(adjacent, crossing(head))))
            def _(slot=slot):
                hop(slot, head, sx, beside).wait_send()

        slot_x = z * nx + 1 - x

        @pl.when(jnp.logical_and(crossing(head), has_up))
        def _():
            hop(slot_x, head, su, up).wait_send()

        @pl.when(jnp.logical_and(crossing(head), has_down))
        def _():
            hop(slot_x, head, sd, down).wait_send()

        return carry

    lax.fori_loop(0, kv_heads, drain_kv, 0)
    for dist in range(1, nz):
        meta_column(dist)[1].wait_send()
    for send in meta_sends:
        send.wait_send()

    def drain(s, carry):
        for h in range(2):
            over_x(s, mine, h).wait_send()
            over_y(s, mine, h).wait_send()
        over_y(s, chip_x, 0).wait_send()
        over_x(s, chip_y, 1).wait_send()
        for k in range(chips):
            over_core(s, core, k).wait_send()
        to_partner(s).wait_send()
        for copy in (to_relay_y, to_relay_x, direct_x, direct_y, summed_x, summed_y):
            copy(s).wait_send()
        return carry

    lax.fori_loop(0, nz, drain, 0)
    for i in range(1, nz):
        z_send(sources[i]).wait_send()
        home(sources[i]).wait_send()


def plan(own, on, last, ready, transform, gather_back, pass_back, finish):
    return (
        (own, 0), (on, 0), (own, 1), (last, 0), (on, 1), (own, 2), (ready, 0),
        (transform, 0), (last, 1), (on, 2), (own, 3),
        (transform, 1), (last, 2), (on, 3), (gather_back, 1),
        (transform, 2), (last, 3), (gather_back, 2), (pass_back, 1),
        (transform, 3), (gather_back, 0), (finish, 1), (pass_back, 2), (gather_back, 3),
        (finish, 2), (pass_back, 3), (pass_back, 0), (finish, 3), (finish, 0),
    )


def fused(
    residual_in, query_proj, key_proj, value_proj, query_gain, key_gain, out_weight, post_gain,
    pre_gain, route_ids, group_weight, first_share, gate_weight, up_weight, down_weight,
):
    n_sp = lax.axis_size("sp")
    n_dp = lax.axis_size("dp")
    tokens, width = query_proj.shape[1:]
    kv_heads = key_proj.shape[2] // HEAD_DIM
    heads = width // HEAD_DIM
    nz = GROUPS
    nx = n_sp // nz
    cores = 2
    chips = nx * (n_dp // cores)
    experts = gate_weight.shape[0] * n_sp * n_dp
    cap = max(16, 4 * tokens // experts)
    block = tokens // nz
    slots = chips * cap
    ff = gate_weight.shape[2]
    length = n_sp * tokens
    cos, sin = angle_tables(length)
    vmem = pl.BlockSpec(memory_space=pltpu.VMEM)
    hbm = pl.BlockSpec(memory_space=pl.ANY)
    dma = pltpu.SemaphoreType.DMA

    def buf(*shape, kind=BF16):
        return pltpu.VMEM(shape, kind)

    out = pl.pallas_call(
        functools.partial(layer_kernel, nz, nx, cores),
        out_shape=jax.ShapeDtypeStruct((tokens, width), BF16),
        in_specs=[vmem] * 11 + [hbm] * 6,
        out_specs=vmem,
        scratch_shapes=[
            buf(n_sp, kv_heads, 2, tokens, HEAD_DIM),
            buf(heads, tokens, HEAD_DIM),
            buf(tokens, width // kv_heads),
            buf(tokens, width, kind=F32),
            buf(tokens, HEAD_DIM, kind=F32), buf(tokens, HEAD_DIM, kind=F32),
            buf(width, width), buf(width, ff), buf(width, ff), buf(ff, width),
            dma((6,)),
            dma((n_sp, kv_heads)), dma((n_sp, kv_heads)), dma((n_sp, kv_heads)),
            dma((n_sp, kv_heads)),
            buf(tokens, tokens), buf(tokens, tokens),
            buf(nz, 1, tokens, kind=F32), buf(nz, cores, chips, 1, tokens, kind=F32),
            buf(nz, cores, slots, tokens), buf(nz, cores, slots, 1, kind=F32),
            buf(nz, tokens, cores * slots),
            dma((nz,)), dma((nz,)), dma((3,)), dma((3,)),
            buf(tokens, width), buf(nz, block, width), buf(nz, cores, chips, block, width),
            buf(nz, cores, slots, width), buf(nz, slots, width),
            buf(nz, chips, block, width),
            buf(nz, 2, block // 2, width), buf(nz, 2, block // 2, width),
            buf(nz, 2, block // 2, width), buf(nz, block, width),
            dma((nz,)), dma((nz,)),
            dma((nz, chips, 2)), dma((nz, chips, 2)), dma((nz, chips, 2)), dma((nz, chips, 2)),
            dma((nz, chips)), dma((nz, chips)),
            dma((nz,)), dma((nz,)),
            dma((nz, 4)), dma((nz, 4)), dma((nz, 2)), dma((nz, 2)),
            dma((nz,)), dma((nz,)),
        ],
        compiler_params=pltpu.CompilerParams(
            collective_id=0, has_side_effects=True, vmem_limit_bytes=VMEM_LIMIT
        ),
        name="layer",
    )(
        query_proj[0], key_proj[0], value_proj[0],
        query_gain.reshape(1, -1), key_gain.reshape(1, -1),
        residual_in[0], post_gain.reshape(1, -1), pre_gain.reshape(1, -1),
        route_ids[0], group_weight, first_share,
        jnp.asarray(cos), jnp.asarray(sin), out_weight,
        gate_weight[0], up_weight[0], down_weight[0],
    )
    return out.reshape(1, tokens, width)


def solution(mesh):
    tok3 = P("dp", "sp", None)
    tok2 = P("dp", "sp")
    weight = P(("sp", "dp"), None, None)
    placed = (
        tok3, tok3, tok3, tok3, P(), P(), P(), P(), P(), tok3, tok2, tok2, weight, weight, weight,
    )
    small = mesh.shape["sp"] == 2 * GROUPS and mesh.shape["dp"] == 4
    return jax.shard_map(
        fused if small else local, mesh=mesh, in_specs=placed, out_specs=P("dp", "sp", None), check_vma=False
    )
```

```python
import functools

import jax
import jax.numpy as jnp
import numpy as np
from jax import lax
from jax.experimental import pallas as pl
from jax.experimental.pallas import tpu as pltpu
from jax.sharding import PartitionSpec as P

HEAD_DIM = 128
GRID_W = 64
GROUPS = 4
EPSILON = 1e-06
MESH = pl.DeviceIdType.MESH
VMEM_LIMIT = 60 * 1024 * 1024
F32 = jnp.float32
BF16 = jnp.bfloat16


def angle_tables(length):
    quarter = HEAD_DIM // 4
    inverse = 10000.0 ** (-np.arange(quarter, dtype=np.float64) / quarter)
    positions = np.arange(length)
    rows = (positions // GRID_W)[:, None] * inverse
    cols = (positions % GRID_W)[:, None] * inverse
    angles = np.concatenate([rows, rows, cols, cols], axis=-1)
    sign = np.where(np.arange(HEAD_DIM) % (2 * quarter) < quarter, -1.0, 1.0)
    return np.cos(angles).astype(np.float32), (np.sin(angles) * sign).astype(np.float32)


def rotate(raw, gain, cos, sin):
    floats = raw.astype(F32)
    normed = floats * lax.rsqrt(jnp.mean(floats * floats, axis=-1, keepdims=True) + EPSILON) * gain
    quarter = HEAD_DIM // 4
    lane = lax.broadcasted_iota(jnp.int32, normed.shape, 1)
    turned = jnp.where(
        (lane & (2 * quarter - 1)) < quarter,
        pltpu.roll(normed, HEAD_DIM - quarter, 1),
        pltpu.roll(normed, quarter, 1),
    )
    return (normed * cos + turned * sin).astype(BF16)


def remote(src, dst, send_sem, recv_sem, device):
    return pltpu.make_async_remote_copy(
        src_ref=src,
        dst_ref=dst,
        send_sem=send_sem,
        recv_sem=recv_sem,
        device_id=device,
        device_id_type=MESH,
    )


def attention_kernel(
    nz, nx,
    q_ref, k_ref, v_ref, qg_ref, kg_ref, cos_ref, sin_ref, res_ref, post_ref, pre_ref, ow_hbm,
    stream_ref, normed_ref,
    k_all, v_all, q_rot, k_rot, att, acc, ow, ow_sem,
    rk, rv, skx, sku, skd, svx, svu, svd,
):
    tokens, width = q_ref.shape
    heads = width // HEAD_DIM
    kv_heads = k_ref.shape[1] // HEAD_DIM
    group = heads // kv_heads
    me = lax.axis_index("sp")
    dp = lax.axis_index("dp")
    z, x = me // nx, me % nx
    up, down = (me + nx, dp), (me - nx, dp)
    has_up, has_down = z < nz - 1, z > 0
    both = ((k_ref, k_all, rk, skx, sku, skd), (v_ref, v_all, rv, svx, svu, svd))

    load_ow = pltpu.make_async_copy(ow_hbm, ow, ow_sem)
    load_ow.start()

    barrier = pltpu.get_barrier_semaphore()
    around = [(lax.rem(z + 1, nz) * nx + x, dp), (lax.rem(z + nz - 1, nz) * nx + x, dp)]
    beside = [(z * nx + lax.rem(x + off, nx), dp) for off in range(1, nx)]
    for device in around + beside:
        pl.semaphore_signal(barrier, inc=1, device_id=device, device_id_type=MESH)
    pl.semaphore_wait(barrier, len(around) + len(beside))

    def lanes_of(head):
        return pl.ds(pl.multiple_of(head * HEAD_DIM, HEAD_DIM), HEAD_DIM)

    def hop(src, buf, recv, send, slot, head, device):
        return remote(src, buf.at[slot, head], send, recv.at[slot, head], device)

    def send_own(head):
        for raw, buf, recv, sx, su, sd in both:
            src = raw.at[:, lanes_of(head)]

            @pl.when(has_up)
            def _():
                hop(src, buf, recv, su.at[me, head], me, head, up).start()

            @pl.when(has_down)
            def _():
                hop(src, buf, recv, sd.at[me, head], me, head, down).start()

        for raw, buf, recv, sx, su, sd in both:
            src = raw.at[:, lanes_of(head)]
            for off in range(1, nx):
                hop(src, buf, recv, sx.at[me, head, off], me, head, beside[off - 1]).start()

    def arrived(buf, recv, slot, head):
        block = buf.at[slot, head]
        remote(block, block, recv.at[slot, head], recv.at[slot, head], up).wait_recv()

    def relay(head):
        for dist in range(1, nz):
            for below in (True, False):
                source = z - dist if below else z + dist
                present = source >= 0 if below else source < nz
                further = has_up if below else has_down
                onward = up if below else down

                @pl.when(present)
                def _(source=source, below=below, further=further, onward=onward):
                    slot = source * nx + x
                    for _raw, buf, recv, sx, su, sd in both:
                        arrived(buf, recv, slot, head)
                        src = buf.at[slot, head]
                        send = su if below else sd

                        @pl.when(further)
                        def _(src=src, buf=buf, recv=recv, send=send):
                            hop(src, buf, recv, send.at[slot, head], slot, head, onward).start()

                        for off in range(1, nx):
                            hop(
                                src, buf, recv, sx.at[slot, head, off], slot, head,
                                beside[off - 1],
                            ).start()

    length = nz * nx * tokens
    factor = float(HEAD_DIM**-0.5 * np.log2(np.e))
    span = group * HEAD_DIM

    def attend(kv):
        for plane in range(nz):
            for off in range(1, nx):
                slot = plane * nx + lax.rem(x + off, nx)
                arrived(k_all, rk, slot, kv)
                arrived(v_all, rv, slot, kv)
        k_all[me, kv] = k_ref[:, lanes_of(kv)]
        v_all[me, kv] = v_ref[:, lanes_of(kv)]

        def place(slot, carry):
            rows = pl.ds(pl.multiple_of(slot * tokens, tokens), tokens)
            k_rot[rows, :] = rotate(k_all[slot, kv], kg_ref[...], cos_ref[rows, :], sin_ref[rows, :])
            return carry

        lax.fori_loop(0, nz * nx, place, 0)
        keys = k_rot[...]
        values = v_all[:, kv].reshape(length, HEAD_DIM)
        for member in range(group):
            scores = lax.dot_general(
                q_rot[kv * group + member], keys, (((1,), (1,)), ((), ())),
                preferred_element_type=F32,
            )
            top = jnp.max(scores, axis=-1, keepdims=True)
            raised = jnp.exp2((scores - top) * factor)
            probs = (raised * (1.0 / jnp.sum(raised, axis=-1, keepdims=True))).astype(BF16)
            att[:, member * HEAD_DIM : (member + 1) * HEAD_DIM] = jnp.dot(
                probs, values, preferred_element_type=F32
            ).astype(BF16)
        part = ow.at[pl.ds(pl.multiple_of(kv * span, span), span), :]
        tile = 1024
        for start in range(0, width, tile):
            columns = slice(start, start + tile)
            acc[:, columns] += jnp.dot(att[...], part[:, columns], preferred_element_type=F32)

    send_own(0)
    for head in range(1, min(3, kv_heads)):
        send_own(head)
    own = pl.multiple_of(me * tokens, tokens)
    q_cos = cos_ref[pl.ds(own, tokens), :]
    q_sin = sin_ref[pl.ds(own, tokens), :]
    for head in range(heads):
        q_rot[head] = rotate(
            q_ref[:, head * HEAD_DIM : (head + 1) * HEAD_DIM], qg_ref[...], q_cos, q_sin
        )
    acc[...] = jnp.zeros_like(acc)
    relay(0)
    load_ow.wait()

    def one_head(kv, carry):
        @pl.when(kv + 3 < kv_heads)
        def _():
            send_own(kv + 3)

        @pl.when(kv + 1 < kv_heads)
        def _():
            relay(kv + 1)

        attend(kv)
        return carry

    lax.fori_loop(0, kv_heads, one_head, 0)

    blend = acc[...].astype(BF16).astype(F32)
    blend = blend * lax.rsqrt(jnp.mean(blend * blend, axis=-1, keepdims=True) + EPSILON)
    stream = (res_ref[...].astype(F32) + blend * post_ref[...]).astype(BF16)
    stream_ref[...] = stream
    wide = stream.astype(F32)
    wide = wide * lax.rsqrt(jnp.mean(wide * wide, axis=-1, keepdims=True) + EPSILON)
    normed_ref[...] = (wide * pre_ref[...]).astype(BF16)

    def sent(buf, sem, device):
        block = buf.at[0, 0]
        remote(block, block, sem, sem, device).wait_send()

    def drain(head, carry):
        for _raw, buf, recv, sx, su, sd in both:
            for plane in range(nz):
                slot = plane * nx + x

                @pl.when(jnp.logical_and(has_up, z >= plane))
                def _(slot=slot):
                    sent(buf, su.at[slot, head], up)

                @pl.when(jnp.logical_and(has_down, z <= plane))
                def _(slot=slot):
                    sent(buf, sd.at[slot, head], down)

                for off in range(1, nx):
                    sent(buf, sx.at[slot, head, off], beside[off - 1])
        return carry

    lax.fori_loop(0, kv_heads, drain, 0)


def before(tokens):
    row = lax.broadcasted_iota(jnp.int32, (tokens, tokens), 0)
    col = lax.broadcasted_iota(jnp.int32, (tokens, tokens), 1)
    return (row < col).astype(F32).astype(BF16)


def group_choice(meta, first_expert, count, rows):
    tokens = meta.shape[1]
    low = first_expert.astype(F32)
    member = jnp.where((meta[0:1] >= low) & (meta[0:1] < low + float(count)), 1.0, 0.0)
    rank = jnp.dot(
        jnp.broadcast_to(member, (8, tokens)).astype(BF16),
        before(tokens),
        preferred_element_type=F32,
    )[0:1]
    place = lax.broadcasted_iota(jnp.int32, (rows, tokens), 0).astype(F32)
    return jnp.where(rank == place, 1.0, 0.0) * member


def slot_choice(meta, first_expert, count, cap):
    tokens = meta.shape[1]
    names = lax.broadcasted_iota(jnp.int32, (count, tokens), 0).astype(F32)
    names = names + first_expert.astype(F32)
    first = jnp.where(meta[0:1] == names, 1.0, 0.0)
    second = jnp.where(meta[1:2] == names, 1.0, 0.0)
    rank = jnp.dot((first + second).astype(BF16), before(tokens), preferred_element_type=F32)
    row = lax.broadcasted_iota(jnp.int32, (count * cap, count), 0)
    start = lax.broadcasted_iota(jnp.int32, (count * cap, count), 1) * cap
    widen = jnp.where((row >= start) & (row < start + cap), 1.0, 0.0).astype(BF16)

    def widened(values):
        return jnp.dot(widen, values.astype(BF16), preferred_element_type=F32)

    place = lax.broadcasted_iota(jnp.int32, (count * cap, tokens), 0) & (cap - 1)
    hit = jnp.where(widened(rank) == place.astype(F32), 1.0, 0.0)
    return widened(first) * hit, widened(second) * hit


def contract(left, right, dims):
    return lax.dot_general(
        left.astype(BF16), right.astype(BF16), ((dims[:1], dims[1:]), ((), ())),
        preferred_element_type=F32,
    )


def expert_kernel(
    nz, nx, n_dp,
    normed_ref, stream_ref, meta_ref, wg_hbm, wu_hbm, wd_hbm,
    out_ref,
    wg, wu, wd, w_sem, p1, r1, metas, p2, r2, o2, back, mix, fin,
    s1, t1, sm, tm, s2, t2, s3, t3, s4, t4,
):
    tokens, width = normed_ref.shape
    count, cap = p2.shape[1], p2.shape[2]
    rows = p1.shape[1]
    sp = lax.axis_index("sp")
    dp = lax.axis_index("dp")
    z, x = sp // nx, sp % nx
    me = x * n_dp + dp

    loads = [
        pltpu.make_async_copy(src, dst, w_sem.at[i])
        for i, (src, dst) in enumerate(((wg_hbm, wg), (wu_hbm, wu), (wd_hbm, wd)))
    ]
    for load in loads:
        load.start()

    def plane_peer(off):
        j = lax.rem(me + off, count)
        return j, (z * nx + j // n_dp, j % n_dp)

    def column_peer(dist):
        plane = lax.rem(z + dist, nz)
        return plane, (plane * nx + x, dp)

    barrier = pltpu.get_barrier_semaphore()
    for off in range(1, count):
        pl.semaphore_signal(barrier, inc=1, device_id=plane_peer(off)[1], device_id_type=MESH)
    for dist in range(1, nz):
        pl.semaphore_signal(barrier, inc=1, device_id=column_peer(dist)[1], device_id_type=MESH)

    meta = meta_ref[...]
    for g in range(nz):
        pick = group_choice(meta, jnp.int32(g * count), count, rows)
        p1[g] = contract(pick, normed_ref[...], (1, 0)).astype(BF16)
    metas[z] = meta
    r1[z] = p1[z]

    pl.semaphore_wait(barrier, count - 1 + nz - 1)
    for dist in range(1, nz):
        plane, device = column_peer(dist)
        remote(meta_ref, metas.at[z], sm.at[plane], tm.at[z], device).start()
        remote(p1.at[plane], r1.at[z], s1.at[plane], t1.at[z], device).start()

    first_expert = z * count

    def dispatch(dist, carry):
        source, device = column_peer(dist)

        @pl.when(dist > 0)
        def _():
            remote(meta_ref, metas.at[source], sm.at[source], tm.at[source], device).wait_recv()
            remote(p1.at[source], r1.at[source], s1.at[source], t1.at[source], device).wait_recv()

        got = metas[source]
        group = group_choice(got, first_expert, count, rows)
        first, second = slot_choice(got, first_expert, count, cap)
        pick = contract(first + second, group, (1, 1))
        packed = contract(pick, r1[source], (1, 0)).astype(BF16)
        p2[source] = packed.reshape(count, cap, width)
        r2[source, me] = p2[source, me]
        for off in range(1, count):
            j, device = plane_peer(off)
            remote(
                p2.at[source, j], r2.at[source, me], s2.at[source, j], t2.at[source, me], device
            ).start()
        return carry

    lax.fori_loop(0, nz, dispatch, 0)
    for load in loads:
        load.wait()

    def transform(dist, carry):
        source = lax.rem(z + dist + 1, nz)
        for off in range(1, count):
            j, device = plane_peer(off)
            remote(
                p2.at[source, j], r2.at[source, j], s2.at[source, j], t2.at[source, j], device
            ).wait_recv()
        arrived = r2[source].reshape(count * cap, width)
        gated = jnp.dot(arrived, wg[...], preferred_element_type=F32)
        lifted = jnp.dot(arrived, wu[...], preferred_element_type=F32)
        hidden = (gated / (1.0 + jnp.exp(-gated)) * lifted).astype(BF16)
        result = jnp.dot(hidden, wd[...], preferred_element_type=F32).astype(BF16)
        o2[source] = result.reshape(count, cap, width)
        back[source, me] = o2[source, me]
        for off in range(1, count):
            j, device = plane_peer(off)
            remote(
                o2.at[source, j], back.at[source, me], s3.at[source, j], t3.at[source, me], device
            ).start()
        return carry

    lax.fori_loop(0, nz, transform, 0)

    def combine(dist, carry):
        source, column = column_peer(dist + 1)
        for off in range(1, count):
            j, device = plane_peer(off)
            remote(
                o2.at[source, j], back.at[source, j], s3.at[source, j], t3.at[source, j], device
            ).wait_recv()
        got = metas[source]
        group = group_choice(got, first_expert, count, rows)
        first, second = slot_choice(got, first_expert, count, cap)
        outs = back[source].reshape(count * cap, width)
        one = contract(contract(group, first, (1, 1)), outs, (1, 0))
        two = contract(contract(group, second, (1, 1)), outs, (1, 0))
        weight = jnp.sum(group * got[2:3], axis=1, keepdims=True)
        share = jnp.sum(group * got[3:4], axis=1, keepdims=True)
        total = (weight * (share * one + (1.0 - share) * two)).astype(BF16)
        mix[source] = total

        @pl.when(dist == nz - 1)
        def _():
            fin[source] = total

        @pl.when(dist < nz - 1)
        def _():
            remote(mix.at[source], fin.at[z], s4.at[source], t4.at[z], column).start()

        return carry

    lax.fori_loop(0, nz, combine, 0)

    picks = [
        group_choice(meta, jnp.int32(g * count), count, rows) for g in range(nz)
    ]
    for dist in range(1, nz):
        plane, device = column_peer(dist)
        remote(mix.at[plane], fin.at[plane], s4.at[plane], t4.at[plane], device).wait_recv()
    every = jnp.concatenate(picks, axis=0)
    added = contract(every, fin[...].reshape(tokens, width), (0, 0))
    out_ref[...] = (stream_ref[...].astype(F32) + added).astype(BF16)

    for dist in range(1, nz):
        plane, device = column_peer(dist)
        remote(meta_ref, metas.at[z], sm.at[plane], tm.at[z], device).wait_send()
        remote(p1.at[plane], r1.at[z], s1.at[plane], t1.at[z], device).wait_send()
        remote(mix.at[plane], fin.at[z], s4.at[plane], t4.at[z], device).wait_send()

    def drain(source, carry):
        for off in range(1, count):
            j, device = plane_peer(off)
            remote(
                p2.at[source, j], r2.at[source, me], s2.at[source, j], t2.at[source, me], device
            ).wait_send()
            remote(
                o2.at[source, j], back.at[source, me], s3.at[source, j], t3.at[source, me], device
            ).wait_send()
        return carry

    lax.fori_loop(0, nz, drain, 0)


def local(
    residual_in, query_proj, key_proj, value_proj, query_gain, key_gain, out_weight, post_gain,
    pre_gain, route_ids, group_weight, first_share, gate_weight, up_weight, down_weight,
):
    n_sp = lax.axis_size("sp")
    n_dp = lax.axis_size("dp")
    tokens, width = query_proj.shape[1:]
    kv_width = key_proj.shape[2]
    heads, kv_heads = width // HEAD_DIM, kv_width // HEAD_DIM
    nz = GROUPS
    nx = n_sp // nz
    length = n_sp * tokens
    cos, sin = angle_tables(length)
    vmem = pl.BlockSpec(memory_space=pltpu.VMEM)
    hbm = pl.BlockSpec(memory_space=pl.ANY)
    dma = pltpu.SemaphoreType.DMA
    row = jax.ShapeDtypeStruct((tokens, width), BF16)
    stream, normed = pl.pallas_call(
        functools.partial(attention_kernel, nz, nx),
        out_shape=(row, row),
        in_specs=[vmem] * 10 + [hbm],
        out_specs=(vmem, vmem),
        scratch_shapes=[
            pltpu.VMEM((n_sp, kv_heads, tokens, HEAD_DIM), BF16),
            pltpu.VMEM((n_sp, kv_heads, tokens, HEAD_DIM), BF16),
            pltpu.VMEM((heads, tokens, HEAD_DIM), BF16),
            pltpu.VMEM((length, HEAD_DIM), BF16),
            pltpu.VMEM((tokens, width // kv_heads), BF16),
            pltpu.VMEM((tokens, width), F32),
            pltpu.VMEM((width, width), BF16),
            dma,
            dma((n_sp, kv_heads)), dma((n_sp, kv_heads)),
            dma((n_sp, kv_heads, nx)), dma((n_sp, kv_heads)), dma((n_sp, kv_heads)),
            dma((n_sp, kv_heads, nx)), dma((n_sp, kv_heads)), dma((n_sp, kv_heads)),
        ],
        compiler_params=pltpu.CompilerParams(
            collective_id=0, has_side_effects=True, vmem_limit_bytes=VMEM_LIMIT
        ),
        name="attention",
    )(
        query_proj[0], key_proj[0], value_proj[0],
        query_gain.reshape(1, -1), key_gain.reshape(1, -1),
        jnp.asarray(cos), jnp.asarray(sin),
        residual_in[0], post_gain.reshape(1, -1), pre_gain.reshape(1, -1), out_weight,
    )

    experts = gate_weight.shape[0] * n_sp * n_dp
    count = experts // nz
    cap = max(16, 4 * tokens // experts)
    rows = tokens // nz
    ff = gate_weight.shape[2]
    meta = jnp.concatenate(
        [route_ids[0].T.astype(F32), group_weight, first_share, jnp.zeros((4, tokens), F32)], axis=0
    )
    blocks = pltpu.VMEM((nz, count, cap, width), BF16)
    lines = pltpu.VMEM((nz, rows, width), BF16)
    out = pl.pallas_call(
        functools.partial(expert_kernel, nz, nx, n_dp),
        out_shape=row,
        in_specs=[vmem] * 3 + [hbm] * 3,
        out_specs=vmem,
        scratch_shapes=[
            pltpu.VMEM((width, ff), BF16),
            pltpu.VMEM((width, ff), BF16),
            pltpu.VMEM((ff, width), BF16),
            dma((3,)),
            lines, lines,
            pltpu.VMEM((nz, 8, tokens), F32),
            blocks, blocks, blocks, blocks,
            lines, lines,
            dma((nz,)), dma((nz,)), dma((nz,)), dma((nz,)),
            dma((nz, count)), dma((nz, count)), dma((nz, count)), dma((nz, count)),
            dma((nz,)), dma((nz,)),
        ],
        compiler_params=pltpu.CompilerParams(
            collective_id=1, has_side_effects=True, vmem_limit_bytes=VMEM_LIMIT
        ),
        name="experts",
    )(normed, stream, meta, gate_weight[0], up_weight[0], down_weight[0])
    return out.reshape(1, tokens, width)


def layer_kernel(
    nz, nx, cores,
    q_hbm, k_hbm, v_hbm, qg_hbm, kg_hbm, res_hbm, post_hbm, pre_hbm, route_hbm, gw_hbm, fs_hbm,
    cos_hbm, sin_hbm, ow_hbm, wg_hbm, wu_hbm, wd_hbm,
    out_hbm,
    q_ref, k_ref, v_ref, qg_ref, kg_ref, res_ref, post_ref, pre_ref, route_ref, gw_ref, fs_ref,
    cos, sin, ow, wg, wu, wd, load_sem,
    kv, q_rot, att, acc,
    rk_own, rk_x, rk_z, kv_x_sent, kv_z_sent,
    perm, perm_back, mrow, metas, picks, weights, backs,
    zs_sem, zr_sem, ms_sem, mr_sem,
    stream, srt, rows, y, other, part, relay, direct, summed, fin, out, out_sem,
    t_z, t_a, t_b, t_c, t_d, t_core, spread_sent,
    t_other, t_up, t_side, t_last, t_home, back_sent,
):
    tokens, width = q_ref.shape
    heads = width // HEAD_DIM
    kv_heads = k_ref.shape[1] // HEAD_DIM
    group = heads // kv_heads
    slots_kv = nz * nx
    length = slots_kv * tokens
    last_head = kv_heads - 1
    chips = metas.shape[2]
    count = chips * cores
    block = tokens // nz
    cap = y.shape[2] // chips
    half = block // 2
    me = lax.axis_index("sp")
    dp = lax.axis_index("dp")
    z, x = me // nx, me % nx
    side, core = dp // cores, dp % cores
    up, down = (me + nx, dp), (me - nx, dp)
    beside = (z * nx + 1 - x, dp)
    across = (me, (1 - side) * cores + core)
    partner = (me, side * cores + 1 - core)
    has_up, has_down = z < nz - 1, z > 0
    mine = side * nx + x
    chip_x, chip_y = side * nx + 1 - x, (1 - side) * nx + x
    chip_d = (1 - side) * nx + 1 - x

    def column(plane):
        return (plane * nx + x, dp)

    flip = z >= nz // 2
    low = jnp.where(flip, nz - 1 - z, z)

    def source_of(i):
        if i == 0:
            return z
        near = (i - 1) + jnp.where(low <= i - 1, 1, 0)
        return jnp.where(flip, nz - 1 - near, near)

    sources = [source_of(i) for i in range(nz)]

    barrier = pltpu.get_barrier_semaphore()
    greeted = [column(lax.rem(z + dist, nz)) for dist in range(1, nz)] + [beside, across, partner]
    for device in greeted:
        pl.semaphore_signal(barrier, inc=1, device_id=device, device_id_type=MESH)

    own = pl.multiple_of(me * tokens, tokens)
    loads = [
        pltpu.make_async_copy(src, dst, load_sem.at[i])
        for i, (src, dst) in enumerate((
            (k_hbm, k_ref), (v_hbm, v_ref), (kg_hbm, kg_ref),
            (cos_hbm.at[pl.ds(own, tokens)], cos), (sin_hbm.at[pl.ds(own, tokens)], sin),
            (q_hbm, q_ref), (qg_hbm, qg_ref), (route_hbm, route_ref), (gw_hbm, gw_ref),
            (fs_hbm, fs_ref), (ow_hbm, ow), (res_hbm, res_ref), (post_hbm, post_ref),
            (pre_hbm, pre_ref), (wg_hbm, wg), (wu_hbm, wu), (wd_hbm, wd),
        ))
    ]
    for load in loads:
        load.start()

    for load in loads[:5]:
        load.wait()
    for head in range(kv_heads):
        columns = slice(head * HEAD_DIM, (head + 1) * HEAD_DIM)
        kv[head * slots_kv + me, 1] = v_ref[:, columns]
        kv[head * slots_kv + me, 0] = rotate(k_ref[:, columns], kg_ref[...], cos[...], sin[...])

    pl.semaphore_wait(barrier, len(greeted))

    def hop(slot, head, device, sent, landed):
        view = kv.at[head * slots_kv + slot]
        return remote(view, view, sent.at[0], landed, device)

    def bytes_of(units, sent, landed):
        view = kv.at[pl.ds(0, units)]
        return remote(view, view, sent, landed, beside)

    def own_beside(head):
        return hop(me, head, beside, kv_x_sent, rk_own.at[head])

    def pass_beside(slot, head):
        return hop(slot, head, beside, kv_x_sent, rk_x.at[head])

    def pass_on(slot, source, head, device):
        return hop(slot, head, device, kv_z_sent, rk_z.at[source, head])

    def cross_on(head, device):
        return hop(z * nx + 1 - x, head, device, kv_z_sent, rk_x.at[head])

    def crossing(head):
        return lax.rem(head, 2) == 1

    late_up, late_down = z == nz - 2, z == 1
    at_end = jnp.logical_or(z == 0, z == nz - 1)

    for head in range(kv_heads):
        own_beside(head).start()
        soon_up = has_up if head < last_head else jnp.logical_and(has_up, ~late_up)
        soon_down = has_down if head < last_head else jnp.logical_and(has_down, ~late_down)

        @pl.when(soon_up)
        def _(head=head):
            pass_on(me, z, head, up).start()

        @pl.when(soon_down)
        def _(head=head):
            pass_on(me, z, head, down).start()

    def relay_kv(head, before_last):
        final = head == last_head
        bytes_of(1, kv_x_sent.at[0], rk_own.at[head]).wait_recv()
        crosses = crossing(head)
        for on, late, device in ((has_up, late_up, up), (has_down, late_down, down)):
            @pl.when(jnp.logical_and(crosses & on, ~(final & late)))
            def _(device=device):
                cross_on(head, device).start()

        def step(dist, given):
            for below in (True, False):
                source = z - dist if below else z + dist
                present = source >= 0 if below else source < nz
                further = has_up if below else has_down
                onward = up if below else down

                @pl.when(jnp.logical_and(present, given))
                def _(source=source, further=further, onward=onward):
                    slot = source * nx + x
                    bytes_of(1, kv_z_sent.at[0], rk_z.at[source, head]).wait_recv()

                    @pl.when(further)
                    def _():
                        pass_on(slot, source, head, onward).start()

                    if dist == 1:
                        @pl.when(~crosses)
                        def _():
                            pass_beside(slot, head).start()
                    else:
                        pass_beside(slot, head).start()

        step(1, ~(final & at_end))
        for dist in range(2, nz):
            @pl.when(final & (at_end if dist == nz - 1 else (dist == nz - 2) & ~at_end))
            def _():
                before_last()

            step(dist, True)
        step(1, final & at_end)
        for late, device in ((late_up, up), (late_down, down)):
            @pl.when(final & late)
            def _(device=device):
                pass_on(me, z, head, device).start()

                @pl.when(crosses)
                def _():
                    cross_on(head, device).start()

    for load in loads[5:10]:
        load.wait()
    for head in range(heads):
        q_rot[head] = rotate(
            q_ref[:, head * HEAD_DIM : (head + 1) * HEAD_DIM], qg_ref[...], cos[...], sin[...]
        )
    acc[...] = jnp.zeros_like(acc)

    row = lax.broadcasted_iota(jnp.int32, (tokens, tokens), 0)
    lane = lax.broadcasted_iota(jnp.int32, (tokens, tokens), 1)

    def routing():
        first = route_ref[0:1].astype(F32)
        second = route_ref[1:2].astype(F32)
        of_lane = jnp.zeros_like(first)
        for g in range(1, nz):
            of_lane = of_lane + jnp.where(first >= float(g * count), 1.0, 0.0)
        of = jnp.sum(jnp.where(row == lane, of_lane, 0.0), axis=1, keepdims=True)
        same = of == of_lane
        rank = jnp.sum(jnp.where(same & (lane < row), 1.0, 0.0), axis=1, keepdims=True)
        rank_lane = jnp.sum(jnp.where(same & (row < lane), 1.0, 0.0), axis=0, keepdims=True)
        place = (of * float(block) + rank).astype(jnp.int32)
        place_lane = (of_lane * float(block) + rank_lane).astype(jnp.int32)
        perm[...] = jnp.where(row == place_lane, 1.0, 0.0).astype(BF16)
        perm_back[...] = jnp.where(place == lane, 1.0, 0.0).astype(BF16)
        fields = (
            first, second,
            gw_ref[...] * fs_ref[...], gw_ref[...] * (1.0 - fs_ref[...]),
        )
        chosen = lax.broadcasted_iota(jnp.int32, (8, tokens), 0).astype(F32) == of_lane
        at = rank.astype(jnp.int32)
        table = jnp.zeros((8, tokens), F32)
        for f, field in enumerate(fields):
            spread = jnp.where(lane == at + f * block, 1.0, 0.0)
            table += lax.dot_general(
                jnp.where(chosen, field, 0.0), spread, (((1,), (0,)), ((), ())),
                precision=lax.Precision.HIGHEST, preferred_element_type=F32,
            )
        for g in range(nz):
            mrow[g] = table[g : g + 1]

    routing()
    metas[z, core, mine] = mrow[z]

    def meta_column(dist):
        plane = lax.rem(z + dist, nz)
        return remote(
            mrow.at[plane], metas.at[z, core, mine], zs_sem.at[0], zr_sem.at[0], column(plane)
        )

    def meta_all():
        view = mrow.at[pl.ds(0, nz - 1)]
        return remote(view, view, zs_sem.at[0], zr_sem.at[0], beside)

    for dist in range(1, nz):
        meta_column(dist).start()

    def meta_copy(view, step, device):
        return remote(view, view, ms_sem.at[step], mr_sem.at[step], device)

    pair = pl.ds(side * nx, nx)
    other_pair = pl.ds((1 - side) * nx, nx)
    meta_sends = (
        meta_copy(metas.at[:, core, mine], 0, beside),
        meta_copy(metas.at[:, core, pair], 1, across),
        meta_copy(metas.at[:, core], 2, partner),
    )
    meta_recvs = (
        meta_copy(metas.at[:, core, chip_x], 0, beside),
        meta_copy(metas.at[:, core, other_pair], 1, across),
        meta_copy(metas.at[:, 1 - core], 2, partner),
    )

    def choice(plane, of_core, expert):
        table = metas[plane, of_core].reshape(chips, tokens)
        first = table[:, 0:block] == expert
        second = table[:, block : 2 * block] == expert
        member = jnp.where(first | second, 1.0, 0.0)
        weight = jnp.where(first, table[:, 2 * block : 3 * block], 0.0)
        weight = weight + jnp.where(second, table[:, 3 * block : 4 * block], 0.0)
        r = lax.broadcasted_iota(jnp.int32, (block, block), 0)
        c = lax.broadcasted_iota(jnp.int32, (block, block), 1)
        earlier = jnp.where(r < c, 1.0, 0.0).astype(BF16)
        rank = jnp.dot(
            jnp.concatenate([member] * (8 // chips), axis=0).astype(BF16), earlier,
            preferred_element_type=F32,
        )[:chips]
        place = lax.broadcasted_iota(jnp.int32, (chips, cap, block), 1).astype(F32)
        hit = jnp.where(rank[:, None, :] == place, 1.0, 0.0) * member[:, None, :]
        of_slot = jnp.sum(hit * weight[:, None, :], axis=2, keepdims=True).reshape(chips * cap, 1)
        flat = hit.reshape(chips * cap, block).astype(BF16)
        wide_row = lax.broadcasted_iota(jnp.int32, (block, tokens), 0)
        wide_lane = lax.broadcasted_iota(jnp.int32, (block, tokens), 1)
        widen = jnp.where(lax.rem(wide_lane, block) == wide_row, 1.0, 0.0).astype(BF16)
        spread = jnp.dot(flat, widen, preferred_element_type=F32)
        slot = lax.broadcasted_iota(jnp.int32, (chips * cap, tokens), 0) // cap
        chip = lax.broadcasted_iota(jnp.int32, (chips * cap, tokens), 1) // block
        return jnp.where(slot == chip, spread, 0.0), of_slot

    def tables():
        expert = (z * count + x * (count // nx) + dp).astype(F32)
        twin = (z * count + x * (count // nx) + side * cores + 1 - core).astype(F32)

        def one_plane(plane, carry):
            for of_core in range(cores):
                pick, of_slot = choice(plane, of_core, expert)
                picks[plane, of_core] = pick.astype(BF16)
                weights[plane, of_core] = of_slot
            back, _ = choice(plane, core, expert)
            theirs, _ = choice(plane, core, twin)
            backs[plane] = jnp.concatenate([back, theirs], axis=0).T.astype(BF16)
            return carry

        lax.fori_loop(0, nz, one_plane, 0)

    factor = float(HEAD_DIM**-0.5 * np.log2(np.e))
    span = group * HEAD_DIM

    def attend(head):
        here = pl.ds(head * slots_kv, slots_kv)
        keys = kv[here, 0].reshape(length, HEAD_DIM)
        values = kv[here, 1].reshape(length, HEAD_DIM)
        for member in range(group):
            scores = lax.dot_general(
                q_rot[head * group + member], keys, (((1,), (1,)), ((), ())),
                preferred_element_type=F32,
            )
            top = jnp.max(scores, axis=-1, keepdims=True)
            raised = jnp.exp2((scores - top) * factor)
            total = jnp.sum(raised, axis=-1, keepdims=True)
            mixed = jnp.dot(raised.astype(BF16), values, preferred_element_type=F32)
            att[:, member * HEAD_DIM : (member + 1) * HEAD_DIM] = (mixed / total).astype(BF16)
        above = ow.at[pl.ds(pl.multiple_of(head * span, span), span), :]
        tile = 1024
        for start in range(0, width, tile):
            columns = slice(start, start + tile)
            acc[:, columns] += jnp.dot(att[...], above[:, columns], preferred_element_type=F32)

    def prepare():
        meta_recvs[2].wait_recv()
        tables()

    relay_kv(jnp.int32(0), prepare)
    meta_all().wait_recv()
    meta_sends[0].start()
    loads[10].wait()

    def one_head(head, carry):
        @pl.when(head + 1 < kv_heads)
        def _():
            relay_kv(head + 1, prepare)

        @pl.when(head == 0)
        def _():
            meta_recvs[0].wait_recv()
            meta_sends[1].start()

        @pl.when(head == 1)
        def _():
            meta_recvs[1].wait_recv()
            meta_sends[2].start()

        bytes_of(nz - 1, kv_x_sent.at[0], rk_x.at[head]).wait_recv()
        attend(head)
        return carry

    lax.fori_loop(0, kv_heads, one_head, 0)
    for load in loads[11:14]:
        load.wait()

    blend = acc[...].astype(BF16).astype(F32)
    blend = blend * lax.rsqrt(jnp.mean(blend * blend, axis=-1, keepdims=True) + EPSILON)
    flow = (res_ref[...].astype(F32) + blend * post_ref[...]).astype(BF16)
    stream[...] = flow
    wide = flow.astype(F32)
    wide = wide * lax.rsqrt(jnp.mean(wide * wide, axis=-1, keepdims=True) + EPSILON)
    normed = (wide * pre_ref[...]).astype(BF16)
    srt[...] = jnp.dot(perm[...], normed, preferred_element_type=F32).astype(BF16).reshape(srt.shape)

    def unit(s, of_core, chip, h=0):
        return ((s * cores + of_core) * chips + chip) * 2 + h

    def units(first, amount):
        return rows.at[pl.ds(first, amount)]

    def waiting(amount, landed):
        return remote(units(0, amount), units(0, amount), spread_sent.at[0], landed, partner)

    def z_send(plane):
        return remote(
            srt.at[pl.ds(2 * plane, 2)], units(unit(z, core, mine), 2), spread_sent.at[0], t_z.at[z],
            column(plane),
        )

    for i in range(1, nz):
        z_send(sources[i]).start()
    rows[pl.ds(unit(z, core, mine), 2)] = srt[pl.ds(2 * z, 2)]

    def over(s, chip, h, landed, device):
        view = rows.at[unit(s, core, chip, h)]
        return remote(view, view, spread_sent.at[0], landed.at[s], device)

    def over_core(s, chip):
        view = units(unit(s, core, chip), 2)
        return remote(view, view, spread_sent.at[0], t_core.at[s], partner)

    def spread_own(i):
        s = sources[i]
        if i > 0:
            waiting(2, t_z.at[s]).wait_recv()
        over(s, mine, 0, t_a, beside).start()
        over(s, mine, 1, t_b, across).start()
        over(s, mine, 1, t_c, beside).start()
        over(s, mine, 0, t_c, across).start()
        over_core(s, mine).start()

    def spread_on(i):
        s = sources[i]
        waiting(1, t_a.at[s]).wait_recv()
        over(s, chip_x, 0, t_d, across).start()
        waiting(1, t_b.at[s]).wait_recv()
        over(s, chip_y, 1, t_d, beside).start()

    def spread_core(i):
        s = sources[i]
        waiting(2, t_c.at[s]).wait_recv()
        over_core(s, chip_x).start()
        over_core(s, chip_y).start()

    def spread_last(i):
        s = sources[i]
        waiting(2, t_d.at[s]).wait_recv()
        over_core(s, chip_d).start()

    def to_partner(s):
        return remote(y.at[s, 1 - core], other.at[s], back_sent.at[0], t_other.at[s], partner)

    def transform(i):
        s = sources[i]
        waiting(2 * chips, t_core.at[s]).wait_recv()
        packed = [
            jnp.dot(
                picks[s, q], rows[pl.ds(unit(s, q, 0), 2 * chips)].reshape(tokens, width), preferred_element_type=F32
            ).astype(BF16)
            for q in range(cores)
        ]
        packed = jnp.concatenate(packed, axis=0)
        gated = jnp.dot(packed, wg[...], preferred_element_type=F32)
        lifted = jnp.dot(packed, wu[...], preferred_element_type=F32)
        hidden = (gated / (1.0 + jnp.exp(-gated)) * lifted).astype(BF16)
        result = jnp.dot(hidden, wd[...], preferred_element_type=F32)
        slots = chips * cap
        for q in range(cores):
            y[s, q] = (result[q * slots : (q + 1) * slots] * weights[s, q]).astype(BF16)
        to_partner(s).start()

    def back(s, chip, h, into, at, landed, device):
        return remote(
            part.at[s, chip, halves[h]], into.at[s, at], back_sent.at[0], landed.at[s], device
        )

    halves = (pl.ds(0, half), pl.ds(half, half))

    def gather_back(i):
        s = sources[i]
        to_partner(s).wait_recv()
        outs = jnp.concatenate([y[s, core], other[s]], axis=0)
        part[s] = jnp.dot(backs[s], outs, preferred_element_type=F32).astype(BF16).reshape(
            chips, block, width
        )
        back(s, chip_d, 0, relay, 0, t_up, across).start()
        back(s, chip_d, 1, relay, 1, t_side, beside).start()
        back(s, chip_x, 1, direct, 1, t_last, beside).start()
        back(s, chip_y, 0, direct, 0, t_last, across).start()

    def add(left, right):
        return (left.astype(F32) + right.astype(F32)).astype(BF16)

    def pass_back(i):
        s = sources[i]
        waiting(1, t_up.at[s]).wait_recv()
        part[s, chip_x, halves[0]] = add(part[s, chip_x, halves[0]], relay[s, 0])
        back(s, chip_x, 0, summed, 0, t_last, beside).start()
        waiting(1, t_side.at[s]).wait_recv()
        part[s, chip_y, halves[1]] = add(part[s, chip_y, halves[1]], relay[s, 1])
        back(s, chip_y, 1, summed, 1, t_last, across).start()

    def home(s):
        return remote(part.at[s, mine], fin.at[z], back_sent.at[0], t_home.at[0], column(s))

    def finish(i):
        s = sources[i]
        waiting(4, t_last.at[s]).wait_recv()
        for h in range(2):
            total = part[s, mine, halves[h]].astype(F32) + direct[s, h].astype(F32)
            total = (total + summed[s, h].astype(F32)).astype(BF16)
            if i > 0:
                part[s, mine, halves[h]] = total
            else:
                fin[s, halves[h]] = total
        if i > 0:
            home(s).start()

    def weights_ready(i):
        for load in loads[14:]:
            load.wait()

    for stage, i in plan(
        spread_own, spread_on, spread_core, spread_last, weights_ready, transform, gather_back, pass_back, finish
    ):
        stage(i)

    waiting(2 * (nz - 1), t_home.at[0]).wait_recv()
    tile = width // 4
    stores = []
    for n, start in enumerate(range(0, width, tile)):
        columns = slice(start, start + tile)
        added = jnp.dot(
            perm_back[...], fin[:, :, columns].reshape(tokens, tile), preferred_element_type=F32
        )
        out[:, columns] = (stream[:, columns].astype(F32) + added).astype(BF16)
        store = pltpu.make_async_copy(out.at[:, columns], out_hbm.at[:, columns], out_sem.at[n])
        store.start()
        stores.append(store)

    for plane in range(nz):
        lanes = sum(head % 2 for head in range(kv_heads))
        upward = (plane + 1) * kv_heads + lanes if plane < nz - 1 else 0
        downward = (nz - plane) * kv_heads + lanes if plane > 0 else 0
        sideways = nz * kv_heads - lanes * sum(0 <= plane + d < nz for d in (-1, 1))

        @pl.when(z == plane)
        def _(vertical=upward + downward, sideways=sideways):
            bytes_of(vertical, kv_z_sent.at[0], rk_own.at[0]).wait_send()
            bytes_of(sideways, kv_x_sent.at[0], rk_own.at[0]).wait_send()

    meta_all().wait_send()
    for send in meta_sends:
        send.wait_send()
    spread_units = 2 * (nz - 1) + nz * (6 + 2 * chips)
    waiting(spread_units, t_core.at[0]).wait_send()
    back_units = nz * (2 * chips * cap // block + 6) + 2 * (nz - 1)
    returned = units(0, back_units)
    remote(returned, returned, back_sent.at[0], t_core.at[0], partner).wait_send()
    for store in stores:
        store.wait()


def plan(own, on, share, last, ready, transform, gather_back, pass_back, finish):
    return (
        (own, 0), (on, 0), (own, 1), (share, 0), (on, 1), (own, 2), (last, 0), (share, 1),
        (ready, 0), (transform, 0), (on, 2), (own, 3), (last, 1), (share, 2), (transform, 1),
        (on, 3), (last, 2), (share, 3), (gather_back, 1), (transform, 2), (last, 3),
        (gather_back, 2), (transform, 3), (gather_back, 3), (pass_back, 2), (pass_back, 3),
        (finish, 2), (gather_back, 0), (pass_back, 1), (finish, 3), (finish, 1),
        (pass_back, 0), (finish, 0),
    )


def fused(
    residual_in, query_proj, key_proj, value_proj, query_gain, key_gain, out_weight, post_gain,
    pre_gain, route_ids, group_weight, first_share, gate_weight, up_weight, down_weight,
):
    n_sp = lax.axis_size("sp")
    n_dp = lax.axis_size("dp")
    tokens, width = query_proj.shape[1:]
    kv_heads = key_proj.shape[2] // HEAD_DIM
    heads = width // HEAD_DIM
    nz = GROUPS
    nx = n_sp // nz
    cores = 2
    chips = nx * (n_dp // cores)
    experts = gate_weight.shape[0] * n_sp * n_dp
    cap = max(16, 4 * tokens // experts)
    block = tokens // nz
    slots = chips * cap
    ff = gate_weight.shape[2]
    length = n_sp * tokens
    cos, sin = angle_tables(length)
    vmem = pl.BlockSpec(memory_space=pltpu.VMEM)
    hbm = pl.BlockSpec(memory_space=pl.ANY)
    dma = pltpu.SemaphoreType.DMA

    def buf(*shape, kind=BF16):
        return pltpu.VMEM(shape, kind)

    out = pl.pallas_call(
        functools.partial(layer_kernel, nz, nx, cores),
        out_shape=jax.ShapeDtypeStruct((tokens, width), BF16),
        in_specs=[hbm] * 17,
        out_specs=hbm,
        scratch_shapes=[
            buf(tokens, width), buf(tokens, kv_heads * HEAD_DIM), buf(tokens, kv_heads * HEAD_DIM),
            buf(1, HEAD_DIM, kind=F32), buf(1, HEAD_DIM, kind=F32), buf(tokens, width),
            buf(1, width, kind=F32), buf(1, width, kind=F32),
            buf(2, tokens, kind=jnp.int32), buf(1, tokens, kind=F32), buf(1, tokens, kind=F32),
            buf(tokens, HEAD_DIM, kind=F32), buf(tokens, HEAD_DIM, kind=F32),
            buf(width, width), buf(width, ff), buf(width, ff), buf(ff, width),
            dma((17,)),
            buf(kv_heads * n_sp, 2, tokens, HEAD_DIM),
            buf(heads, tokens, HEAD_DIM),
            buf(tokens, width // kv_heads),
            buf(tokens, width, kind=F32),
            dma((kv_heads,)), dma((kv_heads,)), dma((nz, kv_heads)), dma((1,)), dma((1,)),
            buf(tokens, tokens), buf(tokens, tokens),
            buf(nz, 1, tokens, kind=F32), buf(nz, cores, chips, 1, tokens, kind=F32),
            buf(nz, cores, slots, tokens), buf(nz, cores, slots, 1, kind=F32),
            buf(nz, tokens, cores * slots),
            dma((1,)), dma((1,)), dma((3,)), dma((3,)),
            buf(tokens, width), buf(2 * nz, block // 2, width),
            buf(nz * cores * chips * 2, block // 2, width),
            buf(nz, cores, slots, width), buf(nz, slots, width),
            buf(nz, chips, block, width),
            buf(nz, 2, block // 2, width), buf(nz, 2, block // 2, width),
            buf(nz, 2, block // 2, width), buf(nz, block, width),
            buf(tokens, width), dma((4,)),
            dma((nz,)), dma((nz,)), dma((nz,)), dma((nz,)), dma((nz,)), dma((nz,)), dma((1,)),
            dma((nz,)), dma((nz,)), dma((nz,)), dma((nz,)), dma((1,)), dma((1,)),
        ],
        compiler_params=pltpu.CompilerParams(
            collective_id=0, has_side_effects=True, vmem_limit_bytes=VMEM_LIMIT
        ),
        name="layer",
    )(
        query_proj[0], key_proj[0], value_proj[0],
        query_gain.reshape(1, -1), key_gain.reshape(1, -1),
        residual_in[0], post_gain.reshape(1, -1), pre_gain.reshape(1, -1),
        route_ids[0].T, group_weight, first_share,
        jnp.asarray(cos), jnp.asarray(sin), out_weight,
        gate_weight[0], up_weight[0], down_weight[0],
    )
    return out.reshape(1, tokens, width)


def solution(mesh):
    tok3 = P("dp", "sp", None)
    tok2 = P("dp", "sp")
    weight = P(("sp", "dp"), None, None)
    placed = (
        tok3, tok3, tok3, tok3, P(), P(), P(), P(), P(), tok3, tok2, tok2, weight, weight, weight,
    )
    small = mesh.shape["sp"] == 2 * GROUPS and mesh.shape["dp"] == 4
    return jax.shard_map(
        fused if small else local, mesh=mesh, in_specs=placed, out_specs=P("dp", "sp", None), check_vma=False
    )
```

```python
import functools

import jax
import jax.numpy as jnp
import numpy as np
from jax import lax
from jax.experimental import pallas as pl
from jax.experimental.pallas import tpu as pltpu
from jax.sharding import PartitionSpec as P

HEAD_DIM = 128
GRID_W = 64
GROUPS = 4
EPSILON = 1e-06
MESH = pl.DeviceIdType.MESH
VMEM_LIMIT = 60 * 1024 * 1024
F32 = jnp.float32
BF16 = jnp.bfloat16


def angle_tables(length):
    quarter = HEAD_DIM // 4
    inverse = 10000.0 ** (-np.arange(quarter, dtype=np.float64) / quarter)
    positions = np.arange(length)
    rows = (positions // GRID_W)[:, None] * inverse
    cols = (positions % GRID_W)[:, None] * inverse
    angles = np.concatenate([rows, rows, cols, cols], axis=-1)
    sign = np.where(np.arange(HEAD_DIM) % (2 * quarter) < quarter, -1.0, 1.0)
    return np.cos(angles).astype(np.float32), (np.sin(angles) * sign).astype(np.float32)


def rotate(raw, gain, cos, sin):
    floats = raw.astype(F32)
    normed = floats * lax.rsqrt(jnp.mean(floats * floats, axis=-1, keepdims=True) + EPSILON) * gain
    quarter = HEAD_DIM // 4
    lane = lax.broadcasted_iota(jnp.int32, normed.shape, 1)
    turned = jnp.where(
        (lane & (2 * quarter - 1)) < quarter,
        pltpu.roll(normed, HEAD_DIM - quarter, 1),
        pltpu.roll(normed, quarter, 1),
    )
    return (normed * cos + turned * sin).astype(BF16)


def remote(src, dst, send_sem, recv_sem, device):
    return pltpu.make_async_remote_copy(
        src_ref=src,
        dst_ref=dst,
        send_sem=send_sem,
        recv_sem=recv_sem,
        device_id=device,
        device_id_type=MESH,
    )


def attention_kernel(
    nz, nx,
    q_ref, k_ref, v_ref, qg_ref, kg_ref, cos_ref, sin_ref, res_ref, post_ref, pre_ref, ow_hbm,
    stream_ref, normed_ref,
    k_all, v_all, q_rot, k_rot, att, acc, ow, ow_sem,
    rk, rv, skx, sku, skd, svx, svu, svd,
):
    tokens, width = q_ref.shape
    heads = width // HEAD_DIM
    kv_heads = k_ref.shape[1] // HEAD_DIM
    group = heads // kv_heads
    me = lax.axis_index("sp")
    dp = lax.axis_index("dp")
    z, x = me // nx, me % nx
    up, down = (me + nx, dp), (me - nx, dp)
    has_up, has_down = z < nz - 1, z > 0
    both = ((k_ref, k_all, rk, skx, sku, skd), (v_ref, v_all, rv, svx, svu, svd))

    load_ow = pltpu.make_async_copy(ow_hbm, ow, ow_sem)
    load_ow.start()

    barrier = pltpu.get_barrier_semaphore()
    around = [(lax.rem(z + 1, nz) * nx + x, dp), (lax.rem(z + nz - 1, nz) * nx + x, dp)]
    beside = [(z * nx + lax.rem(x + off, nx), dp) for off in range(1, nx)]
    for device in around + beside:
        pl.semaphore_signal(barrier, inc=1, device_id=device, device_id_type=MESH)
    pl.semaphore_wait(barrier, len(around) + len(beside))

    def lanes_of(head):
        return pl.ds(pl.multiple_of(head * HEAD_DIM, HEAD_DIM), HEAD_DIM)

    def hop(src, buf, recv, send, slot, head, device):
        return remote(src, buf.at[slot, head], send, recv.at[slot, head], device)

    def send_own(head):
        for raw, buf, recv, sx, su, sd in both:
            src = raw.at[:, lanes_of(head)]

            @pl.when(has_up)
            def _():
                hop(src, buf, recv, su.at[me, head], me, head, up).start()

            @pl.when(has_down)
            def _():
                hop(src, buf, recv, sd.at[me, head], me, head, down).start()

        for raw, buf, recv, sx, su, sd in both:
            src = raw.at[:, lanes_of(head)]
            for off in range(1, nx):
                hop(src, buf, recv, sx.at[me, head, off], me, head, beside[off - 1]).start()

    def arrived(buf, recv, slot, head):
        block = buf.at[slot, head]
        remote(block, block, recv.at[slot, head], recv.at[slot, head], up).wait_recv()

    def relay(head):
        for dist in range(1, nz):
            for below in (True, False):
                source = z - dist if below else z + dist
                present = source >= 0 if below else source < nz
                further = has_up if below else has_down
                onward = up if below else down

                @pl.when(present)
                def _(source=source, below=below, further=further, onward=onward):
                    slot = source * nx + x
                    for _raw, buf, recv, sx, su, sd in both:
                        arrived(buf, recv, slot, head)
                        src = buf.at[slot, head]
                        send = su if below else sd

                        @pl.when(further)
                        def _(src=src, buf=buf, recv=recv, send=send):
                            hop(src, buf, recv, send.at[slot, head], slot, head, onward).start()

                        for off in range(1, nx):
                            hop(
                                src, buf, recv, sx.at[slot, head, off], slot, head,
                                beside[off - 1],
                            ).start()

    length = nz * nx * tokens
    factor = float(HEAD_DIM**-0.5 * np.log2(np.e))
    span = group * HEAD_DIM

    def attend(kv):
        for plane in range(nz):
            for off in range(1, nx):
                slot = plane * nx + lax.rem(x + off, nx)
                arrived(k_all, rk, slot, kv)
                arrived(v_all, rv, slot, kv)
        k_all[me, kv] = k_ref[:, lanes_of(kv)]
        v_all[me, kv] = v_ref[:, lanes_of(kv)]

        def place(slot, carry):
            rows = pl.ds(pl.multiple_of(slot * tokens, tokens), tokens)
            k_rot[rows, :] = rotate(k_all[slot, kv], kg_ref[...], cos_ref[rows, :], sin_ref[rows, :])
            return carry

        lax.fori_loop(0, nz * nx, place, 0)
        keys = k_rot[...]
        values = v_all[:, kv].reshape(length, HEAD_DIM)
        for member in range(group):
            scores = lax.dot_general(
                q_rot[kv * group + member], keys, (((1,), (1,)), ((), ())),
                preferred_element_type=F32,
            )
            top = jnp.max(scores, axis=-1, keepdims=True)
            raised = jnp.exp2((scores - top) * factor)
            probs = (raised * (1.0 / jnp.sum(raised, axis=-1, keepdims=True))).astype(BF16)
            att[:, member * HEAD_DIM : (member + 1) * HEAD_DIM] = jnp.dot(
                probs, values, preferred_element_type=F32
            ).astype(BF16)
        part = ow.at[pl.ds(pl.multiple_of(kv * span, span), span), :]
        tile = 1024
        for start in range(0, width, tile):
            columns = slice(start, start + tile)
            acc[:, columns] += jnp.dot(att[...], part[:, columns], preferred_element_type=F32)

    send_own(0)
    for head in range(1, min(3, kv_heads)):
        send_own(head)
    own = pl.multiple_of(me * tokens, tokens)
    q_cos = cos_ref[pl.ds(own, tokens), :]
    q_sin = sin_ref[pl.ds(own, tokens), :]
    for head in range(heads):
        q_rot[head] = rotate(
            q_ref[:, head * HEAD_DIM : (head + 1) * HEAD_DIM], qg_ref[...], q_cos, q_sin
        )
    acc[...] = jnp.zeros_like(acc)
    relay(0)
    load_ow.wait()

    def one_head(kv, carry):
        @pl.when(kv + 3 < kv_heads)
        def _():
            send_own(kv + 3)

        @pl.when(kv + 1 < kv_heads)
        def _():
            relay(kv + 1)

        attend(kv)
        return carry

    lax.fori_loop(0, kv_heads, one_head, 0)

    blend = acc[...].astype(BF16).astype(F32)
    blend = blend * lax.rsqrt(jnp.mean(blend * blend, axis=-1, keepdims=True) + EPSILON)
    stream = (res_ref[...].astype(F32) + blend * post_ref[...]).astype(BF16)
    stream_ref[...] = stream
    wide = stream.astype(F32)
    wide = wide * lax.rsqrt(jnp.mean(wide * wide, axis=-1, keepdims=True) + EPSILON)
    normed_ref[...] = (wide * pre_ref[...]).astype(BF16)

    def sent(buf, sem, device):
        block = buf.at[0, 0]
        remote(block, block, sem, sem, device).wait_send()

    def drain(head, carry):
        for _raw, buf, recv, sx, su, sd in both:
            for plane in range(nz):
                slot = plane * nx + x

                @pl.when(jnp.logical_and(has_up, z >= plane))
                def _(slot=slot):
                    sent(buf, su.at[slot, head], up)

                @pl.when(jnp.logical_and(has_down, z <= plane))
                def _(slot=slot):
                    sent(buf, sd.at[slot, head], down)

                for off in range(1, nx):
                    sent(buf, sx.at[slot, head, off], beside[off - 1])
        return carry

    lax.fori_loop(0, kv_heads, drain, 0)


def before(tokens):
    row = lax.broadcasted_iota(jnp.int32, (tokens, tokens), 0)
    col = lax.broadcasted_iota(jnp.int32, (tokens, tokens), 1)
    return (row < col).astype(F32).astype(BF16)


def group_choice(meta, first_expert, count, rows):
    tokens = meta.shape[1]
    low = first_expert.astype(F32)
    member = jnp.where((meta[0:1] >= low) & (meta[0:1] < low + float(count)), 1.0, 0.0)
    rank = jnp.dot(
        jnp.broadcast_to(member, (8, tokens)).astype(BF16),
        before(tokens),
        preferred_element_type=F32,
    )[0:1]
    place = lax.broadcasted_iota(jnp.int32, (rows, tokens), 0).astype(F32)
    return jnp.where(rank == place, 1.0, 0.0) * member


def slot_choice(meta, first_expert, count, cap):
    tokens = meta.shape[1]
    names = lax.broadcasted_iota(jnp.int32, (count, tokens), 0).astype(F32)
    names = names + first_expert.astype(F32)
    first = jnp.where(meta[0:1] == names, 1.0, 0.0)
    second = jnp.where(meta[1:2] == names, 1.0, 0.0)
    rank = jnp.dot((first + second).astype(BF16), before(tokens), preferred_element_type=F32)
    row = lax.broadcasted_iota(jnp.int32, (count * cap, count), 0)
    start = lax.broadcasted_iota(jnp.int32, (count * cap, count), 1) * cap
    widen = jnp.where((row >= start) & (row < start + cap), 1.0, 0.0).astype(BF16)

    def widened(values):
        return jnp.dot(widen, values.astype(BF16), preferred_element_type=F32)

    place = lax.broadcasted_iota(jnp.int32, (count * cap, tokens), 0) & (cap - 1)
    hit = jnp.where(widened(rank) == place.astype(F32), 1.0, 0.0)
    return widened(first) * hit, widened(second) * hit


def contract(left, right, dims):
    return lax.dot_general(
        left.astype(BF16), right.astype(BF16), ((dims[:1], dims[1:]), ((), ())),
        preferred_element_type=F32,
    )


def expert_kernel(
    nz, nx, n_dp,
    normed_ref, stream_ref, meta_ref, wg_hbm, wu_hbm, wd_hbm,
    out_ref,
    wg, wu, wd, w_sem, p1, r1, metas, p2, r2, o2, back, mix, fin,
    s1, t1, sm, tm, s2, t2, s3, t3, s4, t4,
):
    tokens, width = normed_ref.shape
    count, cap = p2.shape[1], p2.shape[2]
    rows = p1.shape[1]
    sp = lax.axis_index("sp")
    dp = lax.axis_index("dp")
    z, x = sp // nx, sp % nx
    me = x * n_dp + dp

    loads = [
        pltpu.make_async_copy(src, dst, w_sem.at[i])
        for i, (src, dst) in enumerate(((wg_hbm, wg), (wu_hbm, wu), (wd_hbm, wd)))
    ]
    for load in loads:
        load.start()

    def plane_peer(off):
        j = lax.rem(me + off, count)
        return j, (z * nx + j // n_dp, j % n_dp)

    def column_peer(dist):
        plane = lax.rem(z + dist, nz)
        return plane, (plane * nx + x, dp)

    barrier = pltpu.get_barrier_semaphore()
    for off in range(1, count):
        pl.semaphore_signal(barrier, inc=1, device_id=plane_peer(off)[1], device_id_type=MESH)
    for dist in range(1, nz):
        pl.semaphore_signal(barrier, inc=1, device_id=column_peer(dist)[1], device_id_type=MESH)

    meta = meta_ref[...]
    for g in range(nz):
        pick = group_choice(meta, jnp.int32(g * count), count, rows)
        p1[g] = contract(pick, normed_ref[...], (1, 0)).astype(BF16)
    metas[z] = meta
    r1[z] = p1[z]

    pl.semaphore_wait(barrier, count - 1 + nz - 1)
    for dist in range(1, nz):
        plane, device = column_peer(dist)
        remote(meta_ref, metas.at[z], sm.at[plane], tm.at[z], device).start()
        remote(p1.at[plane], r1.at[z], s1.at[plane], t1.at[z], device).start()

    first_expert = z * count

    def dispatch(dist, carry):
        source, device = column_peer(dist)

        @pl.when(dist > 0)
        def _():
            remote(meta_ref, metas.at[source], sm.at[source], tm.at[source], device).wait_recv()
            remote(p1.at[source], r1.at[source], s1.at[source], t1.at[source], device).wait_recv()

        got = metas[source]
        group = group_choice(got, first_expert, count, rows)
        first, second = slot_choice(got, first_expert, count, cap)
        pick = contract(first + second, group, (1, 1))
        packed = contract(pick, r1[source], (1, 0)).astype(BF16)
        p2[source] = packed.reshape(count, cap, width)
        r2[source, me] = p2[source, me]
        for off in range(1, count):
            j, device = plane_peer(off)
            remote(
                p2.at[source, j], r2.at[source, me], s2.at[source, j], t2.at[source, me], device
            ).start()
        return carry

    lax.fori_loop(0, nz, dispatch, 0)
    for load in loads:
        load.wait()

    def transform(dist, carry):
        source = lax.rem(z + dist + 1, nz)
        for off in range(1, count):
            j, device = plane_peer(off)
            remote(
                p2.at[source, j], r2.at[source, j], s2.at[source, j], t2.at[source, j], device
            ).wait_recv()
        arrived = r2[source].reshape(count * cap, width)
        gated = jnp.dot(arrived, wg[...], preferred_element_type=F32)
        lifted = jnp.dot(arrived, wu[...], preferred_element_type=F32)
        hidden = (gated / (1.0 + jnp.exp(-gated)) * lifted).astype(BF16)
        result = jnp.dot(hidden, wd[...], preferred_element_type=F32).astype(BF16)
        o2[source] = result.reshape(count, cap, width)
        back[source, me] = o2[source, me]
        for off in range(1, count):
            j, device = plane_peer(off)
            remote(
                o2.at[source, j], back.at[source, me], s3.at[source, j], t3.at[source, me], device
            ).start()
        return carry

    lax.fori_loop(0, nz, transform, 0)

    def combine(dist, carry):
        source, column = column_peer(dist + 1)
        for off in range(1, count):
            j, device = plane_peer(off)
            remote(
                o2.at[source, j], back.at[source, j], s3.at[source, j], t3.at[source, j], device
            ).wait_recv()
        got = metas[source]
        group = group_choice(got, first_expert, count, rows)
        first, second = slot_choice(got, first_expert, count, cap)
        outs = back[source].reshape(count * cap, width)
        one = contract(contract(group, first, (1, 1)), outs, (1, 0))
        two = contract(contract(group, second, (1, 1)), outs, (1, 0))
        weight = jnp.sum(group * got[2:3], axis=1, keepdims=True)
        share = jnp.sum(group * got[3:4], axis=1, keepdims=True)
        total = (weight * (share * one + (1.0 - share) * two)).astype(BF16)
        mix[source] = total

        @pl.when(dist == nz - 1)
        def _():
            fin[source] = total

        @pl.when(dist < nz - 1)
        def _():
            remote(mix.at[source], fin.at[z], s4.at[source], t4.at[z], column).start()

        return carry

    lax.fori_loop(0, nz, combine, 0)

    picks = [
        group_choice(meta, jnp.int32(g * count), count, rows) for g in range(nz)
    ]
    for dist in range(1, nz):
        plane, device = column_peer(dist)
        remote(mix.at[plane], fin.at[plane], s4.at[plane], t4.at[plane], device).wait_recv()
    every = jnp.concatenate(picks, axis=0)
    added = contract(every, fin[...].reshape(tokens, width), (0, 0))
    out_ref[...] = (stream_ref[...].astype(F32) + added).astype(BF16)

    for dist in range(1, nz):
        plane, device = column_peer(dist)
        remote(meta_ref, metas.at[z], sm.at[plane], tm.at[z], device).wait_send()
        remote(p1.at[plane], r1.at[z], s1.at[plane], t1.at[z], device).wait_send()
        remote(mix.at[plane], fin.at[z], s4.at[plane], t4.at[z], device).wait_send()

    def drain(source, carry):
        for off in range(1, count):
            j, device = plane_peer(off)
            remote(
                p2.at[source, j], r2.at[source, me], s2.at[source, j], t2.at[source, me], device
            ).wait_send()
            remote(
                o2.at[source, j], back.at[source, me], s3.at[source, j], t3.at[source, me], device
            ).wait_send()
        return carry

    lax.fori_loop(0, nz, drain, 0)


def local(
    residual_in, query_proj, key_proj, value_proj, query_gain, key_gain, out_weight, post_gain,
    pre_gain, route_ids, group_weight, first_share, gate_weight, up_weight, down_weight,
):
    n_sp = lax.axis_size("sp")
    n_dp = lax.axis_size("dp")
    tokens, width = query_proj.shape[1:]
    kv_width = key_proj.shape[2]
    heads, kv_heads = width // HEAD_DIM, kv_width // HEAD_DIM
    nz = GROUPS
    nx = n_sp // nz
    length = n_sp * tokens
    cos, sin = angle_tables(length)
    vmem = pl.BlockSpec(memory_space=pltpu.VMEM)
    hbm = pl.BlockSpec(memory_space=pl.ANY)
    dma = pltpu.SemaphoreType.DMA
    row = jax.ShapeDtypeStruct((tokens, width), BF16)
    stream, normed = pl.pallas_call(
        functools.partial(attention_kernel, nz, nx),
        out_shape=(row, row),
        in_specs=[vmem] * 10 + [hbm],
        out_specs=(vmem, vmem),
        scratch_shapes=[
            pltpu.VMEM((n_sp, kv_heads, tokens, HEAD_DIM), BF16),
            pltpu.VMEM((n_sp, kv_heads, tokens, HEAD_DIM), BF16),
            pltpu.VMEM((heads, tokens, HEAD_DIM), BF16),
            pltpu.VMEM((length, HEAD_DIM), BF16),
            pltpu.VMEM((tokens, width // kv_heads), BF16),
            pltpu.VMEM((tokens, width), F32),
            pltpu.VMEM((width, width), BF16),
            dma,
            dma((n_sp, kv_heads)), dma((n_sp, kv_heads)),
            dma((n_sp, kv_heads, nx)), dma((n_sp, kv_heads)), dma((n_sp, kv_heads)),
            dma((n_sp, kv_heads, nx)), dma((n_sp, kv_heads)), dma((n_sp, kv_heads)),
        ],
        compiler_params=pltpu.CompilerParams(
            collective_id=0, has_side_effects=True, vmem_limit_bytes=VMEM_LIMIT
        ),
        name="attention",
    )(
        query_proj[0], key_proj[0], value_proj[0],
        query_gain.reshape(1, -1), key_gain.reshape(1, -1),
        jnp.asarray(cos), jnp.asarray(sin),
        residual_in[0], post_gain.reshape(1, -1), pre_gain.reshape(1, -1), out_weight,
    )

    experts = gate_weight.shape[0] * n_sp * n_dp
    count = experts // nz
    cap = max(16, 4 * tokens // experts)
    rows = tokens // nz
    ff = gate_weight.shape[2]
    meta = jnp.concatenate(
        [route_ids[0].T.astype(F32), group_weight, first_share, jnp.zeros((4, tokens), F32)], axis=0
    )
    blocks = pltpu.VMEM((nz, count, cap, width), BF16)
    lines = pltpu.VMEM((nz, rows, width), BF16)
    out = pl.pallas_call(
        functools.partial(expert_kernel, nz, nx, n_dp),
        out_shape=row,
        in_specs=[vmem] * 3 + [hbm] * 3,
        out_specs=vmem,
        scratch_shapes=[
            pltpu.VMEM((width, ff), BF16),
            pltpu.VMEM((width, ff), BF16),
            pltpu.VMEM((ff, width), BF16),
            dma((3,)),
            lines, lines,
            pltpu.VMEM((nz, 8, tokens), F32),
            blocks, blocks, blocks, blocks,
            lines, lines,
            dma((nz,)), dma((nz,)), dma((nz,)), dma((nz,)),
            dma((nz, count)), dma((nz, count)), dma((nz, count)), dma((nz, count)),
            dma((nz,)), dma((nz,)),
        ],
        compiler_params=pltpu.CompilerParams(
            collective_id=1, has_side_effects=True, vmem_limit_bytes=VMEM_LIMIT
        ),
        name="experts",
    )(normed, stream, meta, gate_weight[0], up_weight[0], down_weight[0])
    return out.reshape(1, tokens, width)


def layer_kernel(
    nz, nx, cores,
    q_hbm, k_hbm, v_hbm, qg_hbm, kg_hbm, res_hbm, post_hbm, pre_hbm, route_hbm, gw_hbm, fs_hbm,
    cos_hbm, sin_hbm, ow_hbm, wg_hbm, wu_hbm, wd_hbm,
    out_hbm,
    q_ref, k_ref, v_ref, qg_ref, kg_ref, res_ref, post_ref, pre_ref, route_ref, gw_ref, fs_ref,
    cos, sin, ow, wg, wu, wd, load_sem,
    kv, q_rot, att, acc,
    rk_own, rk_x, rk_z, kv_x_sent, kv_z_sent,
    perm, perm_back, mrow, metas, picks, weights, backs,
    zs_sem, zr_sem, ms_sem, mr_sem,
    stream, srt, rows, y, other, part, relay, direct, summed, fin, out, out_sem,
    t_z, t_a, t_b, t_c, t_d, t_core, spread_sent,
    t_other, t_up, t_side, t_last, t_home, back_sent,
):
    tokens, width = q_ref.shape
    heads = width // HEAD_DIM
    kv_heads = k_ref.shape[1] // HEAD_DIM
    group = heads // kv_heads
    slots_kv = nz * nx
    length = slots_kv * tokens
    last_head = kv_heads - 1
    chips = metas.shape[2]
    count = chips * cores
    block = tokens // nz
    cap = y.shape[2] // chips
    half = block // 2
    me = lax.axis_index("sp")
    dp = lax.axis_index("dp")
    z, x = me // nx, me % nx
    side, core = dp // cores, dp % cores
    up, down = (me + nx, dp), (me - nx, dp)
    beside = (z * nx + 1 - x, dp)
    across = (me, (1 - side) * cores + core)
    partner = (me, side * cores + 1 - core)
    has_up, has_down = z < nz - 1, z > 0
    sides = chips // nx
    mine = x * sides + side
    chip_x, chip_y = (1 - x) * sides + side, x * sides + 1 - side
    chip_d = (1 - x) * sides + 1 - side

    def column(plane):
        return (plane * nx + x, dp)

    flip = z >= nz // 2
    low = jnp.where(flip, nz - 1 - z, z)
    inner = (2, 0, 3)

    def source_of(i):
        if i == 0:
            return z
        near = jnp.where(low == 0, i, inner[i - 1])
        return jnp.where(flip, nz - 1 - near, near)

    sources = [source_of(i) for i in range(nz)]

    barrier = pltpu.get_barrier_semaphore()
    greeted = [column(lax.rem(z + dist, nz)) for dist in range(1, nz)] + [beside, across, partner]
    for device in greeted:
        pl.semaphore_signal(barrier, inc=1, device_id=device, device_id_type=MESH)

    own = pl.multiple_of(me * tokens, tokens)
    loads = [
        pltpu.make_async_copy(src, dst, load_sem.at[i])
        for i, (src, dst) in enumerate((
            (k_hbm, k_ref), (v_hbm, v_ref), (kg_hbm, kg_ref),
            (cos_hbm.at[pl.ds(own, tokens)], cos), (sin_hbm.at[pl.ds(own, tokens)], sin),
            (q_hbm, q_ref), (qg_hbm, qg_ref), (route_hbm, route_ref), (gw_hbm, gw_ref),
            (fs_hbm, fs_ref), (ow_hbm, ow), (res_hbm, res_ref), (post_hbm, post_ref),
            (pre_hbm, pre_ref), (wg_hbm, wg), (wu_hbm, wu), (wd_hbm, wd),
        ))
    ]
    for load in loads:
        load.start()

    for load in loads[:5]:
        load.wait()
    for head in range(kv_heads):
        columns = slice(head * HEAD_DIM, (head + 1) * HEAD_DIM)
        kv[head * slots_kv + me, 1] = v_ref[:, columns]
        kv[head * slots_kv + me, 0] = rotate(k_ref[:, columns], kg_ref[...], cos[...], sin[...])

    pl.semaphore_wait(barrier, len(greeted))

    def hop(slot, head, device, sent, landed):
        view = kv.at[head * slots_kv + slot]
        return remote(view, view, sent.at[0], landed, device)

    def bytes_of(units, sent, landed):
        view = kv.at[pl.ds(0, units)]
        return remote(view, view, sent, landed, beside)

    def own_beside(head):
        return hop(me, head, beside, kv_x_sent, rk_own.at[head])

    def pass_beside(slot, head):
        return hop(slot, head, beside, kv_x_sent, rk_x.at[head])

    def pass_on(slot, source, head, device):
        return hop(slot, head, device, kv_z_sent, rk_z.at[source, head])

    def cross_on(head, device):
        return hop(z * nx + 1 - x, head, device, kv_z_sent, rk_x.at[head])

    late_up, late_down = z == nz - 2, z == 1
    at_end = jnp.logical_or(z == 0, z == nz - 1)

    def send_own(head):
        final = head == last_head
        own_beside(head).start()
        for on, late, device in ((has_up, late_up, up), (has_down, late_down, down)):
            @pl.when(on & ~late if final else on)
            def _(device=device):
                pass_on(me, z, head, device).start()

    def take_own(head):
        bytes_of(1, kv_x_sent.at[0], rk_own.at[head]).wait_recv()

    def crosses(head):
        return head % 2 == 1

    def cross(head):
        final = head == last_head
        take_own(head)
        for on, late, device in ((has_up, late_up, up), (has_down, late_down, down)):
            @pl.when(on & ~late if final else on)
            def _(device=device):
                cross_on(head, device).start()

    def relay_kv(head, dist, given=True):
        for below in (True, False):
            source = z - dist if below else z + dist
            present = source >= 0 if below else source < nz
            further = has_up if below else has_down
            onward = up if below else down

            @pl.when(present & given)
            def _(source=source, further=further, onward=onward):
                slot = source * nx + x
                bytes_of(1, kv_z_sent.at[0], rk_z.at[source, head]).wait_recv()

                @pl.when(further)
                def _():
                    pass_on(slot, source, head, onward).start()

                if dist > 1 or not crosses(head):
                    pass_beside(slot, head).start()

    def send_late(head):
        for late, device in ((late_up, up), (late_down, down)):
            @pl.when(late)
            def _(device=device):
                pass_on(me, z, head, device).start()
                if crosses(head):
                    cross_on(head, device).start()

    def wave(step):
        for dist in range(1, nz):
            head = step - (dist - 1)
            if 0 <= head < kv_heads:
                relay_kv(head, dist, ~at_end if head == last_head and dist == 1 else True)
                if dist == 1 and crosses(head):
                    cross(head)
        if step == kv_heads + nz - 4:
            send_late(last_head)
        if step + 2 < kv_heads:
            send_own(step + 2)

    for head in range(2):
        send_own(head)

    for load in loads[5:10]:
        load.wait()
    for head in range(heads):
        q_rot[head] = rotate(
            q_ref[:, head * HEAD_DIM : (head + 1) * HEAD_DIM], qg_ref[...], cos[...], sin[...]
        )
    acc[...] = jnp.zeros_like(acc)

    row = lax.broadcasted_iota(jnp.int32, (tokens, tokens), 0)
    lane = lax.broadcasted_iota(jnp.int32, (tokens, tokens), 1)

    def routing():
        first = route_ref[0:1].astype(F32)
        second = route_ref[1:2].astype(F32)
        of_lane = jnp.zeros_like(first)
        for g in range(1, nz):
            of_lane = of_lane + jnp.where(first >= float(g * count), 1.0, 0.0)
        of = jnp.sum(jnp.where(row == lane, of_lane, 0.0), axis=1, keepdims=True)
        same = of == of_lane
        rank = jnp.sum(jnp.where(same & (lane < row), 1.0, 0.0), axis=1, keepdims=True)
        rank_lane = jnp.sum(jnp.where(same & (row < lane), 1.0, 0.0), axis=0, keepdims=True)
        place = (of * float(block) + rank).astype(jnp.int32)
        place_lane = (of_lane * float(block) + rank_lane).astype(jnp.int32)
        perm[...] = jnp.where(row == place_lane, 1.0, 0.0).astype(BF16)
        perm_back[...] = jnp.where(place == lane, 1.0, 0.0).astype(BF16)
        fields = (
            first, second,
            gw_ref[...] * fs_ref[...], gw_ref[...] * (1.0 - fs_ref[...]),
        )
        chosen = lax.broadcasted_iota(jnp.int32, (8, tokens), 0).astype(F32) == of_lane
        at = rank.astype(jnp.int32)
        table = jnp.zeros((8, tokens), F32)
        for f, field in enumerate(fields):
            spread = jnp.where(lane == at + f * block, 1.0, 0.0)
            table += lax.dot_general(
                jnp.where(chosen, field, 0.0), spread, (((1,), (0,)), ((), ())),
                precision=lax.Precision.HIGHEST, preferred_element_type=F32,
            )
        for g in range(nz):
            mrow[g] = table[g : g + 1]

    routing()
    metas[z, core, mine] = mrow[z]

    def meta_column(dist):
        plane = lax.rem(z + dist, nz)
        return remote(
            mrow.at[plane], metas.at[z, core, mine], zs_sem.at[0], zr_sem.at[0], column(plane)
        )

    def meta_all():
        view = mrow.at[pl.ds(0, nz - 1)]
        return remote(view, view, zs_sem.at[0], zr_sem.at[0], beside)

    for dist in range(1, nz):
        meta_column(dist).start()

    def meta_copy(view, step, device):
        return remote(view, view, ms_sem.at[step], mr_sem.at[step], device)

    pair = pl.ds(x * sides, sides)
    other_pair = pl.ds((1 - x) * sides, sides)
    meta_sends = (
        meta_copy(metas.at[:, core, mine], 0, across),
        meta_copy(metas.at[:, core, pair], 1, partner),
        meta_copy(metas.at[:, :, pair], 2, beside),
    )
    meta_recvs = (
        meta_copy(metas.at[:, core, chip_y], 0, across),
        meta_copy(metas.at[:, 1 - core, pair], 1, partner),
        meta_copy(metas.at[:, :, other_pair], 2, beside),
    )

    def choice(plane, of_core, expert):
        table = metas[plane, of_core].reshape(chips, tokens)
        first = table[:, 0:block] == expert
        second = table[:, block : 2 * block] == expert
        member = jnp.where(first | second, 1.0, 0.0)
        weight = jnp.where(first, table[:, 2 * block : 3 * block], 0.0)
        weight = weight + jnp.where(second, table[:, 3 * block : 4 * block], 0.0)
        r = lax.broadcasted_iota(jnp.int32, (block, block), 0)
        c = lax.broadcasted_iota(jnp.int32, (block, block), 1)
        earlier = jnp.where(r < c, 1.0, 0.0).astype(BF16)
        rank = jnp.dot(
            jnp.concatenate([member] * (8 // chips), axis=0).astype(BF16), earlier,
            preferred_element_type=F32,
        )[:chips]
        place = lax.broadcasted_iota(jnp.int32, (chips, cap, block), 1).astype(F32)
        hit = jnp.where(rank[:, None, :] == place, 1.0, 0.0) * member[:, None, :]
        of_slot = jnp.sum(hit * weight[:, None, :], axis=2, keepdims=True).reshape(chips * cap, 1)
        flat = hit.reshape(chips * cap, block).astype(BF16)
        wide_row = lax.broadcasted_iota(jnp.int32, (block, tokens), 0)
        wide_lane = lax.broadcasted_iota(jnp.int32, (block, tokens), 1)
        widen = jnp.where(lax.rem(wide_lane, block) == wide_row, 1.0, 0.0).astype(BF16)
        spread = jnp.dot(flat, widen, preferred_element_type=F32)
        slot = lax.broadcasted_iota(jnp.int32, (chips * cap, tokens), 0) // cap
        chip = lax.broadcasted_iota(jnp.int32, (chips * cap, tokens), 1) // block
        return jnp.where(slot == chip, spread, 0.0), of_slot

    def tables():
        expert = (z * count + x * (count // nx) + dp).astype(F32)
        twin = (z * count + x * (count // nx) + side * cores + 1 - core).astype(F32)

        def one_plane(plane, carry):
            for of_core in range(cores):
                pick, of_slot = choice(plane, of_core, expert)
                picks[plane, of_core] = pick.astype(BF16)
                weights[plane, of_core] = of_slot
            back, _ = choice(plane, core, expert)
            theirs, _ = choice(plane, core, twin)
            backs[plane] = jnp.concatenate([back, theirs], axis=0).T.astype(BF16)
            return carry

        lax.fori_loop(0, nz, one_plane, 0)

    factor = float(HEAD_DIM**-0.5 * np.log2(np.e))
    span = group * HEAD_DIM

    def attend(head):
        here = pl.ds(head * slots_kv, slots_kv)
        keys = kv[here, 0].reshape(length, HEAD_DIM)
        values = kv[here, 1].reshape(length, HEAD_DIM)
        for member in range(group):
            scores = lax.dot_general(
                q_rot[head * group + member], keys, (((1,), (1,)), ((), ())),
                preferred_element_type=F32,
            )
            top = jnp.max(scores, axis=-1, keepdims=True)
            raised = jnp.exp2((scores - top) * factor)
            total = jnp.sum(raised, axis=-1, keepdims=True)
            mixed = jnp.dot(raised.astype(BF16), values, preferred_element_type=F32)
            att[:, member * HEAD_DIM : (member + 1) * HEAD_DIM] = (mixed / total).astype(BF16)
        above = ow.at[pl.ds(pl.multiple_of(head * span, span), span), :]
        tile = 1024
        for start in range(0, width, tile):
            columns = slice(start, start + tile)
            acc[:, columns] += jnp.dot(att[...], above[:, columns], preferred_element_type=F32)

    wave(0)
    wave(1)
    meta_all().wait_recv()
    meta_sends[0].start()
    wave(2)
    meta_recvs[0].wait_recv()
    meta_sends[1].start()
    meta_recvs[1].wait_recv()
    meta_sends[2].start()
    loads[10].wait()
    wave(3)
    wave(4)

    def one_head(head, carry):
        @pl.when(head == 1)
        def _():
            wave(5)

        @pl.when(head == 2)
        def _():
            relay_kv(last_head, 1, at_end)

        @pl.when(lax.rem(head, 2) == 0)
        def _():
            take_own(head)

        bytes_of(nz - 1, kv_x_sent.at[0], rk_x.at[head]).wait_recv()
        attend(head)
        return carry

    lax.fori_loop(0, kv_heads, one_head, 0)
    for load in loads[11:14]:
        load.wait()

    blend = acc[...].astype(BF16).astype(F32)
    blend = blend * lax.rsqrt(jnp.mean(blend * blend, axis=-1, keepdims=True) + EPSILON)
    flow = (res_ref[...].astype(F32) + blend * post_ref[...]).astype(BF16)
    stream[...] = flow
    wide = flow.astype(F32)
    wide = wide * lax.rsqrt(jnp.mean(wide * wide, axis=-1, keepdims=True) + EPSILON)
    normed = (wide * pre_ref[...]).astype(BF16)
    srt[...] = jnp.dot(perm[...], normed, preferred_element_type=F32).astype(BF16).reshape(srt.shape)

    def unit(s, of_core, chip, h=0):
        return ((s * cores + of_core) * chips + chip) * 2 + h

    def units(first, amount):
        return rows.at[pl.ds(first, amount)]

    def waiting(amount, landed):
        return remote(units(0, amount), units(0, amount), spread_sent.at[0], landed, partner)

    def z_send(plane):
        return remote(
            srt.at[pl.ds(2 * plane, 2)], units(unit(z, core, mine), 2), spread_sent.at[0], t_z.at[z],
            column(plane),
        )

    z_send(sources[1]).start()

    @pl.when(~at_end)
    def _():
        z_send(sources[2]).start()

    rows[pl.ds(unit(z, core, mine), 2)] = srt[pl.ds(2 * z, 2)]

    def over(s, chip, h, landed, device):
        view = rows.at[unit(s, core, chip, h)]
        return remote(view, view, spread_sent.at[0], landed.at[s], device)

    def over_core(s, chip):
        view = units(unit(s, core, chip), 2)
        return remote(view, view, spread_sent.at[0], t_core.at[s], partner)

    def route_tables(i):
        z_send(jnp.where(at_end, sources[2], sources[3])).start()
        meta_recvs[2].wait_recv()
        tables()

    def send_far(i):
        @pl.when(at_end)
        def _():
            z_send(sources[i]).start()

    def spread_own(i):
        s = sources[i]
        if i > 0:
            waiting(2, t_z.at[s]).wait_recv()
        over(s, mine, 0, t_a, beside).start()
        over(s, mine, 1, t_b, across).start()
        over(s, mine, 1, t_c, beside).start()
        over(s, mine, 0, t_c, across).start()
        over_core(s, mine).start()

    def spread_on(i):
        s = sources[i]
        waiting(1, t_a.at[s]).wait_recv()
        over(s, chip_x, 0, t_d, across).start()
        waiting(1, t_b.at[s]).wait_recv()
        over(s, chip_y, 1, t_d, beside).start()

    def spread_core(i):
        s = sources[i]
        waiting(2, t_c.at[s]).wait_recv()
        over_core(s, chip_x).start()
        over_core(s, chip_y).start()

    def spread_last(i):
        s = sources[i]
        waiting(2, t_d.at[s]).wait_recv()
        over_core(s, chip_d).start()

    def to_partner(s):
        return remote(y.at[s, 1 - core], other.at[s], back_sent.at[0], t_other.at[s], partner)

    def transform(i):
        s = sources[i]
        waiting(2 * chips, t_core.at[s]).wait_recv()
        packed = [
            jnp.dot(
                picks[s, q], rows[pl.ds(unit(s, q, 0), 2 * chips)].reshape(tokens, width), preferred_element_type=F32
            ).astype(BF16)
            for q in range(cores)
        ]
        packed = jnp.concatenate(packed, axis=0)
        gated = jnp.dot(packed, wg[...], preferred_element_type=F32)
        lifted = jnp.dot(packed, wu[...], preferred_element_type=F32)
        hidden = (gated / (1.0 + jnp.exp(-gated)) * lifted).astype(BF16)
        result = jnp.dot(hidden, wd[...], preferred_element_type=F32)
        slots = chips * cap
        for q in range(cores):
            y[s, q] = (result[q * slots : (q + 1) * slots] * weights[s, q]).astype(BF16)
        to_partner(s).start()

    def back(s, chip, h, into, at, landed, device):
        return remote(
            part.at[s, chip, halves[h]], into.at[s, at], back_sent.at[0], landed.at[s], device
        )

    halves = (pl.ds(0, half), pl.ds(half, half))

    def gather_back(i):
        s = sources[i]
        to_partner(s).wait_recv()
        outs = jnp.concatenate([y[s, core], other[s]], axis=0)
        part[s] = jnp.dot(backs[s], outs, preferred_element_type=F32).astype(BF16).reshape(
            chips, block, width
        )
        back(s, chip_d, 0, relay, 0, t_up, across).start()
        back(s, chip_d, 1, relay, 1, t_side, beside).start()
        back(s, chip_x, 1, direct, 1, t_last, beside).start()
        back(s, chip_y, 0, direct, 0, t_last, across).start()

    def add(left, right):
        return (left.astype(F32) + right.astype(F32)).astype(BF16)

    def pass_back(i):
        s = sources[i]
        waiting(1, t_up.at[s]).wait_recv()
        part[s, chip_x, halves[0]] = add(part[s, chip_x, halves[0]], relay[s, 0])
        back(s, chip_x, 0, summed, 0, t_last, beside).start()
        waiting(1, t_side.at[s]).wait_recv()
        part[s, chip_y, halves[1]] = add(part[s, chip_y, halves[1]], relay[s, 1])
        back(s, chip_y, 1, summed, 1, t_last, across).start()

    def home(s):
        return remote(part.at[s, mine], fin.at[z], back_sent.at[0], t_home.at[0], column(s))

    def finish(i):
        s = sources[i]
        waiting(4, t_last.at[s]).wait_recv()
        for h in range(2):
            total = part[s, mine, halves[h]].astype(F32) + direct[s, h].astype(F32)
            total = (total + summed[s, h].astype(F32)).astype(BF16)
            if i > 0:
                part[s, mine, halves[h]] = total
            else:
                fin[s, halves[h]] = total
        if i > 0:
            home(s).start()

    def weights_ready(i):
        for load in loads[14:]:
            load.wait()

    for stage, i in plan(
        route_tables, send_far, spread_own, spread_on, spread_core, spread_last, weights_ready, transform, gather_back, pass_back, finish
    ):
        stage(i)

    waiting(2 * (nz - 1), t_home.at[0]).wait_recv()
    tile = width // 4
    stores = []
    for n, start in enumerate(range(0, width, tile)):
        columns = slice(start, start + tile)
        added = jnp.dot(
            perm_back[...], fin[:, :, columns].reshape(tokens, tile), preferred_element_type=F32
        )
        out[:, columns] = (stream[:, columns].astype(F32) + added).astype(BF16)
        store = pltpu.make_async_copy(out.at[:, columns], out_hbm.at[:, columns], out_sem.at[n])
        store.start()
        stores.append(store)

    for plane in range(nz):
        lanes = sum(head % 2 for head in range(kv_heads))
        upward = (plane + 1) * kv_heads + lanes if plane < nz - 1 else 0
        downward = (nz - plane) * kv_heads + lanes if plane > 0 else 0
        sideways = nz * kv_heads - lanes * sum(0 <= plane + d < nz for d in (-1, 1))

        @pl.when(z == plane)
        def _(vertical=upward + downward, sideways=sideways):
            bytes_of(vertical, kv_z_sent.at[0], rk_own.at[0]).wait_send()
            bytes_of(sideways, kv_x_sent.at[0], rk_own.at[0]).wait_send()

    meta_all().wait_send()
    for send in meta_sends:
        send.wait_send()
    spread_units = 2 * (nz - 1) + nz * (6 + 2 * chips)
    waiting(spread_units, t_core.at[0]).wait_send()
    back_units = nz * (2 * chips * cap // block + 6) + 2 * (nz - 1)
    returned = units(0, back_units)
    remote(returned, returned, back_sent.at[0], t_core.at[0], partner).wait_send()
    for store in stores:
        store.wait()


def plan(route, far, own, on, share, last, ready, transform, gather_back, pass_back, finish):
    return (
        (own, 0), (route, 0), (far, 3), (on, 0), (own, 1), (share, 0), (on, 1), (own, 2),
        (last, 0), (share, 1), (ready, 0), (transform, 0), (on, 2), (own, 3), (last, 1),
        (share, 2), (transform, 1), (on, 3), (gather_back, 1), (last, 2), (transform, 2),
        (share, 3), (gather_back, 2), (last, 3), (pass_back, 1), (transform, 3), (pass_back, 2),
        (finish, 1), (gather_back, 3), (finish, 2), (pass_back, 3), (gather_back, 0),
        (finish, 3), (pass_back, 0), (finish, 0),
    )


def fused(
    residual_in, query_proj, key_proj, value_proj, query_gain, key_gain, out_weight, post_gain,
    pre_gain, route_ids, group_weight, first_share, gate_weight, up_weight, down_weight,
):
    n_sp = lax.axis_size("sp")
    n_dp = lax.axis_size("dp")
    tokens, width = query_proj.shape[1:]
    kv_heads = key_proj.shape[2] // HEAD_DIM
    heads = width // HEAD_DIM
    nz = GROUPS
    nx = n_sp // nz
    cores = 2
    chips = nx * (n_dp // cores)
    experts = gate_weight.shape[0] * n_sp * n_dp
    cap = max(16, 4 * tokens // experts)
    block = tokens // nz
    slots = chips * cap
    ff = gate_weight.shape[2]
    length = n_sp * tokens
    cos, sin = angle_tables(length)
    vmem = pl.BlockSpec(memory_space=pltpu.VMEM)
    hbm = pl.BlockSpec(memory_space=pl.ANY)
    dma = pltpu.SemaphoreType.DMA

    def buf(*shape, kind=BF16):
        return pltpu.VMEM(shape, kind)

    out = pl.pallas_call(
        functools.partial(layer_kernel, nz, nx, cores),
        out_shape=jax.ShapeDtypeStruct((tokens, width), BF16),
        in_specs=[hbm] * 17,
        out_specs=hbm,
        scratch_shapes=[
            buf(tokens, width), buf(tokens, kv_heads * HEAD_DIM), buf(tokens, kv_heads * HEAD_DIM),
            buf(1, HEAD_DIM, kind=F32), buf(1, HEAD_DIM, kind=F32), buf(tokens, width),
            buf(1, width, kind=F32), buf(1, width, kind=F32),
            buf(2, tokens, kind=jnp.int32), buf(1, tokens, kind=F32), buf(1, tokens, kind=F32),
            buf(tokens, HEAD_DIM, kind=F32), buf(tokens, HEAD_DIM, kind=F32),
            buf(width, width), buf(width, ff), buf(width, ff), buf(ff, width),
            dma((17,)),
            buf(kv_heads * n_sp, 2, tokens, HEAD_DIM),
            buf(heads, tokens, HEAD_DIM),
            buf(tokens, width // kv_heads),
            buf(tokens, width, kind=F32),
            dma((kv_heads,)), dma((kv_heads,)), dma((nz, kv_heads)), dma((1,)), dma((1,)),
            buf(tokens, tokens), buf(tokens, tokens),
            buf(nz, 1, tokens, kind=F32), buf(nz, cores, chips, 1, tokens, kind=F32),
            buf(nz, cores, slots, tokens), buf(nz, cores, slots, 1, kind=F32),
            buf(nz, tokens, cores * slots),
            dma((1,)), dma((1,)), dma((3,)), dma((3,)),
            buf(tokens, width), buf(2 * nz, block // 2, width),
            buf(nz * cores * chips * 2, block // 2, width),
            buf(nz, cores, slots, width), buf(nz, slots, width),
            buf(nz, chips, block, width),
            buf(nz, 2, block // 2, width), buf(nz, 2, block // 2, width),
            buf(nz, 2, block // 2, width), buf(nz, block, width),
            buf(tokens, width), dma((4,)),
            dma((nz,)), dma((nz,)), dma((nz,)), dma((nz,)), dma((nz,)), dma((nz,)), dma((1,)),
            dma((nz,)), dma((nz,)), dma((nz,)), dma((nz,)), dma((1,)), dma((1,)),
        ],
        compiler_params=pltpu.CompilerParams(
            collective_id=0, has_side_effects=True, vmem_limit_bytes=VMEM_LIMIT
        ),
        name="layer",
    )(
        query_proj[0], key_proj[0], value_proj[0],
        query_gain.reshape(1, -1), key_gain.reshape(1, -1),
        residual_in[0], post_gain.reshape(1, -1), pre_gain.reshape(1, -1),
        route_ids[0].T, group_weight, first_share,
        jnp.asarray(cos), jnp.asarray(sin), out_weight,
        gate_weight[0], up_weight[0], down_weight[0],
    )
    return out.reshape(1, tokens, width)


def solution(mesh):
    tok3 = P("dp", "sp", None)
    tok2 = P("dp", "sp")
    weight = P(("sp", "dp"), None, None)
    placed = (
        tok3, tok3, tok3, tok3, P(), P(), P(), P(), P(), tok3, tok2, tok2, weight, weight, weight,
    )
    small = mesh.shape["sp"] == 2 * GROUPS and mesh.shape["dp"] == 4
    return jax.shard_map(
        fused if small else local, mesh=mesh, in_specs=placed, out_specs=P("dp", "sp", None), check_vma=False
    )
```

```python
import functools

import jax
import jax.numpy as jnp
import numpy as np
from jax import lax
from jax.experimental import pallas as pl
from jax.experimental.pallas import tpu as pltpu
from jax.sharding import PartitionSpec as P

HEAD_DIM = 128
GRID_W = 64
GROUPS = 4
EPSILON = 1e-06
MESH = pl.DeviceIdType.MESH
VMEM_LIMIT = 60 * 1024 * 1024
F32 = jnp.float32
BF16 = jnp.bfloat16


def angle_tables(length):
    quarter = HEAD_DIM // 4
    inverse = 10000.0 ** (-np.arange(quarter, dtype=np.float64) / quarter)
    positions = np.arange(length)
    rows = (positions // GRID_W)[:, None] * inverse
    cols = (positions % GRID_W)[:, None] * inverse
    angles = np.concatenate([rows, rows, cols, cols], axis=-1)
    sign = np.where(np.arange(HEAD_DIM) % (2 * quarter) < quarter, -1.0, 1.0)
    return np.cos(angles).astype(np.float32), (np.sin(angles) * sign).astype(np.float32)


def rotate(raw, gain, cos, sin):
    floats = raw.astype(F32)
    normed = floats * lax.rsqrt(jnp.mean(floats * floats, axis=-1, keepdims=True) + EPSILON) * gain
    quarter = HEAD_DIM // 4
    lane = lax.broadcasted_iota(jnp.int32, normed.shape, 1)
    turned = jnp.where(
        (lane & (2 * quarter - 1)) < quarter,
        pltpu.roll(normed, HEAD_DIM - quarter, 1),
        pltpu.roll(normed, quarter, 1),
    )
    return (normed * cos + turned * sin).astype(BF16)


def remote(src, dst, send_sem, recv_sem, device):
    return pltpu.make_async_remote_copy(
        src_ref=src,
        dst_ref=dst,
        send_sem=send_sem,
        recv_sem=recv_sem,
        device_id=device,
        device_id_type=MESH,
    )


def attention_kernel(
    nz, nx,
    q_ref, k_ref, v_ref, qg_ref, kg_ref, cos_ref, sin_ref, res_ref, post_ref, pre_ref, ow_hbm,
    stream_ref, normed_ref,
    k_all, v_all, q_rot, k_rot, att, acc, ow, ow_sem,
    rk, rv, skx, sku, skd, svx, svu, svd,
):
    tokens, width = q_ref.shape
    heads = width // HEAD_DIM
    kv_heads = k_ref.shape[1] // HEAD_DIM
    group = heads // kv_heads
    me = lax.axis_index("sp")
    dp = lax.axis_index("dp")
    z, x = me // nx, me % nx
    up, down = (me + nx, dp), (me - nx, dp)
    has_up, has_down = z < nz - 1, z > 0
    both = ((k_ref, k_all, rk, skx, sku, skd), (v_ref, v_all, rv, svx, svu, svd))

    load_ow = pltpu.make_async_copy(ow_hbm, ow, ow_sem)
    load_ow.start()

    barrier = pltpu.get_barrier_semaphore()
    around = [(lax.rem(z + 1, nz) * nx + x, dp), (lax.rem(z + nz - 1, nz) * nx + x, dp)]
    beside = [(z * nx + lax.rem(x + off, nx), dp) for off in range(1, nx)]
    for device in around + beside:
        pl.semaphore_signal(barrier, inc=1, device_id=device, device_id_type=MESH)
    pl.semaphore_wait(barrier, len(around) + len(beside))

    def lanes_of(head):
        return pl.ds(pl.multiple_of(head * HEAD_DIM, HEAD_DIM), HEAD_DIM)

    def hop(src, buf, recv, send, slot, head, device):
        return remote(src, buf.at[slot, head], send, recv.at[slot, head], device)

    def send_own(head):
        for raw, buf, recv, sx, su, sd in both:
            src = raw.at[:, lanes_of(head)]

            @pl.when(has_up)
            def _():
                hop(src, buf, recv, su.at[me, head], me, head, up).start()

            @pl.when(has_down)
            def _():
                hop(src, buf, recv, sd.at[me, head], me, head, down).start()

        for raw, buf, recv, sx, su, sd in both:
            src = raw.at[:, lanes_of(head)]
            for off in range(1, nx):
                hop(src, buf, recv, sx.at[me, head, off], me, head, beside[off - 1]).start()

    def arrived(buf, recv, slot, head):
        block = buf.at[slot, head]
        remote(block, block, recv.at[slot, head], recv.at[slot, head], up).wait_recv()

    def relay(head):
        for dist in range(1, nz):
            for below in (True, False):
                source = z - dist if below else z + dist
                present = source >= 0 if below else source < nz
                further = has_up if below else has_down
                onward = up if below else down

                @pl.when(present)
                def _(source=source, below=below, further=further, onward=onward):
                    slot = source * nx + x
                    for _raw, buf, recv, sx, su, sd in both:
                        arrived(buf, recv, slot, head)
                        src = buf.at[slot, head]
                        send = su if below else sd

                        @pl.when(further)
                        def _(src=src, buf=buf, recv=recv, send=send):
                            hop(src, buf, recv, send.at[slot, head], slot, head, onward).start()

                        for off in range(1, nx):
                            hop(
                                src, buf, recv, sx.at[slot, head, off], slot, head,
                                beside[off - 1],
                            ).start()

    length = nz * nx * tokens
    factor = float(HEAD_DIM**-0.5 * np.log2(np.e))
    span = group * HEAD_DIM

    def attend(kv):
        for plane in range(nz):
            for off in range(1, nx):
                slot = plane * nx + lax.rem(x + off, nx)
                arrived(k_all, rk, slot, kv)
                arrived(v_all, rv, slot, kv)
        k_all[me, kv] = k_ref[:, lanes_of(kv)]
        v_all[me, kv] = v_ref[:, lanes_of(kv)]

        def place(slot, carry):
            rows = pl.ds(pl.multiple_of(slot * tokens, tokens), tokens)
            k_rot[rows, :] = rotate(k_all[slot, kv], kg_ref[...], cos_ref[rows, :], sin_ref[rows, :])
            return carry

        lax.fori_loop(0, nz * nx, place, 0)
        keys = k_rot[...]
        values = v_all[:, kv].reshape(length, HEAD_DIM)
        for member in range(group):
            scores = lax.dot_general(
                q_rot[kv * group + member], keys, (((1,), (1,)), ((), ())),
                preferred_element_type=F32,
            )
            top = jnp.max(scores, axis=-1, keepdims=True)
            raised = jnp.exp2((scores - top) * factor)
            probs = (raised * (1.0 / jnp.sum(raised, axis=-1, keepdims=True))).astype(BF16)
            att[:, member * HEAD_DIM : (member + 1) * HEAD_DIM] = jnp.dot(
                probs, values, preferred_element_type=F32
            ).astype(BF16)
        part = ow.at[pl.ds(pl.multiple_of(kv * span, span), span), :]
        tile = 1024
        for start in range(0, width, tile):
            columns = slice(start, start + tile)
            acc[:, columns] += jnp.dot(att[...], part[:, columns], preferred_element_type=F32)

    send_own(0)
    for head in range(1, min(3, kv_heads)):
        send_own(head)
    own = pl.multiple_of(me * tokens, tokens)
    q_cos = cos_ref[pl.ds(own, tokens), :]
    q_sin = sin_ref[pl.ds(own, tokens), :]
    for head in range(heads):
        q_rot[head] = rotate(
            q_ref[:, head * HEAD_DIM : (head + 1) * HEAD_DIM], qg_ref[...], q_cos, q_sin
        )
    acc[...] = jnp.zeros_like(acc)
    relay(0)
    load_ow.wait()

    def one_head(kv, carry):
        @pl.when(kv + 3 < kv_heads)
        def _():
            send_own(kv + 3)

        @pl.when(kv + 1 < kv_heads)
        def _():
            relay(kv + 1)

        attend(kv)
        return carry

    lax.fori_loop(0, kv_heads, one_head, 0)

    blend = acc[...].astype(BF16).astype(F32)
    blend = blend * lax.rsqrt(jnp.mean(blend * blend, axis=-1, keepdims=True) + EPSILON)
    stream = (res_ref[...].astype(F32) + blend * post_ref[...]).astype(BF16)
    stream_ref[...] = stream
    wide = stream.astype(F32)
    wide = wide * lax.rsqrt(jnp.mean(wide * wide, axis=-1, keepdims=True) + EPSILON)
    normed_ref[...] = (wide * pre_ref[...]).astype(BF16)

    def sent(buf, sem, device):
        block = buf.at[0, 0]
        remote(block, block, sem, sem, device).wait_send()

    def drain(head, carry):
        for _raw, buf, recv, sx, su, sd in both:
            for plane in range(nz):
                slot = plane * nx + x

                @pl.when(jnp.logical_and(has_up, z >= plane))
                def _(slot=slot):
                    sent(buf, su.at[slot, head], up)

                @pl.when(jnp.logical_and(has_down, z <= plane))
                def _(slot=slot):
                    sent(buf, sd.at[slot, head], down)

                for off in range(1, nx):
                    sent(buf, sx.at[slot, head, off], beside[off - 1])
        return carry

    lax.fori_loop(0, kv_heads, drain, 0)


def before(tokens):
    row = lax.broadcasted_iota(jnp.int32, (tokens, tokens), 0)
    col = lax.broadcasted_iota(jnp.int32, (tokens, tokens), 1)
    return (row < col).astype(F32).astype(BF16)


def group_choice(meta, first_expert, count, rows):
    tokens = meta.shape[1]
    low = first_expert.astype(F32)
    member = jnp.where((meta[0:1] >= low) & (meta[0:1] < low + float(count)), 1.0, 0.0)
    rank = jnp.dot(
        jnp.broadcast_to(member, (8, tokens)).astype(BF16),
        before(tokens),
        preferred_element_type=F32,
    )[0:1]
    place = lax.broadcasted_iota(jnp.int32, (rows, tokens), 0).astype(F32)
    return jnp.where(rank == place, 1.0, 0.0) * member


def slot_choice(meta, first_expert, count, cap):
    tokens = meta.shape[1]
    names = lax.broadcasted_iota(jnp.int32, (count, tokens), 0).astype(F32)
    names = names + first_expert.astype(F32)
    first = jnp.where(meta[0:1] == names, 1.0, 0.0)
    second = jnp.where(meta[1:2] == names, 1.0, 0.0)
    rank = jnp.dot((first + second).astype(BF16), before(tokens), preferred_element_type=F32)
    row = lax.broadcasted_iota(jnp.int32, (count * cap, count), 0)
    start = lax.broadcasted_iota(jnp.int32, (count * cap, count), 1) * cap
    widen = jnp.where((row >= start) & (row < start + cap), 1.0, 0.0).astype(BF16)

    def widened(values):
        return jnp.dot(widen, values.astype(BF16), preferred_element_type=F32)

    place = lax.broadcasted_iota(jnp.int32, (count * cap, tokens), 0) & (cap - 1)
    hit = jnp.where(widened(rank) == place.astype(F32), 1.0, 0.0)
    return widened(first) * hit, widened(second) * hit


def contract(left, right, dims):
    return lax.dot_general(
        left.astype(BF16), right.astype(BF16), ((dims[:1], dims[1:]), ((), ())),
        preferred_element_type=F32,
    )


def expert_kernel(
    nz, nx, n_dp,
    normed_ref, stream_ref, meta_ref, wg_hbm, wu_hbm, wd_hbm,
    out_ref,
    wg, wu, wd, w_sem, p1, r1, metas, p2, r2, o2, back, mix, fin,
    s1, t1, sm, tm, s2, t2, s3, t3, s4, t4,
):
    tokens, width = normed_ref.shape
    count, cap = p2.shape[1], p2.shape[2]
    rows = p1.shape[1]
    sp = lax.axis_index("sp")
    dp = lax.axis_index("dp")
    z, x = sp // nx, sp % nx
    me = x * n_dp + dp

    loads = [
        pltpu.make_async_copy(src, dst, w_sem.at[i])
        for i, (src, dst) in enumerate(((wg_hbm, wg), (wu_hbm, wu), (wd_hbm, wd)))
    ]
    for load in loads:
        load.start()

    def plane_peer(off):
        j = lax.rem(me + off, count)
        return j, (z * nx + j // n_dp, j % n_dp)

    def column_peer(dist):
        plane = lax.rem(z + dist, nz)
        return plane, (plane * nx + x, dp)

    barrier = pltpu.get_barrier_semaphore()
    for off in range(1, count):
        pl.semaphore_signal(barrier, inc=1, device_id=plane_peer(off)[1], device_id_type=MESH)
    for dist in range(1, nz):
        pl.semaphore_signal(barrier, inc=1, device_id=column_peer(dist)[1], device_id_type=MESH)

    meta = meta_ref[...]
    for g in range(nz):
        pick = group_choice(meta, jnp.int32(g * count), count, rows)
        p1[g] = contract(pick, normed_ref[...], (1, 0)).astype(BF16)
    metas[z] = meta
    r1[z] = p1[z]

    pl.semaphore_wait(barrier, count - 1 + nz - 1)
    for dist in range(1, nz):
        plane, device = column_peer(dist)
        remote(meta_ref, metas.at[z], sm.at[plane], tm.at[z], device).start()
        remote(p1.at[plane], r1.at[z], s1.at[plane], t1.at[z], device).start()

    first_expert = z * count

    def dispatch(dist, carry):
        source, device = column_peer(dist)

        @pl.when(dist > 0)
        def _():
            remote(meta_ref, metas.at[source], sm.at[source], tm.at[source], device).wait_recv()
            remote(p1.at[source], r1.at[source], s1.at[source], t1.at[source], device).wait_recv()

        got = metas[source]
        group = group_choice(got, first_expert, count, rows)
        first, second = slot_choice(got, first_expert, count, cap)
        pick = contract(first + second, group, (1, 1))
        packed = contract(pick, r1[source], (1, 0)).astype(BF16)
        p2[source] = packed.reshape(count, cap, width)
        r2[source, me] = p2[source, me]
        for off in range(1, count):
            j, device = plane_peer(off)
            remote(
                p2.at[source, j], r2.at[source, me], s2.at[source, j], t2.at[source, me], device
            ).start()
        return carry

    lax.fori_loop(0, nz, dispatch, 0)
    for load in loads:
        load.wait()

    def transform(dist, carry):
        source = lax.rem(z + dist + 1, nz)
        for off in range(1, count):
            j, device = plane_peer(off)
            remote(
                p2.at[source, j], r2.at[source, j], s2.at[source, j], t2.at[source, j], device
            ).wait_recv()
        arrived = r2[source].reshape(count * cap, width)
        gated = jnp.dot(arrived, wg[...], preferred_element_type=F32)
        lifted = jnp.dot(arrived, wu[...], preferred_element_type=F32)
        hidden = (gated / (1.0 + jnp.exp(-gated)) * lifted).astype(BF16)
        result = jnp.dot(hidden, wd[...], preferred_element_type=F32).astype(BF16)
        o2[source] = result.reshape(count, cap, width)
        back[source, me] = o2[source, me]
        for off in range(1, count):
            j, device = plane_peer(off)
            remote(
                o2.at[source, j], back.at[source, me], s3.at[source, j], t3.at[source, me], device
            ).start()
        return carry

    lax.fori_loop(0, nz, transform, 0)

    def combine(dist, carry):
        source, column = column_peer(dist + 1)
        for off in range(1, count):
            j, device = plane_peer(off)
            remote(
                o2.at[source, j], back.at[source, j], s3.at[source, j], t3.at[source, j], device
            ).wait_recv()
        got = metas[source]
        group = group_choice(got, first_expert, count, rows)
        first, second = slot_choice(got, first_expert, count, cap)
        outs = back[source].reshape(count * cap, width)
        one = contract(contract(group, first, (1, 1)), outs, (1, 0))
        two = contract(contract(group, second, (1, 1)), outs, (1, 0))
        weight = jnp.sum(group * got[2:3], axis=1, keepdims=True)
        share = jnp.sum(group * got[3:4], axis=1, keepdims=True)
        total = (weight * (share * one + (1.0 - share) * two)).astype(BF16)
        mix[source] = total

        @pl.when(dist == nz - 1)
        def _():
            fin[source] = total

        @pl.when(dist < nz - 1)
        def _():
            remote(mix.at[source], fin.at[z], s4.at[source], t4.at[z], column).start()

        return carry

    lax.fori_loop(0, nz, combine, 0)

    picks = [
        group_choice(meta, jnp.int32(g * count), count, rows) for g in range(nz)
    ]
    for dist in range(1, nz):
        plane, device = column_peer(dist)
        remote(mix.at[plane], fin.at[plane], s4.at[plane], t4.at[plane], device).wait_recv()
    every = jnp.concatenate(picks, axis=0)
    added = contract(every, fin[...].reshape(tokens, width), (0, 0))
    out_ref[...] = (stream_ref[...].astype(F32) + added).astype(BF16)

    for dist in range(1, nz):
        plane, device = column_peer(dist)
        remote(meta_ref, metas.at[z], sm.at[plane], tm.at[z], device).wait_send()
        remote(p1.at[plane], r1.at[z], s1.at[plane], t1.at[z], device).wait_send()
        remote(mix.at[plane], fin.at[z], s4.at[plane], t4.at[z], device).wait_send()

    def drain(source, carry):
        for off in range(1, count):
            j, device = plane_peer(off)
            remote(
                p2.at[source, j], r2.at[source, me], s2.at[source, j], t2.at[source, me], device
            ).wait_send()
            remote(
                o2.at[source, j], back.at[source, me], s3.at[source, j], t3.at[source, me], device
            ).wait_send()
        return carry

    lax.fori_loop(0, nz, drain, 0)


def local(
    residual_in, query_proj, key_proj, value_proj, query_gain, key_gain, out_weight, post_gain,
    pre_gain, route_ids, group_weight, first_share, gate_weight, up_weight, down_weight,
):
    n_sp = lax.axis_size("sp")
    n_dp = lax.axis_size("dp")
    tokens, width = query_proj.shape[1:]
    kv_width = key_proj.shape[2]
    heads, kv_heads = width // HEAD_DIM, kv_width // HEAD_DIM
    nz = GROUPS
    nx = n_sp // nz
    length = n_sp * tokens
    cos, sin = angle_tables(length)
    vmem = pl.BlockSpec(memory_space=pltpu.VMEM)
    hbm = pl.BlockSpec(memory_space=pl.ANY)
    dma = pltpu.SemaphoreType.DMA
    row = jax.ShapeDtypeStruct((tokens, width), BF16)
    stream, normed = pl.pallas_call(
        functools.partial(attention_kernel, nz, nx),
        out_shape=(row, row),
        in_specs=[vmem] * 10 + [hbm],
        out_specs=(vmem, vmem),
        scratch_shapes=[
            pltpu.VMEM((n_sp, kv_heads, tokens, HEAD_DIM), BF16),
            pltpu.VMEM((n_sp, kv_heads, tokens, HEAD_DIM), BF16),
            pltpu.VMEM((heads, tokens, HEAD_DIM), BF16),
            pltpu.VMEM((length, HEAD_DIM), BF16),
            pltpu.VMEM((tokens, width // kv_heads), BF16),
            pltpu.VMEM((tokens, width), F32),
            pltpu.VMEM((width, width), BF16),
            dma,
            dma((n_sp, kv_heads)), dma((n_sp, kv_heads)),
            dma((n_sp, kv_heads, nx)), dma((n_sp, kv_heads)), dma((n_sp, kv_heads)),
            dma((n_sp, kv_heads, nx)), dma((n_sp, kv_heads)), dma((n_sp, kv_heads)),
        ],
        compiler_params=pltpu.CompilerParams(
            collective_id=0, has_side_effects=True, vmem_limit_bytes=VMEM_LIMIT
        ),
        name="attention",
    )(
        query_proj[0], key_proj[0], value_proj[0],
        query_gain.reshape(1, -1), key_gain.reshape(1, -1),
        jnp.asarray(cos), jnp.asarray(sin),
        residual_in[0], post_gain.reshape(1, -1), pre_gain.reshape(1, -1), out_weight,
    )

    experts = gate_weight.shape[0] * n_sp * n_dp
    count = experts // nz
    cap = max(16, 4 * tokens // experts)
    rows = tokens // nz
    ff = gate_weight.shape[2]
    meta = jnp.concatenate(
        [route_ids[0].T.astype(F32), group_weight, first_share, jnp.zeros((4, tokens), F32)], axis=0
    )
    blocks = pltpu.VMEM((nz, count, cap, width), BF16)
    lines = pltpu.VMEM((nz, rows, width), BF16)
    out = pl.pallas_call(
        functools.partial(expert_kernel, nz, nx, n_dp),
        out_shape=row,
        in_specs=[vmem] * 3 + [hbm] * 3,
        out_specs=vmem,
        scratch_shapes=[
            pltpu.VMEM((width, ff), BF16),
            pltpu.VMEM((width, ff), BF16),
            pltpu.VMEM((ff, width), BF16),
            dma((3,)),
            lines, lines,
            pltpu.VMEM((nz, 8, tokens), F32),
            blocks, blocks, blocks, blocks,
            lines, lines,
            dma((nz,)), dma((nz,)), dma((nz,)), dma((nz,)),
            dma((nz, count)), dma((nz, count)), dma((nz, count)), dma((nz, count)),
            dma((nz,)), dma((nz,)),
        ],
        compiler_params=pltpu.CompilerParams(
            collective_id=1, has_side_effects=True, vmem_limit_bytes=VMEM_LIMIT
        ),
        name="experts",
    )(normed, stream, meta, gate_weight[0], up_weight[0], down_weight[0])
    return out.reshape(1, tokens, width)


LAYER_VMEM_LIMIT = 50 * 1024 * 1024


def layer_kernel(
    nz, nx, cores,
    q_hbm, k_hbm, v_hbm, qg_hbm, kg_hbm, res_hbm, post_hbm, pre_hbm, route_hbm, gw_hbm, fs_hbm,
    cos_hbm, sin_hbm, ow_hbm, wg_hbm, wu_hbm, wd_hbm,
    out,
    q_ref, k_ref, v_ref, qg_ref, kg_ref, res_ref, post_ref, pre_ref, route_ref, gw_ref, fs_ref,
    cos, sin, ow, wg, wu, wd, load_sem,
    kv, q_rot, att, acc, summing,
    rk_own, rk_x, rk_z, kv_x_sent, kv_z_sent,
    perm, perm_back, mrow, metas, picks, weights, backs,
    zs_sem, zr_sem, ms_sem, mr_sem,
    stream, srt, rows, y, other, part, relay, direct, summed, fin,
    t_z, t_a, t_b, t_c, t_d, t_core, spread_sent,
    t_other, t_up, t_side, t_last, t_home, back_sent,
):
    tokens, width = q_ref.shape
    heads = width // HEAD_DIM
    kv_heads = k_ref.shape[1] // HEAD_DIM
    group = heads // kv_heads
    slots_kv = nz * nx
    length = slots_kv * tokens
    last_head = kv_heads - 1
    chips = metas.shape[2]
    count = chips * cores
    block = tokens // nz
    cap = y.shape[2] // chips
    half = block // 2
    me = lax.axis_index("sp")
    dp = lax.axis_index("dp")
    z, x = me // nx, me % nx
    side, core = dp // cores, dp % cores
    up, down = (me + nx, dp), (me - nx, dp)
    beside = (z * nx + 1 - x, dp)
    across = (me, (1 - side) * cores + core)
    partner = (me, side * cores + 1 - core)
    has_up, has_down = z < nz - 1, z > 0
    sides = chips // nx
    mine = x * sides + side
    chip_x, chip_y = (1 - x) * sides + side, x * sides + 1 - side
    chip_d = (1 - x) * sides + 1 - side

    def column(plane):
        return (plane * nx + x, dp)

    flip = z >= nz // 2
    low = jnp.where(flip, nz - 1 - z, z)
    inner = (2, 0, 3)

    def source_of(i):
        if i == 0:
            return z
        near = jnp.where(low == 0, i, inner[i - 1])
        return jnp.where(flip, nz - 1 - near, near)

    sources = [source_of(i) for i in range(nz)]

    barrier = pltpu.get_barrier_semaphore()
    greeted = [column(lax.rem(z + dist, nz)) for dist in range(1, nz)] + [beside, across, partner]
    for device in greeted:
        pl.semaphore_signal(barrier, inc=1, device_id=device, device_id_type=MESH)

    own = pl.multiple_of(me * tokens, tokens)
    loads = [
        pltpu.make_async_copy(src, dst, load_sem.at[i])
        for i, (src, dst) in enumerate((
            (k_hbm, k_ref), (v_hbm, v_ref), (kg_hbm, kg_ref),
            (cos_hbm.at[pl.ds(own, tokens)], cos), (sin_hbm.at[pl.ds(own, tokens)], sin),
            (q_hbm, q_ref), (qg_hbm, qg_ref), (route_hbm, route_ref), (gw_hbm, gw_ref),
            (fs_hbm, fs_ref), (ow_hbm, ow), (res_hbm, res_ref), (post_hbm, post_ref),
            (pre_hbm, pre_ref), (wg_hbm, wg), (wu_hbm, wu), (wd_hbm, wd),
        ))
    ]
    for load in loads:
        load.start()

    for load in loads[:5]:
        load.wait()
    for head in range(kv_heads):
        columns = slice(head * HEAD_DIM, (head + 1) * HEAD_DIM)
        kv[head * slots_kv + me, 1] = v_ref[:, columns]
        kv[head * slots_kv + me, 0] = rotate(k_ref[:, columns], kg_ref[...], cos[...], sin[...])

    pl.semaphore_wait(barrier, len(greeted))

    def hop(slot, head, device, sent, landed):
        view = kv.at[head * slots_kv + slot]
        return remote(view, view, sent.at[0], landed, device)

    def bytes_of(units, sent, landed):
        view = kv.at[pl.ds(0, units)]
        return remote(view, view, sent, landed, beside)

    def own_beside(head):
        return hop(me, head, beside, kv_x_sent, rk_own.at[head])

    def pass_beside(slot, head):
        return hop(slot, head, beside, kv_x_sent, rk_x.at[head])

    def pass_on(slot, source, head, device):
        return hop(slot, head, device, kv_z_sent, rk_z.at[source, head])

    def cross_on(head, device):
        return hop(z * nx + 1 - x, head, device, kv_z_sent, rk_x.at[head])

    late_up, late_down = z == nz - 2, z == 1
    at_end = jnp.logical_or(z == 0, z == nz - 1)

    def send_own(head):
        final = head == last_head
        own_beside(head).start()
        for on, late, device in ((has_up, late_up, up), (has_down, late_down, down)):
            @pl.when(on & ~late if final else on)
            def _(device=device):
                pass_on(me, z, head, device).start()

    def take_own(head):
        bytes_of(1, kv_x_sent.at[0], rk_own.at[head]).wait_recv()

    def crosses(head):
        return head % 2 == 1

    def cross(head):
        final = head == last_head
        take_own(head)
        for on, late, device in ((has_up, late_up, up), (has_down, late_down, down)):
            @pl.when(on & ~late if final else on)
            def _(device=device):
                cross_on(head, device).start()

    def relay_kv(head, dist, given=True):
        for below in (True, False):
            source = z - dist if below else z + dist
            present = source >= 0 if below else source < nz
            further = has_up if below else has_down
            onward = up if below else down

            @pl.when(present & given)
            def _(source=source, further=further, onward=onward):
                slot = source * nx + x
                bytes_of(1, kv_z_sent.at[0], rk_z.at[source, head]).wait_recv()

                @pl.when(further)
                def _():
                    pass_on(slot, source, head, onward).start()

                if dist > 1 or not crosses(head):
                    pass_beside(slot, head).start()

    def send_late(head):
        for late, device in ((late_up, up), (late_down, down)):
            @pl.when(late)
            def _(device=device):
                pass_on(me, z, head, device).start()
                if crosses(head):
                    cross_on(head, device).start()

    def wave(step):
        for dist in range(1, nz):
            head = step - (dist - 1)
            if 0 <= head < kv_heads:
                relay_kv(head, dist, ~at_end if head == last_head and dist == 1 else True)
                if dist == 1 and crosses(head):
                    cross(head)
        if step == kv_heads + nz - 4:
            send_late(last_head)
        if step + 2 < kv_heads:
            send_own(step + 2)

    for head in range(2):
        send_own(head)

    for load in loads[5:10]:
        load.wait()
    for head in range(heads):
        q_rot[head] = rotate(
            q_ref[:, head * HEAD_DIM : (head + 1) * HEAD_DIM], qg_ref[...], cos[...], sin[...]
        )
    acc[...] = jnp.zeros_like(acc)
    summing[:, HEAD_DIM:] = jnp.ones((length, HEAD_DIM), BF16)

    row = lax.broadcasted_iota(jnp.int32, (tokens, tokens), 0)
    lane = lax.broadcasted_iota(jnp.int32, (tokens, tokens), 1)

    def routing():
        first = route_ref[0:1].astype(F32)
        second = route_ref[1:2].astype(F32)
        of_lane = jnp.zeros_like(first)
        for g in range(1, nz):
            of_lane = of_lane + jnp.where(first >= float(g * count), 1.0, 0.0)
        of = jnp.sum(jnp.where(row == lane, of_lane, 0.0), axis=1, keepdims=True)
        same = of == of_lane
        rank = jnp.sum(jnp.where(same & (lane < row), 1.0, 0.0), axis=1, keepdims=True)
        rank_lane = jnp.sum(jnp.where(same & (row < lane), 1.0, 0.0), axis=0, keepdims=True)
        place = (of * float(block) + rank).astype(jnp.int32)
        place_lane = (of_lane * float(block) + rank_lane).astype(jnp.int32)
        perm[...] = jnp.where(row == place_lane, 1.0, 0.0).astype(BF16)
        perm_back[...] = jnp.where(place == lane, 1.0, 0.0).astype(BF16)
        fields = (
            first, second,
            gw_ref[...] * fs_ref[...], gw_ref[...] * (1.0 - fs_ref[...]),
        )
        chosen = lax.broadcasted_iota(jnp.int32, (8, tokens), 0).astype(F32) == of_lane
        at = rank.astype(jnp.int32)
        table = jnp.zeros((8, tokens), F32)
        for f, field in enumerate(fields):
            spread = jnp.where(lane == at + f * block, 1.0, 0.0)
            table += lax.dot_general(
                jnp.where(chosen, field, 0.0), spread, (((1,), (0,)), ((), ())),
                precision=lax.Precision.HIGHEST, preferred_element_type=F32,
            )
        for g in range(nz):
            mrow[g] = table[g : g + 1]

    routing()
    metas[z, core, mine] = mrow[z]

    def meta_column(dist):
        plane = lax.rem(z + dist, nz)
        return remote(
            mrow.at[plane], metas.at[z, core, mine], zs_sem.at[0], zr_sem.at[0], column(plane)
        )

    def meta_all():
        view = mrow.at[pl.ds(0, nz - 1)]
        return remote(view, view, zs_sem.at[0], zr_sem.at[0], beside)

    for dist in range(1, nz):
        meta_column(dist).start()

    def meta_copy(view, step, device):
        return remote(view, view, ms_sem.at[step], mr_sem.at[step], device)

    pair = pl.ds(x * sides, sides)
    other_pair = pl.ds((1 - x) * sides, sides)
    meta_sends = (
        meta_copy(metas.at[:, core, mine], 0, across),
        meta_copy(metas.at[:, core, pair], 1, partner),
        meta_copy(metas.at[:, :, pair], 2, beside),
    )
    meta_recvs = (
        meta_copy(metas.at[:, core, chip_y], 0, across),
        meta_copy(metas.at[:, 1 - core, pair], 1, partner),
        meta_copy(metas.at[:, :, other_pair], 2, beside),
    )

    def choice(plane, of_core, expert):
        table = metas[plane, of_core].reshape(chips, tokens)
        first = table[:, 0:block] == expert
        second = table[:, block : 2 * block] == expert
        member = jnp.where(first | second, 1.0, 0.0)
        weight = jnp.where(first, table[:, 2 * block : 3 * block], 0.0)
        weight = weight + jnp.where(second, table[:, 3 * block : 4 * block], 0.0)
        r = lax.broadcasted_iota(jnp.int32, (block, block), 0)
        c = lax.broadcasted_iota(jnp.int32, (block, block), 1)
        earlier = jnp.where(r < c, 1.0, 0.0).astype(BF16)
        rank = jnp.dot(
            jnp.concatenate([member] * (8 // chips), axis=0).astype(BF16), earlier,
            preferred_element_type=F32,
        )[:chips]
        place = lax.broadcasted_iota(jnp.int32, (chips, cap, block), 1).astype(F32)
        hit = jnp.where(rank[:, None, :] == place, 1.0, 0.0) * member[:, None, :]
        of_slot = jnp.sum(hit * weight[:, None, :], axis=2, keepdims=True).reshape(chips * cap, 1)
        flat = hit.reshape(chips * cap, block).astype(BF16)
        wide_row = lax.broadcasted_iota(jnp.int32, (block, tokens), 0)
        wide_lane = lax.broadcasted_iota(jnp.int32, (block, tokens), 1)
        widen = jnp.where(lax.rem(wide_lane, block) == wide_row, 1.0, 0.0).astype(BF16)
        spread = jnp.dot(flat, widen, preferred_element_type=F32)
        slot = lax.broadcasted_iota(jnp.int32, (chips * cap, tokens), 0) // cap
        chip = lax.broadcasted_iota(jnp.int32, (chips * cap, tokens), 1) // block
        return jnp.where(slot == chip, spread, 0.0), of_slot

    def tables():
        expert = (z * count + x * (count // nx) + dp).astype(F32)
        twin = (z * count + x * (count // nx) + side * cores + 1 - core).astype(F32)

        def one_plane(plane, carry):
            for of_core in range(cores):
                pick, of_slot = choice(plane, of_core, expert)
                picks[plane, of_core] = pick.astype(BF16)
                weights[plane, of_core] = of_slot
            back, _ = choice(plane, core, expert)
            theirs, _ = choice(plane, core, twin)
            backs[plane] = jnp.concatenate([back, theirs], axis=0).T.astype(BF16)
            return carry

        lax.fori_loop(0, nz, one_plane, 0)

    factor = float(HEAD_DIM**-0.5 * np.log2(np.e))
    span = group * HEAD_DIM

    def attend(head):
        here = pl.ds(head * slots_kv, slots_kv)
        keys = kv[here, 0].reshape(length, HEAD_DIM)
        summing[:, :HEAD_DIM] = kv[here, 1].reshape(length, HEAD_DIM)

        def scores_of(member):
            return lax.dot_general(
                q_rot[head * group + member], keys, (((1,), (1,)), ((), ())),
                preferred_element_type=F32,
            )

        scores = scores_of(0)
        for member in range(group):
            later = scores_of(member + 1) if member + 1 < group else None
            top = jnp.max(scores, axis=-1, keepdims=True)
            raised = jnp.exp2((scores - top) * factor).astype(BF16)
            mixed = jnp.dot(raised, summing[...], preferred_element_type=F32)
            att[:, member * HEAD_DIM : (member + 1) * HEAD_DIM] = (
                mixed[:, :HEAD_DIM] / mixed[:, HEAD_DIM:]
            ).astype(BF16)
            scores = later
        above = ow.at[pl.ds(pl.multiple_of(head * span, span), span), :]
        tile = 1024
        for start in range(0, width, tile):
            columns = slice(start, start + tile)
            acc[:, columns] += jnp.dot(att[...], above[:, columns], preferred_element_type=F32)

    wave(0)
    wave(1)
    meta_all().wait_recv()
    meta_sends[0].start()
    wave(2)
    meta_recvs[0].wait_recv()
    meta_sends[1].start()
    meta_recvs[1].wait_recv()
    meta_sends[2].start()
    loads[10].wait()
    wave(3)
    wave(4)

    def one_head(head, carry):
        @pl.when(head == 1)
        def _():
            wave(5)

        @pl.when(head == 2)
        def _():
            relay_kv(last_head, 1, at_end)

        @pl.when(lax.rem(head, 2) == 0)
        def _():
            take_own(head)

        bytes_of(nz - 1, kv_x_sent.at[0], rk_x.at[head]).wait_recv()
        attend(head)
        return carry

    lax.fori_loop(0, kv_heads, one_head, 0)
    for load in loads[11:14]:
        load.wait()

    blend = acc[...].astype(BF16).astype(F32)
    blend = blend * lax.rsqrt(jnp.mean(blend * blend, axis=-1, keepdims=True) + EPSILON)
    flow = (res_ref[...].astype(F32) + blend * post_ref[...]).astype(BF16)
    stream[...] = flow
    wide = flow.astype(F32)
    wide = wide * lax.rsqrt(jnp.mean(wide * wide, axis=-1, keepdims=True) + EPSILON)
    normed = (wide * pre_ref[...]).astype(BF16)
    srt[...] = jnp.dot(perm[...], normed, preferred_element_type=F32).astype(BF16).reshape(srt.shape)

    def unit(s, of_core, chip, h=0):
        return ((s * cores + of_core) * chips + chip) * 2 + h

    def units(first, amount):
        return rows.at[pl.ds(first, amount)]

    def waiting(amount, landed):
        return remote(units(0, amount), units(0, amount), spread_sent.at[0], landed, partner)

    def z_send(plane):
        return remote(
            srt.at[pl.ds(2 * plane, 2)], units(unit(z, core, mine), 2), spread_sent.at[0], t_z.at[z],
            column(plane),
        )

    z_send(sources[1]).start()

    @pl.when(~at_end)
    def _():
        z_send(sources[2]).start()

    rows[pl.ds(unit(z, core, mine), 2)] = srt[pl.ds(2 * z, 2)]

    def over(s, chip, h, landed, device):
        view = rows.at[unit(s, core, chip, h)]
        return remote(view, view, spread_sent.at[0], landed.at[s], device)

    def over_core(s, chip):
        view = units(unit(s, core, chip), 2)
        return remote(view, view, spread_sent.at[0], t_core.at[s], partner)

    def route_tables(i):
        z_send(jnp.where(at_end, sources[2], sources[3])).start()
        meta_recvs[2].wait_recv()
        tables()

    def send_far(i):
        @pl.when(at_end)
        def _():
            z_send(sources[i]).start()

    def spread_own(i):
        s = sources[i]
        if i > 0:
            waiting(2, t_z.at[s]).wait_recv()
        over(s, mine, 0, t_a, beside).start()
        over(s, mine, 1, t_b, across).start()
        over(s, mine, 1, t_c, beside).start()
        over(s, mine, 0, t_c, across).start()
        over_core(s, mine).start()

    def spread_on(i):
        s = sources[i]
        waiting(1, t_a.at[s]).wait_recv()
        over(s, chip_x, 0, t_d, across).start()
        waiting(1, t_b.at[s]).wait_recv()
        over(s, chip_y, 1, t_d, beside).start()

    def spread_core(i):
        s = sources[i]
        waiting(2, t_c.at[s]).wait_recv()
        over_core(s, chip_x).start()
        over_core(s, chip_y).start()

    def spread_last(i):
        s = sources[i]
        waiting(2, t_d.at[s]).wait_recv()
        over_core(s, chip_d).start()

    def to_partner(s):
        return remote(y.at[s, 1 - core], other.at[s], back_sent.at[0], t_other.at[s], partner)

    def transform(i):
        s = sources[i]
        waiting(2 * chips, t_core.at[s]).wait_recv()
        packed = [
            jnp.dot(
                picks[s, q], rows[pl.ds(unit(s, q, 0), 2 * chips)].reshape(tokens, width), preferred_element_type=F32
            ).astype(BF16)
            for q in range(cores)
        ]
        packed = jnp.concatenate(packed, axis=0)
        gated = jnp.dot(packed, wg[...], preferred_element_type=F32)
        lifted = jnp.dot(packed, wu[...], preferred_element_type=F32)
        hidden = (gated / (1.0 + jnp.exp(-gated)) * lifted).astype(BF16)
        result = jnp.dot(hidden, wd[...], preferred_element_type=F32)
        slots = chips * cap
        for q in range(cores):
            y[s, q] = (result[q * slots : (q + 1) * slots] * weights[s, q]).astype(BF16)
        to_partner(s).start()

    def back(s, chip, h, into, at, landed, device):
        return remote(
            part.at[s, chip, halves[h]], into.at[s, at], back_sent.at[0], landed.at[s], device
        )

    halves = (pl.ds(0, half), pl.ds(half, half))

    def gather_back(i):
        s = sources[i]
        to_partner(s).wait_recv()
        outs = jnp.concatenate([y[s, core], other[s]], axis=0)
        part[s] = jnp.dot(backs[s], outs, preferred_element_type=F32).astype(BF16).reshape(
            chips, block, width
        )
        back(s, chip_d, 0, relay, 0, t_up, across).start()
        back(s, chip_d, 1, relay, 1, t_side, beside).start()
        back(s, chip_x, 1, direct, 1, t_last, beside).start()
        back(s, chip_y, 0, direct, 0, t_last, across).start()

    def add(left, right):
        return (left.astype(F32) + right.astype(F32)).astype(BF16)

    def pass_back(i):
        s = sources[i]
        waiting(1, t_up.at[s]).wait_recv()
        part[s, chip_x, halves[0]] = add(part[s, chip_x, halves[0]], relay[s, 0])
        back(s, chip_x, 0, summed, 0, t_last, beside).start()
        waiting(1, t_side.at[s]).wait_recv()
        part[s, chip_y, halves[1]] = add(part[s, chip_y, halves[1]], relay[s, 1])
        back(s, chip_y, 1, summed, 1, t_last, across).start()

    def home(s):
        return remote(part.at[s, mine], fin.at[z], back_sent.at[0], t_home.at[0], column(s))

    def finish(i):
        s = sources[i]
        waiting(4, t_last.at[s]).wait_recv()
        for h in range(2):
            total = part[s, mine, halves[h]].astype(F32) + direct[s, h].astype(F32)
            total = (total + summed[s, h].astype(F32)).astype(BF16)
            if i > 0:
                part[s, mine, halves[h]] = total
            else:
                fin[s, halves[h]] = total
        if i > 0:
            home(s).start()

    def weights_ready(i):
        for load in loads[14:]:
            load.wait()

    for stage, i in plan(
        route_tables, send_far, spread_own, spread_on, spread_core, spread_last, weights_ready, transform, gather_back, pass_back, finish
    ):
        stage(i)

    waiting(2 * (nz - 1), t_home.at[0]).wait_recv()
    tile = width // 4
    for start in range(0, width, tile):
        columns = slice(start, start + tile)
        added = jnp.dot(
            perm_back[...], fin[:, :, columns].reshape(tokens, tile), preferred_element_type=F32
        )
        out[:, columns] = (stream[:, columns].astype(F32) + added).astype(BF16)

    for plane in range(nz):
        lanes = sum(head % 2 for head in range(kv_heads))
        upward = (plane + 1) * kv_heads + lanes if plane < nz - 1 else 0
        downward = (nz - plane) * kv_heads + lanes if plane > 0 else 0
        sideways = nz * kv_heads - lanes * sum(0 <= plane + d < nz for d in (-1, 1))

        @pl.when(z == plane)
        def _(vertical=upward + downward, sideways=sideways):
            bytes_of(vertical, kv_z_sent.at[0], rk_own.at[0]).wait_send()
            bytes_of(sideways, kv_x_sent.at[0], rk_own.at[0]).wait_send()

    meta_all().wait_send()
    for send in meta_sends:
        send.wait_send()
    spread_units = 2 * (nz - 1) + nz * (6 + 2 * chips)
    waiting(spread_units, t_core.at[0]).wait_send()
    back_units = nz * (2 * chips * cap // block + 6) + 2 * (nz - 1)
    returned = units(0, back_units)
    remote(returned, returned, back_sent.at[0], t_core.at[0], partner).wait_send()


def plan(route, far, own, on, share, last, ready, transform, gather_back, pass_back, finish):
    return (
        (own, 0), (route, 0), (far, 3), (on, 0), (own, 1), (share, 0), (on, 1), (last, 0),
        (own, 2), (share, 1), (ready, 0), (transform, 0), (on, 2), (last, 1), (own, 3),
        (share, 2), (transform, 1), (on, 3), (gather_back, 1), (last, 2), (transform, 2),
        (share, 3), (pass_back, 1), (gather_back, 2), (last, 3), (transform, 3), (finish, 1),
        (pass_back, 2), (gather_back, 3), (finish, 2), (pass_back, 3), (gather_back, 0),
        (finish, 3), (pass_back, 0), (finish, 0),
    )


def fused(
    residual_in, query_proj, key_proj, value_proj, query_gain, key_gain, out_weight, post_gain,
    pre_gain, route_ids, group_weight, first_share, gate_weight, up_weight, down_weight,
):
    n_sp = lax.axis_size("sp")
    n_dp = lax.axis_size("dp")
    tokens, width = query_proj.shape[1:]
    kv_heads = key_proj.shape[2] // HEAD_DIM
    heads = width // HEAD_DIM
    nz = GROUPS
    nx = n_sp // nz
    cores = 2
    chips = nx * (n_dp // cores)
    experts = gate_weight.shape[0] * n_sp * n_dp
    cap = max(16, 4 * tokens // experts)
    block = tokens // nz
    slots = chips * cap
    ff = gate_weight.shape[2]
    length = n_sp * tokens
    cos, sin = angle_tables(length)
    vmem = pl.BlockSpec(memory_space=pltpu.VMEM)
    hbm = pl.BlockSpec(memory_space=pl.ANY)
    dma = pltpu.SemaphoreType.DMA

    def buf(*shape, kind=BF16):
        return pltpu.VMEM(shape, kind)

    out = pl.pallas_call(
        functools.partial(layer_kernel, nz, nx, cores),
        out_shape=jax.ShapeDtypeStruct((tokens, width), BF16),
        in_specs=[hbm] * 17,
        out_specs=vmem,
        scratch_shapes=[
            buf(tokens, width), buf(tokens, kv_heads * HEAD_DIM), buf(tokens, kv_heads * HEAD_DIM),
            buf(1, HEAD_DIM, kind=F32), buf(1, HEAD_DIM, kind=F32), buf(tokens, width),
            buf(1, width, kind=F32), buf(1, width, kind=F32),
            buf(2, tokens, kind=jnp.int32), buf(1, tokens, kind=F32), buf(1, tokens, kind=F32),
            buf(tokens, HEAD_DIM, kind=F32), buf(tokens, HEAD_DIM, kind=F32),
            buf(width, width), buf(width, ff), buf(width, ff), buf(ff, width),
            dma((17,)),
            buf(kv_heads * n_sp, 2, tokens, HEAD_DIM),
            buf(heads, tokens, HEAD_DIM),
            buf(tokens, width // kv_heads),
            buf(tokens, width, kind=F32),
            buf(length, 2 * HEAD_DIM),
            dma((kv_heads,)), dma((kv_heads,)), dma((nz, kv_heads)), dma((1,)), dma((1,)),
            buf(tokens, tokens), buf(tokens, tokens),
            buf(nz, 1, tokens, kind=F32), buf(nz, cores, chips, 1, tokens, kind=F32),
            buf(nz, cores, slots, tokens), buf(nz, cores, slots, 1, kind=F32),
            buf(nz, tokens, cores * slots),
            dma((1,)), dma((1,)), dma((3,)), dma((3,)),
            buf(tokens, width), buf(2 * nz, block // 2, width),
            buf(nz * cores * chips * 2, block // 2, width),
            buf(nz, cores, slots, width), buf(nz, slots, width),
            buf(nz, chips, block, width),
            buf(nz, 2, block // 2, width), buf(nz, 2, block // 2, width),
            buf(nz, 2, block // 2, width), buf(nz, block, width),
            dma((nz,)), dma((nz,)), dma((nz,)), dma((nz,)), dma((nz,)), dma((nz,)), dma((1,)),
            dma((nz,)), dma((nz,)), dma((nz,)), dma((nz,)), dma((1,)), dma((1,)),
        ],
        compiler_params=pltpu.CompilerParams(
            collective_id=0, has_side_effects=True, vmem_limit_bytes=LAYER_VMEM_LIMIT
        ),
        name="layer",
    )(*(pltpu.with_memory_space_constraint(array, pltpu.HBM) for array in (
        query_proj[0], key_proj[0], value_proj[0],
        query_gain.reshape(1, -1), key_gain.reshape(1, -1),
        residual_in[0], post_gain.reshape(1, -1), pre_gain.reshape(1, -1),
        route_ids[0].T, group_weight, first_share,
        jnp.asarray(cos), jnp.asarray(sin), out_weight,
        gate_weight[0], up_weight[0], down_weight[0],
    )))
    return out.reshape(1, tokens, width)


def solution(mesh):
    tok3 = P("dp", "sp", None)
    tok2 = P("dp", "sp")
    weight = P(("sp", "dp"), None, None)
    placed = (
        tok3, tok3, tok3, tok3, P(), P(), P(), P(), P(), tok3, tok2, tok2, weight, weight, weight,
    )
    small = mesh.shape["sp"] == 2 * GROUPS and mesh.shape["dp"] == 4
    return jax.shard_map(
        fused if small else local, mesh=mesh, in_specs=placed, out_specs=P("dp", "sp", None), check_vma=False
    )
```

```python
import functools

import jax
import jax.numpy as jnp
import numpy as np
from jax import lax
from jax.experimental import pallas as pl
from jax.experimental.pallas import tpu as pltpu
from jax.sharding import PartitionSpec as P

HEAD_DIM = 128
GRID_W = 64
GROUPS = 4
EPSILON = 1e-06
MESH = pl.DeviceIdType.MESH
VMEM_LIMIT = 60 * 1024 * 1024
F32 = jnp.float32
BF16 = jnp.bfloat16


def angle_tables(length):
    quarter = HEAD_DIM // 4
    inverse = 10000.0 ** (-np.arange(quarter, dtype=np.float64) / quarter)
    positions = np.arange(length)
    rows = (positions // GRID_W)[:, None] * inverse
    cols = (positions % GRID_W)[:, None] * inverse
    angles = np.concatenate([rows, rows, cols, cols], axis=-1)
    sign = np.where(np.arange(HEAD_DIM) % (2 * quarter) < quarter, -1.0, 1.0)
    return np.cos(angles).astype(np.float32), (np.sin(angles) * sign).astype(np.float32)


def rotate(raw, gain, cos, sin):
    floats = raw.astype(F32)
    normed = floats * lax.rsqrt(jnp.mean(floats * floats, axis=-1, keepdims=True) + EPSILON) * gain
    quarter = HEAD_DIM // 4
    lane = lax.broadcasted_iota(jnp.int32, normed.shape, 1)
    turned = jnp.where(
        (lane & (2 * quarter - 1)) < quarter,
        pltpu.roll(normed, HEAD_DIM - quarter, 1),
        pltpu.roll(normed, quarter, 1),
    )
    return (normed * cos + turned * sin).astype(BF16)


def remote(src, dst, send_sem, recv_sem, device):
    return pltpu.make_async_remote_copy(
        src_ref=src,
        dst_ref=dst,
        send_sem=send_sem,
        recv_sem=recv_sem,
        device_id=device,
        device_id_type=MESH,
    )


def attention_kernel(
    nz, nx,
    q_ref, k_ref, v_ref, qg_ref, kg_ref, cos_ref, sin_ref, res_ref, post_ref, pre_ref, ow_hbm,
    stream_ref, normed_ref,
    k_all, v_all, q_rot, k_rot, att, acc, ow, ow_sem,
    rk, rv, skx, sku, skd, svx, svu, svd,
):
    tokens, width = q_ref.shape
    heads = width // HEAD_DIM
    kv_heads = k_ref.shape[1] // HEAD_DIM
    group = heads // kv_heads
    me = lax.axis_index("sp")
    dp = lax.axis_index("dp")
    z, x = me // nx, me % nx
    up, down = (me + nx, dp), (me - nx, dp)
    has_up, has_down = z < nz - 1, z > 0
    both = ((k_ref, k_all, rk, skx, sku, skd), (v_ref, v_all, rv, svx, svu, svd))

    load_ow = pltpu.make_async_copy(ow_hbm, ow, ow_sem)
    load_ow.start()

    barrier = pltpu.get_barrier_semaphore()
    around = [(lax.rem(z + 1, nz) * nx + x, dp), (lax.rem(z + nz - 1, nz) * nx + x, dp)]
    beside = [(z * nx + lax.rem(x + off, nx), dp) for off in range(1, nx)]
    for device in around + beside:
        pl.semaphore_signal(barrier, inc=1, device_id=device, device_id_type=MESH)
    pl.semaphore_wait(barrier, len(around) + len(beside))

    def lanes_of(head):
        return pl.ds(pl.multiple_of(head * HEAD_DIM, HEAD_DIM), HEAD_DIM)

    def hop(src, buf, recv, send, slot, head, device):
        return remote(src, buf.at[slot, head], send, recv.at[slot, head], device)

    def send_own(head):
        for raw, buf, recv, sx, su, sd in both:
            src = raw.at[:, lanes_of(head)]

            @pl.when(has_up)
            def _():
                hop(src, buf, recv, su.at[me, head], me, head, up).start()

            @pl.when(has_down)
            def _():
                hop(src, buf, recv, sd.at[me, head], me, head, down).start()

        for raw, buf, recv, sx, su, sd in both:
            src = raw.at[:, lanes_of(head)]
            for off in range(1, nx):
                hop(src, buf, recv, sx.at[me, head, off], me, head, beside[off - 1]).start()

    def arrived(buf, recv, slot, head):
        block = buf.at[slot, head]
        remote(block, block, recv.at[slot, head], recv.at[slot, head], up).wait_recv()

    def relay(head):
        for dist in range(1, nz):
            for below in (True, False):
                source = z - dist if below else z + dist
                present = source >= 0 if below else source < nz
                further = has_up if below else has_down
                onward = up if below else down

                @pl.when(present)
                def _(source=source, below=below, further=further, onward=onward):
                    slot = source * nx + x
                    for _raw, buf, recv, sx, su, sd in both:
                        arrived(buf, recv, slot, head)
                        src = buf.at[slot, head]
                        send = su if below else sd

                        @pl.when(further)
                        def _(src=src, buf=buf, recv=recv, send=send):
                            hop(src, buf, recv, send.at[slot, head], slot, head, onward).start()

                        for off in range(1, nx):
                            hop(
                                src, buf, recv, sx.at[slot, head, off], slot, head,
                                beside[off - 1],
                            ).start()

    length = nz * nx * tokens
    factor = float(HEAD_DIM**-0.5 * np.log2(np.e))
    span = group * HEAD_DIM

    def attend(kv):
        for plane in range(nz):
            for off in range(1, nx):
                slot = plane * nx + lax.rem(x + off, nx)
                arrived(k_all, rk, slot, kv)
                arrived(v_all, rv, slot, kv)
        k_all[me, kv] = k_ref[:, lanes_of(kv)]
        v_all[me, kv] = v_ref[:, lanes_of(kv)]

        def place(slot, carry):
            rows = pl.ds(pl.multiple_of(slot * tokens, tokens), tokens)
            k_rot[rows, :] = rotate(k_all[slot, kv], kg_ref[...], cos_ref[rows, :], sin_ref[rows, :])
            return carry

        lax.fori_loop(0, nz * nx, place, 0)
        keys = k_rot[...]
        values = v_all[:, kv].reshape(length, HEAD_DIM)
        for member in range(group):
            scores = lax.dot_general(
                q_rot[kv * group + member], keys, (((1,), (1,)), ((), ())),
                preferred_element_type=F32,
            )
            top = jnp.max(scores, axis=-1, keepdims=True)
            raised = jnp.exp2((scores - top) * factor)
            probs = (raised * (1.0 / jnp.sum(raised, axis=-1, keepdims=True))).astype(BF16)
            att[:, member * HEAD_DIM : (member + 1) * HEAD_DIM] = jnp.dot(
                probs, values, preferred_element_type=F32
            ).astype(BF16)
        part = ow.at[pl.ds(pl.multiple_of(kv * span, span), span), :]
        tile = 1024
        for start in range(0, width, tile):
            columns = slice(start, start + tile)
            acc[:, columns] += jnp.dot(att[...], part[:, columns], preferred_element_type=F32)

    send_own(0)
    for head in range(1, min(3, kv_heads)):
        send_own(head)
    own = pl.multiple_of(me * tokens, tokens)
    q_cos = cos_ref[pl.ds(own, tokens), :]
    q_sin = sin_ref[pl.ds(own, tokens), :]
    for head in range(heads):
        q_rot[head] = rotate(
            q_ref[:, head * HEAD_DIM : (head + 1) * HEAD_DIM], qg_ref[...], q_cos, q_sin
        )
    acc[...] = jnp.zeros_like(acc)
    relay(0)
    load_ow.wait()

    def one_head(kv, carry):
        @pl.when(kv + 3 < kv_heads)
        def _():
            send_own(kv + 3)

        @pl.when(kv + 1 < kv_heads)
        def _():
            relay(kv + 1)

        attend(kv)
        return carry

    lax.fori_loop(0, kv_heads, one_head, 0)

    blend = acc[...].astype(BF16).astype(F32)
    blend = blend * lax.rsqrt(jnp.mean(blend * blend, axis=-1, keepdims=True) + EPSILON)
    stream = (res_ref[...].astype(F32) + blend * post_ref[...]).astype(BF16)
    stream_ref[...] = stream
    wide = stream.astype(F32)
    wide = wide * lax.rsqrt(jnp.mean(wide * wide, axis=-1, keepdims=True) + EPSILON)
    normed_ref[...] = (wide * pre_ref[...]).astype(BF16)

    def sent(buf, sem, device):
        block = buf.at[0, 0]
        remote(block, block, sem, sem, device).wait_send()

    def drain(head, carry):
        for _raw, buf, recv, sx, su, sd in both:
            for plane in range(nz):
                slot = plane * nx + x

                @pl.when(jnp.logical_and(has_up, z >= plane))
                def _(slot=slot):
                    sent(buf, su.at[slot, head], up)

                @pl.when(jnp.logical_and(has_down, z <= plane))
                def _(slot=slot):
                    sent(buf, sd.at[slot, head], down)

                for off in range(1, nx):
                    sent(buf, sx.at[slot, head, off], beside[off - 1])
        return carry

    lax.fori_loop(0, kv_heads, drain, 0)


def before(tokens):
    row = lax.broadcasted_iota(jnp.int32, (tokens, tokens), 0)
    col = lax.broadcasted_iota(jnp.int32, (tokens, tokens), 1)
    return (row < col).astype(F32).astype(BF16)


def group_choice(meta, first_expert, count, rows):
    tokens = meta.shape[1]
    low = first_expert.astype(F32)
    member = jnp.where((meta[0:1] >= low) & (meta[0:1] < low + float(count)), 1.0, 0.0)
    rank = jnp.dot(
        jnp.broadcast_to(member, (8, tokens)).astype(BF16),
        before(tokens),
        preferred_element_type=F32,
    )[0:1]
    place = lax.broadcasted_iota(jnp.int32, (rows, tokens), 0).astype(F32)
    return jnp.where(rank == place, 1.0, 0.0) * member


def slot_choice(meta, first_expert, count, cap):
    tokens = meta.shape[1]
    names = lax.broadcasted_iota(jnp.int32, (count, tokens), 0).astype(F32)
    names = names + first_expert.astype(F32)
    first = jnp.where(meta[0:1] == names, 1.0, 0.0)
    second = jnp.where(meta[1:2] == names, 1.0, 0.0)
    rank = jnp.dot((first + second).astype(BF16), before(tokens), preferred_element_type=F32)
    row = lax.broadcasted_iota(jnp.int32, (count * cap, count), 0)
    start = lax.broadcasted_iota(jnp.int32, (count * cap, count), 1) * cap
    widen = jnp.where((row >= start) & (row < start + cap), 1.0, 0.0).astype(BF16)

    def widened(values):
        return jnp.dot(widen, values.astype(BF16), preferred_element_type=F32)

    place = lax.broadcasted_iota(jnp.int32, (count * cap, tokens), 0) & (cap - 1)
    hit = jnp.where(widened(rank) == place.astype(F32), 1.0, 0.0)
    return widened(first) * hit, widened(second) * hit


def contract(left, right, dims):
    return lax.dot_general(
        left.astype(BF16), right.astype(BF16), ((dims[:1], dims[1:]), ((), ())),
        preferred_element_type=F32,
    )


def expert_kernel(
    nz, nx, n_dp,
    normed_ref, stream_ref, meta_ref, wg_hbm, wu_hbm, wd_hbm,
    out_ref,
    wg, wu, wd, w_sem, p1, r1, metas, p2, r2, o2, back, mix, fin,
    s1, t1, sm, tm, s2, t2, s3, t3, s4, t4,
):
    tokens, width = normed_ref.shape
    count, cap = p2.shape[1], p2.shape[2]
    rows = p1.shape[1]
    sp = lax.axis_index("sp")
    dp = lax.axis_index("dp")
    z, x = sp // nx, sp % nx
    me = x * n_dp + dp

    loads = [
        pltpu.make_async_copy(src, dst, w_sem.at[i])
        for i, (src, dst) in enumerate(((wg_hbm, wg), (wu_hbm, wu), (wd_hbm, wd)))
    ]
    for load in loads:
        load.start()

    def plane_peer(off):
        j = lax.rem(me + off, count)
        return j, (z * nx + j // n_dp, j % n_dp)

    def column_peer(dist):
        plane = lax.rem(z + dist, nz)
        return plane, (plane * nx + x, dp)

    barrier = pltpu.get_barrier_semaphore()
    for off in range(1, count):
        pl.semaphore_signal(barrier, inc=1, device_id=plane_peer(off)[1], device_id_type=MESH)
    for dist in range(1, nz):
        pl.semaphore_signal(barrier, inc=1, device_id=column_peer(dist)[1], device_id_type=MESH)

    meta = meta_ref[...]
    for g in range(nz):
        pick = group_choice(meta, jnp.int32(g * count), count, rows)
        p1[g] = contract(pick, normed_ref[...], (1, 0)).astype(BF16)
    metas[z] = meta
    r1[z] = p1[z]

    pl.semaphore_wait(barrier, count - 1 + nz - 1)
    for dist in range(1, nz):
        plane, device = column_peer(dist)
        remote(meta_ref, metas.at[z], sm.at[plane], tm.at[z], device).start()
        remote(p1.at[plane], r1.at[z], s1.at[plane], t1.at[z], device).start()

    first_expert = z * count

    def dispatch(dist, carry):
        source, device = column_peer(dist)

        @pl.when(dist > 0)
        def _():
            remote(meta_ref, metas.at[source], sm.at[source], tm.at[source], device).wait_recv()
            remote(p1.at[source], r1.at[source], s1.at[source], t1.at[source], device).wait_recv()

        got = metas[source]
        group = group_choice(got, first_expert, count, rows)
        first, second = slot_choice(got, first_expert, count, cap)
        pick = contract(first + second, group, (1, 1))
        packed = contract(pick, r1[source], (1, 0)).astype(BF16)
        p2[source] = packed.reshape(count, cap, width)
        r2[source, me] = p2[source, me]
        for off in range(1, count):
            j, device = plane_peer(off)
            remote(
                p2.at[source, j], r2.at[source, me], s2.at[source, j], t2.at[source, me], device
            ).start()
        return carry

    lax.fori_loop(0, nz, dispatch, 0)
    for load in loads:
        load.wait()

    def transform(dist, carry):
        source = lax.rem(z + dist + 1, nz)
        for off in range(1, count):
            j, device = plane_peer(off)
            remote(
                p2.at[source, j], r2.at[source, j], s2.at[source, j], t2.at[source, j], device
            ).wait_recv()
        arrived = r2[source].reshape(count * cap, width)
        gated = jnp.dot(arrived, wg[...], preferred_element_type=F32)
        lifted = jnp.dot(arrived, wu[...], preferred_element_type=F32)
        hidden = (gated / (1.0 + jnp.exp(-gated)) * lifted).astype(BF16)
        result = jnp.dot(hidden, wd[...], preferred_element_type=F32).astype(BF16)
        o2[source] = result.reshape(count, cap, width)
        back[source, me] = o2[source, me]
        for off in range(1, count):
            j, device = plane_peer(off)
            remote(
                o2.at[source, j], back.at[source, me], s3.at[source, j], t3.at[source, me], device
            ).start()
        return carry

    lax.fori_loop(0, nz, transform, 0)

    def combine(dist, carry):
        source, column = column_peer(dist + 1)
        for off in range(1, count):
            j, device = plane_peer(off)
            remote(
                o2.at[source, j], back.at[source, j], s3.at[source, j], t3.at[source, j], device
            ).wait_recv()
        got = metas[source]
        group = group_choice(got, first_expert, count, rows)
        first, second = slot_choice(got, first_expert, count, cap)
        outs = back[source].reshape(count * cap, width)
        one = contract(contract(group, first, (1, 1)), outs, (1, 0))
        two = contract(contract(group, second, (1, 1)), outs, (1, 0))
        weight = jnp.sum(group * got[2:3], axis=1, keepdims=True)
        share = jnp.sum(group * got[3:4], axis=1, keepdims=True)
        total = (weight * (share * one + (1.0 - share) * two)).astype(BF16)
        mix[source] = total

        @pl.when(dist == nz - 1)
        def _():
            fin[source] = total

        @pl.when(dist < nz - 1)
        def _():
            remote(mix.at[source], fin.at[z], s4.at[source], t4.at[z], column).start()

        return carry

    lax.fori_loop(0, nz, combine, 0)

    picks = [
        group_choice(meta, jnp.int32(g * count), count, rows) for g in range(nz)
    ]
    for dist in range(1, nz):
        plane, device = column_peer(dist)
        remote(mix.at[plane], fin.at[plane], s4.at[plane], t4.at[plane], device).wait_recv()
    every = jnp.concatenate(picks, axis=0)
    added = contract(every, fin[...].reshape(tokens, width), (0, 0))
    out_ref[...] = (stream_ref[...].astype(F32) + added).astype(BF16)

    for dist in range(1, nz):
        plane, device = column_peer(dist)
        remote(meta_ref, metas.at[z], sm.at[plane], tm.at[z], device).wait_send()
        remote(p1.at[plane], r1.at[z], s1.at[plane], t1.at[z], device).wait_send()
        remote(mix.at[plane], fin.at[z], s4.at[plane], t4.at[z], device).wait_send()

    def drain(source, carry):
        for off in range(1, count):
            j, device = plane_peer(off)
            remote(
                p2.at[source, j], r2.at[source, me], s2.at[source, j], t2.at[source, me], device
            ).wait_send()
            remote(
                o2.at[source, j], back.at[source, me], s3.at[source, j], t3.at[source, me], device
            ).wait_send()
        return carry

    lax.fori_loop(0, nz, drain, 0)


def local(
    residual_in, query_proj, key_proj, value_proj, query_gain, key_gain, out_weight, post_gain,
    pre_gain, route_ids, group_weight, first_share, gate_weight, up_weight, down_weight,
):
    n_sp = lax.axis_size("sp")
    n_dp = lax.axis_size("dp")
    tokens, width = query_proj.shape[1:]
    kv_width = key_proj.shape[2]
    heads, kv_heads = width // HEAD_DIM, kv_width // HEAD_DIM
    nz = GROUPS
    nx = n_sp // nz
    length = n_sp * tokens
    cos, sin = angle_tables(length)
    vmem = pl.BlockSpec(memory_space=pltpu.VMEM)
    hbm = pl.BlockSpec(memory_space=pl.ANY)
    dma = pltpu.SemaphoreType.DMA
    row = jax.ShapeDtypeStruct((tokens, width), BF16)
    stream, normed = pl.pallas_call(
        functools.partial(attention_kernel, nz, nx),
        out_shape=(row, row),
        in_specs=[vmem] * 10 + [hbm],
        out_specs=(vmem, vmem),
        scratch_shapes=[
            pltpu.VMEM((n_sp, kv_heads, tokens, HEAD_DIM), BF16),
            pltpu.VMEM((n_sp, kv_heads, tokens, HEAD_DIM), BF16),
            pltpu.VMEM((heads, tokens, HEAD_DIM), BF16),
            pltpu.VMEM((length, HEAD_DIM), BF16),
            pltpu.VMEM((tokens, width // kv_heads), BF16),
            pltpu.VMEM((tokens, width), F32),
            pltpu.VMEM((width, width), BF16),
            dma,
            dma((n_sp, kv_heads)), dma((n_sp, kv_heads)),
            dma((n_sp, kv_heads, nx)), dma((n_sp, kv_heads)), dma((n_sp, kv_heads)),
            dma((n_sp, kv_heads, nx)), dma((n_sp, kv_heads)), dma((n_sp, kv_heads)),
        ],
        compiler_params=pltpu.CompilerParams(
            collective_id=0, has_side_effects=True, vmem_limit_bytes=VMEM_LIMIT
        ),
        name="attention",
    )(
        query_proj[0], key_proj[0], value_proj[0],
        query_gain.reshape(1, -1), key_gain.reshape(1, -1),
        jnp.asarray(cos), jnp.asarray(sin),
        residual_in[0], post_gain.reshape(1, -1), pre_gain.reshape(1, -1), out_weight,
    )

    experts = gate_weight.shape[0] * n_sp * n_dp
    count = experts // nz
    cap = max(16, 4 * tokens // experts)
    rows = tokens // nz
    ff = gate_weight.shape[2]
    meta = jnp.concatenate(
        [route_ids[0].T.astype(F32), group_weight, first_share, jnp.zeros((4, tokens), F32)], axis=0
    )
    blocks = pltpu.VMEM((nz, count, cap, width), BF16)
    lines = pltpu.VMEM((nz, rows, width), BF16)
    out = pl.pallas_call(
        functools.partial(expert_kernel, nz, nx, n_dp),
        out_shape=row,
        in_specs=[vmem] * 3 + [hbm] * 3,
        out_specs=vmem,
        scratch_shapes=[
            pltpu.VMEM((width, ff), BF16),
            pltpu.VMEM((width, ff), BF16),
            pltpu.VMEM((ff, width), BF16),
            dma((3,)),
            lines, lines,
            pltpu.VMEM((nz, 8, tokens), F32),
            blocks, blocks, blocks, blocks,
            lines, lines,
            dma((nz,)), dma((nz,)), dma((nz,)), dma((nz,)),
            dma((nz, count)), dma((nz, count)), dma((nz, count)), dma((nz, count)),
            dma((nz,)), dma((nz,)),
        ],
        compiler_params=pltpu.CompilerParams(
            collective_id=1, has_side_effects=True, vmem_limit_bytes=VMEM_LIMIT
        ),
        name="experts",
    )(normed, stream, meta, gate_weight[0], up_weight[0], down_weight[0])
    return out.reshape(1, tokens, width)


LAYER_VMEM_LIMIT = 50 * 1024 * 1024


def layer_kernel(
    nz, nx, cores,
    q_hbm, k_hbm, v_hbm, qg_hbm, kg_hbm, res_hbm, post_hbm, pre_hbm, route_hbm, gw_hbm, fs_hbm,
    cos_hbm, sin_hbm, ow_hbm, wg_hbm, wu_hbm, wd_hbm,
    out,
    q_ref, k_ref, v_ref, qg_ref, kg_ref, res_ref, post_ref, pre_ref, route_ref, gw_ref, fs_ref,
    cos, sin, ow, wg, wu, wd, load_sem,
    kv, q_rot, att, acc, summing,
    rk_own, rk_x, rk_z, kv_x_sent, kv_z_sent,
    perm, perm_back, mrow, metas, picks, weights, backs,
    zs_sem, zr_sem, ms_sem, mr_sem,
    stream, srt, rows, y, other, part, relay, direct, summed, fin,
    t_z, t_a, t_b, t_c, t_d, t_core, spread_sent,
    t_other, t_up, t_side, t_last, t_home, back_sent,
):
    tokens, width = q_ref.shape
    heads = width // HEAD_DIM
    kv_heads = k_ref.shape[1] // HEAD_DIM
    group = heads // kv_heads
    slots_kv = nz * nx
    length = slots_kv * tokens
    last_head = kv_heads - 1
    chips = metas.shape[2]
    count = chips * cores
    block = tokens // nz
    cap = y.shape[2] // chips
    half = block // 2
    me = lax.axis_index("sp")
    dp = lax.axis_index("dp")
    z, x = me // nx, me % nx
    side, core = dp // cores, dp % cores
    up, down = (me + nx, dp), (me - nx, dp)
    beside = (z * nx + 1 - x, dp)
    across = (me, (1 - side) * cores + core)
    partner = (me, side * cores + 1 - core)
    has_up, has_down = z < nz - 1, z > 0
    sides = chips // nx
    mine = x * sides + side
    chip_x, chip_y = (1 - x) * sides + side, x * sides + 1 - side
    chip_d = (1 - x) * sides + 1 - side

    def column(plane):
        return (plane * nx + x, dp)

    flip = z >= nz // 2
    low = jnp.where(flip, nz - 1 - z, z)
    inner = (2, 0, 3)

    def source_of(i):
        if i == 0:
            return z
        near = jnp.where(low == 0, i, inner[i - 1])
        return jnp.where(flip, nz - 1 - near, near)

    sources = [source_of(i) for i in range(nz)]

    own = pl.multiple_of(me * tokens, tokens)
    loads = [
        pltpu.make_async_copy(src, dst, load_sem.at[i])
        for i, (src, dst) in enumerate((
            (k_hbm, k_ref), (v_hbm, v_ref), (kg_hbm, kg_ref),
            (cos_hbm.at[pl.ds(own, tokens)], cos), (sin_hbm.at[pl.ds(own, tokens)], sin),
            (q_hbm, q_ref), (qg_hbm, qg_ref), (route_hbm, route_ref), (gw_hbm, gw_ref),
            (fs_hbm, fs_ref), (ow_hbm, ow), (res_hbm, res_ref), (post_hbm, post_ref),
            (pre_hbm, pre_ref), (wg_hbm, wg), (wu_hbm, wu), (wd_hbm, wd),
        ))
    ]
    for load in loads[:10]:
        load.start()

    barrier = pltpu.get_barrier_semaphore()
    greeted = [column(lax.rem(z + dist, nz)) for dist in range(1, nz)] + [beside, across, partner]
    for device in greeted:
        pl.semaphore_signal(barrier, inc=1, device_id=device, device_id_type=MESH)


    for load in loads[:5]:
        load.wait()
    def turn(head):
        columns = slice(head * HEAD_DIM, (head + 1) * HEAD_DIM)
        kv[head * slots_kv + me, 1] = v_ref[:, columns]
        kv[head * slots_kv + me, 0] = rotate(k_ref[:, columns], kg_ref[...], cos[...], sin[...])

    turn(0)
    pl.semaphore_wait(barrier, len(greeted))

    def hop(slot, head, device, sent, landed):
        view = kv.at[head * slots_kv + slot]
        return remote(view, view, sent.at[0], landed, device)

    def bytes_of(units, sent, landed):
        view = kv.at[pl.ds(0, units)]
        return remote(view, view, sent, landed, beside)

    def own_beside(head):
        return hop(me, head, beside, kv_x_sent, rk_own.at[head])

    def pass_beside(slot, head):
        return hop(slot, head, beside, kv_x_sent, rk_x.at[head])

    def pass_on(slot, source, head, device):
        return hop(slot, head, device, kv_z_sent, rk_z.at[source, head])

    def cross_on(head, device):
        return hop(z * nx + 1 - x, head, device, kv_z_sent, rk_x.at[head])

    late_up, late_down = z == nz - 2, z == 1
    at_end = jnp.logical_or(z == 0, z == nz - 1)

    def send_along(head, given):
        for on, late, device in ((has_up, late_up, up), (has_down, late_down, down)):
            @pl.when((on & ~late if head == last_head else on) & given)
            def _(device=device):
                pass_on(me, z, head, device).start()

    def send_own(head):
        own_beside(head).start()
        send_along(head, True)

    def take_own(head):
        bytes_of(1, kv_x_sent.at[0], rk_own.at[head]).wait_recv()

    def crosses(head):
        return head % 2 == 1

    def cross(head):
        final = head == last_head
        take_own(head)
        for on, late, device in ((has_up, late_up, up), (has_down, late_down, down)):
            @pl.when(on & ~late if final else on)
            def _(device=device):
                cross_on(head, device).start()

    def relay_kv(head, dist, given=True):
        for below in (True, False):
            source = z - dist if below else z + dist
            present = source >= 0 if below else source < nz
            further = has_up if below else has_down
            onward = up if below else down

            @pl.when(present & given)
            def _(source=source, further=further, onward=onward):
                slot = source * nx + x
                bytes_of(1, kv_z_sent.at[0], rk_z.at[source, head]).wait_recv()

                @pl.when(further)
                def _():
                    pass_on(slot, source, head, onward).start()

                if dist > 1 or not crosses(head):
                    pass_beside(slot, head).start()

    def send_late(head):
        for late, device in ((late_up, up), (late_down, down)):
            @pl.when(late)
            def _(device=device):
                pass_on(me, z, head, device).start()
                if crosses(head):
                    cross_on(head, device).start()

    def near_wave(head):
        relay_kv(head, 1, ~at_end if head == last_head else True)
        if head == 0:
            send_own(last_head)
        if crosses(head) and head < last_head:
            cross(head)

    def wave(step):
        for dist in range(2, nz):
            head = step - (dist - 2)
            if 0 <= head < kv_heads:
                relay_kv(head, dist)
            if dist == 2 and head == last_head:
                send_late(last_head)
        if step == 1 and crosses(last_head):
            cross(last_head)

    for head in range(kv_heads):
        if head > 0:
            turn(head)
        if head < last_head:
            send_own(head)
    for load in loads[10:]:
        load.start()

    for load in loads[5:10]:
        load.wait()
    for head in range(heads):
        q_rot[head] = rotate(
            q_ref[:, head * HEAD_DIM : (head + 1) * HEAD_DIM], qg_ref[...], cos[...], sin[...]
        )
    acc[...] = jnp.zeros_like(acc)
    summing[:, HEAD_DIM:] = jnp.ones((length, HEAD_DIM), BF16)

    row = lax.broadcasted_iota(jnp.int32, (tokens, tokens), 0)
    lane = lax.broadcasted_iota(jnp.int32, (tokens, tokens), 1)

    def routing():
        first = route_ref[0:1].astype(F32)
        second = route_ref[1:2].astype(F32)
        of_lane = jnp.zeros_like(first)
        for g in range(1, nz):
            of_lane = of_lane + jnp.where(first >= float(g * count), 1.0, 0.0)
        of = jnp.sum(jnp.where(row == lane, of_lane, 0.0), axis=1, keepdims=True)
        same = of == of_lane
        rank = jnp.sum(jnp.where(same & (lane < row), 1.0, 0.0), axis=1, keepdims=True)
        rank_lane = jnp.sum(jnp.where(same & (row < lane), 1.0, 0.0), axis=0, keepdims=True)
        place = (of * float(block) + rank).astype(jnp.int32)
        place_lane = (of_lane * float(block) + rank_lane).astype(jnp.int32)
        perm[...] = jnp.where(row == place_lane, 1.0, 0.0).astype(BF16)
        perm_back[...] = jnp.where(place == lane, 1.0, 0.0).astype(BF16)
        fields = (
            first, second,
            gw_ref[...] * fs_ref[...], gw_ref[...] * (1.0 - fs_ref[...]),
        )
        chosen = lax.broadcasted_iota(jnp.int32, (8, tokens), 0).astype(F32) == of_lane
        at = rank.astype(jnp.int32)
        table = jnp.zeros((8, tokens), F32)
        for f, field in enumerate(fields):
            spread = jnp.where(lane == at + f * block, 1.0, 0.0)
            table += lax.dot_general(
                jnp.where(chosen, field, 0.0), spread, (((1,), (0,)), ((), ())),
                precision=lax.Precision.HIGHEST, preferred_element_type=F32,
            )
        for g in range(nz):
            mrow[g] = table[g : g + 1]

    routing()
    metas[z, core, mine] = mrow[z]

    def meta_column(dist):
        plane = lax.rem(z + dist, nz)
        return remote(
            mrow.at[plane], metas.at[z, core, mine], zs_sem.at[0], zr_sem.at[0], column(plane)
        )

    def meta_all():
        view = mrow.at[pl.ds(0, nz - 1)]
        return remote(view, view, zs_sem.at[0], zr_sem.at[0], beside)

    for dist in range(1, nz):
        meta_column(dist).start()

    def meta_copy(view, step, device):
        return remote(view, view, ms_sem.at[step], mr_sem.at[step], device)

    pair = pl.ds(x * sides, sides)
    other_pair = pl.ds((1 - x) * sides, sides)
    meta_sends = (
        meta_copy(metas.at[:, core, mine], 0, across),
        meta_copy(metas.at[:, core, pair], 1, partner),
        meta_copy(metas.at[:, :, pair], 2, beside),
    )
    meta_recvs = (
        meta_copy(metas.at[:, core, chip_y], 0, across),
        meta_copy(metas.at[:, 1 - core, pair], 1, partner),
        meta_copy(metas.at[:, :, other_pair], 2, beside),
    )

    def choice(plane, of_core, expert):
        table = metas[plane, of_core].reshape(chips, tokens)
        first = table[:, 0:block] == expert
        second = table[:, block : 2 * block] == expert
        member = jnp.where(first | second, 1.0, 0.0)
        weight = jnp.where(first, table[:, 2 * block : 3 * block], 0.0)
        weight = weight + jnp.where(second, table[:, 3 * block : 4 * block], 0.0)
        r = lax.broadcasted_iota(jnp.int32, (block, block), 0)
        c = lax.broadcasted_iota(jnp.int32, (block, block), 1)
        earlier = jnp.where(r < c, 1.0, 0.0).astype(BF16)
        rank = jnp.dot(
            jnp.concatenate([member] * (8 // chips), axis=0).astype(BF16), earlier,
            preferred_element_type=F32,
        )[:chips]
        place = lax.broadcasted_iota(jnp.int32, (chips, cap, block), 1).astype(F32)
        hit = jnp.where(rank[:, None, :] == place, 1.0, 0.0) * member[:, None, :]
        of_slot = jnp.sum(hit * weight[:, None, :], axis=2, keepdims=True).reshape(chips * cap, 1)
        flat = hit.reshape(chips * cap, block).astype(BF16)
        wide_row = lax.broadcasted_iota(jnp.int32, (block, tokens), 0)
        wide_lane = lax.broadcasted_iota(jnp.int32, (block, tokens), 1)
        widen = jnp.where(lax.rem(wide_lane, block) == wide_row, 1.0, 0.0).astype(BF16)
        spread = jnp.dot(flat, widen, preferred_element_type=F32)
        slot = lax.broadcasted_iota(jnp.int32, (chips * cap, tokens), 0) // cap
        chip = lax.broadcasted_iota(jnp.int32, (chips * cap, tokens), 1) // block
        return jnp.where(slot == chip, spread, 0.0), of_slot

    def tables():
        expert = (z * count + x * (count // nx) + dp).astype(F32)
        twin = (z * count + x * (count // nx) + side * cores + 1 - core).astype(F32)

        def one_plane(plane, carry):
            for of_core in range(cores):
                pick, of_slot = choice(plane, of_core, expert)
                picks[plane, of_core] = pick.astype(BF16)
                weights[plane, of_core] = of_slot
            back, _ = choice(plane, core, expert)
            theirs, _ = choice(plane, core, twin)
            backs[plane] = jnp.concatenate([back, theirs], axis=0).T.astype(BF16)
            return carry

        lax.fori_loop(0, nz, one_plane, 0)

    factor = float(HEAD_DIM**-0.5 * np.log2(np.e))
    span = group * HEAD_DIM

    def attend(head):
        here = pl.ds(head * slots_kv, slots_kv)
        keys = kv[here, 0].reshape(length, HEAD_DIM)
        summing[:, :HEAD_DIM] = kv[here, 1].reshape(length, HEAD_DIM)

        def scores_of(member):
            return lax.dot_general(
                q_rot[head * group + member], keys, (((1,), (1,)), ((), ())),
                preferred_element_type=F32,
            )

        scores = scores_of(0)
        for member in range(group):
            later = scores_of(member + 1) if member + 1 < group else None
            top = jnp.max(scores, axis=-1, keepdims=True)
            raised = jnp.exp2((scores - top) * factor).astype(BF16)
            mixed = jnp.dot(raised, summing[...], preferred_element_type=F32)
            att[:, member * HEAD_DIM : (member + 1) * HEAD_DIM] = (
                mixed[:, :HEAD_DIM] / mixed[:, HEAD_DIM:]
            ).astype(BF16)
            scores = later
        above = ow.at[pl.ds(pl.multiple_of(head * span, span), span), :]
        tile = 1024
        for start in range(0, width, tile):
            columns = slice(start, start + tile)
            acc[:, columns] += jnp.dot(att[...], above[:, columns], preferred_element_type=F32)

    near_wave(0)
    near_wave(1)
    wave(0)
    for head in range(2, kv_heads):
        near_wave(head)
    wave(1)
    meta_all().wait_recv()
    meta_sends[0].start()
    loads[10].wait()
    wave(2)
    wave(3)
    meta_recvs[0].wait_recv()
    meta_sends[1].start()

    def one_head(head, carry):
        @pl.when(head == 1)
        def _():
            wave(4)
            meta_recvs[1].wait_recv()
            meta_sends[2].start()

        @pl.when(head == 2)
        def _():
            relay_kv(last_head, 1, at_end)

        @pl.when(lax.rem(head, 2) == 0)
        def _():
            take_own(head)

        bytes_of(nz - 1, kv_x_sent.at[0], rk_x.at[head]).wait_recv()
        attend(head)
        return carry

    lax.fori_loop(0, kv_heads, one_head, 0)
    for load in loads[11:14]:
        load.wait()

    for start in range(0, tokens, 16):
        lines = slice(start, start + 16)
        blend = acc[lines, :].astype(BF16).astype(F32)
        blend = blend * lax.rsqrt(jnp.mean(blend * blend, axis=-1, keepdims=True) + EPSILON)
        flow = (res_ref[lines, :].astype(F32) + blend * post_ref[...]).astype(BF16)
        stream[lines, :] = flow
        wide = flow.astype(F32)
        wide = wide * lax.rsqrt(jnp.mean(wide * wide, axis=-1, keepdims=True) + EPSILON)
        out[lines, :] = (wide * pre_ref[...]).astype(BF16)
    normed = out[...]
    srt[...] = jnp.dot(perm[...], normed, preferred_element_type=F32).astype(BF16).reshape(srt.shape)

    def unit(s, of_core, chip, h=0):
        return ((s * cores + of_core) * chips + chip) * 2 + h

    def units(first, amount):
        return rows.at[pl.ds(first, amount)]

    def waiting(amount, landed):
        return remote(units(0, amount), units(0, amount), spread_sent.at[0], landed, partner)

    def z_send(plane):
        return remote(
            srt.at[pl.ds(2 * plane, 2)], units(unit(z, core, mine), 2), spread_sent.at[0], t_z.at[z],
            column(plane),
        )

    z_send(sources[1]).start()

    @pl.when(~at_end)
    def _():
        z_send(sources[2]).start()

    rows[pl.ds(unit(z, core, mine), 2)] = srt[pl.ds(2 * z, 2)]

    def over(s, chip, h, landed, device):
        view = rows.at[unit(s, core, chip, h)]
        return remote(view, view, spread_sent.at[0], landed.at[s], device)

    def over_core(s, chip):
        view = units(unit(s, core, chip), 2)
        return remote(view, view, spread_sent.at[0], t_core.at[s], partner)

    def route_tables(i):
        z_send(jnp.where(at_end, sources[2], sources[3])).start()
        meta_recvs[2].wait_recv()
        tables()

    def send_far(i):
        @pl.when(at_end)
        def _():
            z_send(sources[i]).start()

    def spread_own(i):
        s = sources[i]
        if i > 0:
            waiting(2, t_z.at[s]).wait_recv()
        over(s, mine, 0, t_a, beside).start()
        over(s, mine, 1, t_b, across).start()
        over(s, mine, 1, t_c, beside).start()
        over(s, mine, 0, t_c, across).start()
        over_core(s, mine).start()

    def spread_on(i):
        s = sources[i]
        waiting(1, t_a.at[s]).wait_recv()
        over(s, chip_x, 0, t_d, across).start()
        waiting(1, t_b.at[s]).wait_recv()
        over(s, chip_y, 1, t_d, beside).start()

    def spread_core(i):
        s = sources[i]
        waiting(2, t_c.at[s]).wait_recv()
        over_core(s, chip_x).start()
        over_core(s, chip_y).start()

    def spread_last(i):
        s = sources[i]
        waiting(2, t_d.at[s]).wait_recv()
        over_core(s, chip_d).start()

    def to_partner(s):
        return remote(y.at[s, 1 - core], other.at[s], back_sent.at[0], t_other.at[s], partner)

    def transform(i):
        s = sources[i]
        waiting(2 * chips, t_core.at[s]).wait_recv()
        packed = [
            jnp.dot(
                picks[s, q], rows[pl.ds(unit(s, q, 0), 2 * chips)].reshape(tokens, width), preferred_element_type=F32
            ).astype(BF16)
            for q in range(cores)
        ]
        packed = jnp.concatenate(packed, axis=0)
        gated = jnp.dot(packed, wg[...], preferred_element_type=F32)
        lifted = jnp.dot(packed, wu[...], preferred_element_type=F32)
        hidden = (gated / (1.0 + jnp.exp(-gated)) * lifted).astype(BF16)
        result = jnp.dot(hidden, wd[...], preferred_element_type=F32)
        slots = chips * cap
        for q in range(cores):
            y[s, q] = (result[q * slots : (q + 1) * slots] * weights[s, q]).astype(BF16)
        to_partner(s).start()

    def back(s, chip, h, into, at, landed, device):
        return remote(
            part.at[s, chip, halves[h]], into.at[s, at], back_sent.at[0], landed.at[s], device
        )

    halves = (pl.ds(0, half), pl.ds(half, half))

    def gather_back(i):
        s = sources[i]
        to_partner(s).wait_recv()
        outs = jnp.concatenate([y[s, core], other[s]], axis=0)
        part[s] = jnp.dot(backs[s], outs, preferred_element_type=F32).astype(BF16).reshape(
            chips, block, width
        )
        back(s, chip_d, 0, relay, 0, t_up, across).start()
        back(s, chip_d, 1, relay, 1, t_side, beside).start()
        back(s, chip_x, 1, direct, 1, t_last, beside).start()
        back(s, chip_y, 0, direct, 0, t_last, across).start()

    def add(left, right):
        return (left.astype(F32) + right.astype(F32)).astype(BF16)

    def pass_back(i):
        s = sources[i]
        waiting(1, t_up.at[s]).wait_recv()
        part[s, chip_x, halves[0]] = add(part[s, chip_x, halves[0]], relay[s, 0])
        back(s, chip_x, 0, summed, 0, t_last, beside).start()
        waiting(1, t_side.at[s]).wait_recv()
        part[s, chip_y, halves[1]] = add(part[s, chip_y, halves[1]], relay[s, 1])
        back(s, chip_y, 1, summed, 1, t_last, across).start()

    def home(s):
        return remote(part.at[s, mine], fin.at[z], back_sent.at[0], t_home.at[0], column(s))

    def finish(i):
        s = sources[i]
        waiting(4, t_last.at[s]).wait_recv()
        for h in range(2):
            total = part[s, mine, halves[h]].astype(F32) + direct[s, h].astype(F32)
            total = (total + summed[s, h].astype(F32)).astype(BF16)
            if i > 0:
                part[s, mine, halves[h]] = total
            else:
                fin[s, halves[h]] = total
        if i > 0:
            home(s).start()

    def weights_ready(i):
        for load in loads[14:]:
            load.wait()

    for stage, i in plan(
        route_tables, send_far, spread_own, spread_on, spread_core, spread_last, weights_ready, transform, gather_back, pass_back, finish
    ):
        stage(i)

    waiting(2 * (nz - 1), t_home.at[0]).wait_recv()
    tile = width // 4
    for start in range(0, width, tile):
        columns = slice(start, start + tile)
        added = jnp.dot(
            perm_back[...], fin[:, :, columns].reshape(tokens, tile), preferred_element_type=F32
        )
        out[:, columns] = (stream[:, columns].astype(F32) + added).astype(BF16)

    for plane in range(nz):
        lanes = sum(head % 2 for head in range(kv_heads))
        upward = (plane + 1) * kv_heads + lanes if plane < nz - 1 else 0
        downward = (nz - plane) * kv_heads + lanes if plane > 0 else 0
        sideways = nz * kv_heads - lanes * sum(0 <= plane + d < nz for d in (-1, 1))

        @pl.when(z == plane)
        def _(vertical=upward + downward, sideways=sideways):
            bytes_of(vertical, kv_z_sent.at[0], rk_own.at[0]).wait_send()
            bytes_of(sideways, kv_x_sent.at[0], rk_own.at[0]).wait_send()

    meta_all().wait_send()
    for send in meta_sends:
        send.wait_send()
    spread_units = 2 * (nz - 1) + nz * (6 + 2 * chips)
    waiting(spread_units, t_core.at[0]).wait_send()
    back_units = nz * (2 * chips * cap // block + 6) + 2 * (nz - 1)
    returned = units(0, back_units)
    remote(returned, returned, back_sent.at[0], t_core.at[0], partner).wait_send()


def plan(route, far, own, on, share, last, ready, transform, gather_back, pass_back, finish):
    return (
        (own, 0), (route, 0), (far, 3), (on, 0), (own, 1), (share, 0), (on, 1), (last, 0),
        (own, 2), (share, 1), (ready, 0), (transform, 0), (on, 2), (last, 1), (own, 3),
        (share, 2), (transform, 1), (on, 3), (gather_back, 1), (last, 2), (transform, 2),
        (share, 3), (pass_back, 1), (gather_back, 2), (last, 3), (transform, 3), (finish, 1),
        (pass_back, 2), (gather_back, 3), (finish, 2), (pass_back, 3), (gather_back, 0),
        (finish, 3), (pass_back, 0), (finish, 0),
    )


def fused(
    residual_in, query_proj, key_proj, value_proj, query_gain, key_gain, out_weight, post_gain,
    pre_gain, route_ids, group_weight, first_share, gate_weight, up_weight, down_weight,
):
    n_sp = lax.axis_size("sp")
    n_dp = lax.axis_size("dp")
    tokens, width = query_proj.shape[1:]
    kv_heads = key_proj.shape[2] // HEAD_DIM
    heads = width // HEAD_DIM
    nz = GROUPS
    nx = n_sp // nz
    cores = 2
    chips = nx * (n_dp // cores)
    experts = gate_weight.shape[0] * n_sp * n_dp
    cap = max(16, 4 * tokens // experts)
    block = tokens // nz
    slots = chips * cap
    ff = gate_weight.shape[2]
    length = n_sp * tokens
    cos, sin = angle_tables(length)
    vmem = pl.BlockSpec(memory_space=pltpu.VMEM)
    hbm = pl.BlockSpec(memory_space=pl.ANY)
    dma = pltpu.SemaphoreType.DMA

    def buf(*shape, kind=BF16):
        return pltpu.VMEM(shape, kind)

    out = pl.pallas_call(
        functools.partial(layer_kernel, nz, nx, cores),
        out_shape=jax.ShapeDtypeStruct((tokens, width), BF16),
        in_specs=[hbm] * 17,
        out_specs=vmem,
        scratch_shapes=[
            buf(tokens, width), buf(tokens, kv_heads * HEAD_DIM), buf(tokens, kv_heads * HEAD_DIM),
            buf(1, HEAD_DIM, kind=F32), buf(1, HEAD_DIM, kind=F32), buf(tokens, width),
            buf(1, width, kind=F32), buf(1, width, kind=F32),
            buf(2, tokens, kind=jnp.int32), buf(1, tokens, kind=F32), buf(1, tokens, kind=F32),
            buf(tokens, HEAD_DIM, kind=F32), buf(tokens, HEAD_DIM, kind=F32),
            buf(width, width), buf(width, ff), buf(width, ff), buf(ff, width),
            dma((17,)),
            buf(kv_heads * n_sp, 2, tokens, HEAD_DIM),
            buf(heads, tokens, HEAD_DIM),
            buf(tokens, width // kv_heads),
            buf(tokens, width, kind=F32),
            buf(length, 2 * HEAD_DIM),
            dma((kv_heads,)), dma((kv_heads,)), dma((nz, kv_heads)), dma((1,)), dma((1,)),
            buf(tokens, tokens), buf(tokens, tokens),
            buf(nz, 1, tokens, kind=F32), buf(nz, cores, chips, 1, tokens, kind=F32),
            buf(nz, cores, slots, tokens), buf(nz, cores, slots, 1, kind=F32),
            buf(nz, tokens, cores * slots),
            dma((1,)), dma((1,)), dma((3,)), dma((3,)),
            buf(tokens, width), buf(2 * nz, block // 2, width),
            buf(nz * cores * chips * 2, block // 2, width),
            buf(nz, cores, slots, width), buf(nz, slots, width),
            buf(nz, chips, block, width),
            buf(nz, 2, block // 2, width), buf(nz, 2, block // 2, width),
            buf(nz, 2, block // 2, width), buf(nz, block, width),
            dma((nz,)), dma((nz,)), dma((nz,)), dma((nz,)), dma((nz,)), dma((nz,)), dma((1,)),
            dma((nz,)), dma((nz,)), dma((nz,)), dma((nz,)), dma((1,)), dma((1,)),
        ],
        compiler_params=pltpu.CompilerParams(
            collective_id=0, has_side_effects=True, vmem_limit_bytes=LAYER_VMEM_LIMIT
        ),
        name="layer",
    )(*(pltpu.with_memory_space_constraint(array, pltpu.HBM) for array in (
        query_proj[0], key_proj[0], value_proj[0],
        query_gain.reshape(1, -1), key_gain.reshape(1, -1),
        residual_in[0], post_gain.reshape(1, -1), pre_gain.reshape(1, -1),
        route_ids[0].T, group_weight, first_share,
        jnp.asarray(cos), jnp.asarray(sin), out_weight,
        gate_weight[0], up_weight[0], down_weight[0],
    )))
    return out.reshape(1, tokens, width)


def solution(mesh):
    tok3 = P("dp", "sp", None)
    tok2 = P("dp", "sp")
    weight = P(("sp", "dp"), None, None)
    placed = (
        tok3, tok3, tok3, tok3, P(), P(), P(), P(), P(), tok3, tok2, tok2, weight, weight, weight,
    )
    small = mesh.shape["sp"] == 2 * GROUPS and mesh.shape["dp"] == 4
    return jax.shard_map(
        fused if small else local, mesh=mesh, in_specs=placed, out_specs=P("dp", "sp", None), check_vma=False
    )
```
